128 devices in a mesh: sp: 16 (over z, y), tp: 8 (over x, core).
Axes of the slice: x: 4, y: 4, z: 4, core: 2. Of those that a mesh axis runs over, the one named last changes fastest.
Arguments:
- inputs: bfloat16 [8192, 4096], P(('sp', 'tp')), may hold values from -42 to 42
- a_query_w: bfloat16 [4096, 2048], P(None, 'tp'), may hold values from -0.12570312 to 0.12570312
- a_key_w: bfloat16 [4096, 2048], P(None, 'tp'), may hold values from -0.12570312 to 0.12570312
- a_value_w: bfloat16 [4096, 2048], P(None, 'tp'), may hold values from -0.09375 to 0.09375
- b_query_w: bfloat16 [4096, 2048], P(None, 'tp'), may hold values from -0.12570312 to 0.12570312
- b_key_w: bfloat16 [4096, 512], P(None, 'tp'), may hold values from -0.12570312 to 0.12570312
- b_value_w: bfloat16 [4096, 512], P(None, 'tp'), may hold values from -0.09375 to 0.09375
- head_lambda: float32 [16], P('tp'), may hold values from 0.3 to 0.8
- head_gain: float32 [128], replicated, may hold values from 0.1 to 1.9
- sink_logit: float32 [32], P('tp'), may hold values from 2 to 7
- a_out_w: bfloat16 [2048, 4096], P('tp'), may hold values from -0.125 to 0.125
- b_out_w: bfloat16 [2048, 4096], P('tp'), may hold values from -0.625 to 0.625
Outputs:
- mixed: bfloat16 [8192, 4096], P(('sp', 'tp'))
The draws below stay inside these ranges and needn't reach their ends.
All inputs are finite; a program needn't handle non-finite values.
Results may differ from the reference program's by a relative error of at most 0.015.
Values may be sent and summed in bfloat16 or wider, within the bound.
A program may use at most 128 MiB of HBM per device.

```python
import math
import jax
import jax.numpy as jnp
from jax import lax

D = 4096
A_HEADS = 16
B_HEADS = 32
KV_HEADS = 8
HEAD_DIM = 64
VALUE_DIM = 128
WINDOW = 128
TOKENS = 8192
N_TP = 8


def plain_noise(key, salt, columns):
    values = jnp.clip(jax.random.normal(jax.random.fold_in(key, salt), (D, columns), jnp.float32), -6.0, 6.0)
    return values * (1.32 * D ** (-0.5))


def draw_inputs(key, part):
    values = jnp.clip(jax.random.normal(jax.random.fold_in(key, 10), (TOKENS, D), jnp.float32), -6.0, 6.0)
    return values.astype(jnp.bfloat16)


def draw_a_query_w(key, part):
    columns = 2 * A_HEADS * HEAD_DIM
    values = plain_noise(key, 11, columns)
    return values.astype(jnp.bfloat16)


def draw_a_key_w(key, part):
    columns = 2 * A_HEADS * HEAD_DIM
    values = plain_noise(key, 12, columns)
    return values.astype(jnp.bfloat16)


def draw_b_query_w(key, part):
    columns = B_HEADS * HEAD_DIM
    values = plain_noise(key, 13, columns)
    return values.astype(jnp.bfloat16)


def draw_b_key_w(key, part):
    columns = KV_HEADS * HEAD_DIM
    values = plain_noise(key, 14, columns)
    return values.astype(jnp.bfloat16)


def block_levels(key, shape, shards, smallest, high):
    gain, own = 1.0, jax.random.fold_in(key, 6)
    for axis_at, shards_of in shards:
        steps = jnp.exp(jax.random.uniform(jax.random.fold_in(own, axis_at), (shards_of,), jnp.float32, smallest / len(shards), high / len(shards)))
        gain = gain * jnp.repeat(steps, shape[axis_at] // shards_of).reshape([-1 if axis == axis_at else 1 for axis in range(len(shape))])
    return gain


def normal_values(own_key, extent, width, reach, cuts=(), kind=jnp.bfloat16):
    level = block_levels(own_key, extent, cuts, -0.22, 0.18) if cuts else 1.0
    drawn = jax.random.normal(own_key, extent, jnp.float32) * width * level
    return jnp.minimum(jnp.maximum(drawn, -reach), reach).astype(kind)


def setup_inputs(seed: int = 0) -> dict:
    seeds = jax.random.split(jax.random.key(seed), 13)
    inputs = draw_inputs(jax.random.fold_in(seeds[12], 71), 0)
    a_query_w = draw_a_query_w(jax.random.fold_in(seeds[12], 71), 0)
    a_key_w = draw_a_key_w(jax.random.fold_in(seeds[12], 71), 0)
    a_value_w = normal_values(seeds[3], (D, A_HEADS * VALUE_DIM), D ** -0.5, 0.09375, ((1, 8),))
    b_query_w = draw_b_query_w(jax.random.fold_in(seeds[12], 71), 0)
    b_key_w = draw_b_key_w(jax.random.fold_in(seeds[12], 71), 0)
    b_value_w = normal_values(seeds[6], (D, KV_HEADS * HEAD_DIM), D ** -0.5, 0.09375, ((1, 8),))
    head_lambda = jnp.clip(0.3 + 0.5 * jax.random.uniform(seeds[7], (A_HEADS,), jnp.float32) ** block_levels(seeds[7], (A_HEADS,), ((0, 8),), -0.2, 0.2), 0.3, 0.8)
    head_gain = jnp.clip(1.0 + 0.18 * jax.random.normal(seeds[8], (VALUE_DIM,), jnp.float32), 0.1, 1.9)
    sink_logit = jnp.clip(2.0 + 5.0 * jax.random.uniform(seeds[9], (B_HEADS,), jnp.float32) ** block_levels(seeds[9], (B_HEADS,), ((0, 8),), -0.2, 0.2), 2.0, 7.0)
    a_out_w = normal_values(seeds[10], (A_HEADS * VALUE_DIM, D), (A_HEADS * VALUE_DIM) ** -0.5, 0.125, ((0, 8),))
    b_out_w = normal_values(seeds[11], (B_HEADS * HEAD_DIM, D), (5.0 * (B_HEADS * HEAD_DIM) ** -0.5), 0.625, ((0, 8),))
    return {"inputs": inputs, "a_query_w": a_query_w, "a_key_w": a_key_w, "a_value_w": a_value_w, "b_query_w": b_query_w, "b_key_w": b_key_w, "b_value_w": b_value_w, "head_lambda": head_lambda, "head_gain": head_gain, "sink_logit": sink_logit, "a_out_w": a_out_w, "b_out_w": b_out_w}


norm_eps = 0.0001
head_scale = 0.8
mask_fill = -1e+30

def rounded(value):
    return lax.optimization_barrier(value.astype(jnp.bfloat16)).astype(jnp.float32)

def reference(inputs, a_query_w, a_key_w, a_value_w, b_query_w, b_key_w, b_value_w, head_lambda, head_gain, sink_logit, a_out_w, b_out_w):
    length = inputs.shape[0]
    group_size = B_HEADS // KV_HEADS
    score_scale = HEAD_DIM ** (-0.5)
    a_query = jnp.dot(inputs, a_query_w, preferred_element_type=jnp.float32).astype(jnp.bfloat16).reshape(length, A_HEADS, 2, HEAD_DIM)
    a_key = jnp.dot(inputs, a_key_w, preferred_element_type=jnp.float32).astype(jnp.bfloat16).reshape(length, A_HEADS, 2, HEAD_DIM)
    a_value = jnp.dot(inputs, a_value_w, preferred_element_type=jnp.float32).astype(jnp.bfloat16).reshape(length, A_HEADS, VALUE_DIM)
    b_query = jnp.dot(inputs, b_query_w, preferred_element_type=jnp.float32).astype(jnp.bfloat16).reshape(length, KV_HEADS, group_size, HEAD_DIM)
    b_key = jnp.dot(inputs, b_key_w, preferred_element_type=jnp.float32).astype(jnp.bfloat16).reshape(length, KV_HEADS, HEAD_DIM)
    b_value = jnp.dot(inputs, b_value_w, preferred_element_type=jnp.float32).astype(jnp.bfloat16).reshape(length, KV_HEADS, HEAD_DIM)
    query_span = math.gcd(length, 128)
    span_count = length // query_span
    key_pos = jnp.arange(length, dtype=jnp.int32)
    keys_wide = a_key.astype(jnp.float32)
    values_wide = a_value.astype(jnp.float32)

    def differential(block_index):
        block_start = block_index * query_span
        queries = lax.dynamic_slice_in_dim(a_query, block_start, query_span, 0).astype(jnp.float32)
        scores = jnp.einsum('qhmd,khmd->hmqk', queries, keys_wide) * score_scale
        query_pos = block_start + jnp.arange(query_span, dtype=jnp.int32)
        allowed = query_pos[:, None] >= key_pos[None, :]
        scores = jnp.where(allowed, scores, mask_fill)
        row_top = lax.optimization_barrier(jnp.max(scores, axis=-1, keepdims=True))
        weights = jnp.where(allowed, jnp.exp(scores - row_top), 0.0)
        row_total = lax.optimization_barrier(jnp.sum(weights, axis=-1))
        means = jnp.einsum('hmqk,khe->hmqe', rounded(weights), values_wide) / row_total[..., None]
        difference = means[:, 0] - head_lambda[:, None, None] * means[:, 1]
        mean_square = lax.optimization_barrier(jnp.mean(difference * difference, axis=-1, keepdims=True))
        return (difference * lax.rsqrt(mean_square + norm_eps) * head_gain * head_scale).astype(jnp.bfloat16)
    a_heads = lax.map(differential, jnp.arange(span_count, dtype=jnp.int32))
    a_heads = jnp.transpose(a_heads, (1, 0, 2, 3)).reshape(A_HEADS, length, VALUE_DIM)
    pad_keys = jnp.concatenate([jnp.zeros((WINDOW, KV_HEADS, HEAD_DIM), jnp.bfloat16), b_key], axis=0).astype(jnp.float32)
    pad_values = jnp.concatenate([jnp.zeros((WINDOW, KV_HEADS, HEAD_DIM), jnp.bfloat16), b_value], axis=0).astype(jnp.float32)
    sink_term = sink_logit.reshape(KV_HEADS, group_size)[:, :, None]

    def windowed(block_index):
        block_start = block_index * query_span
        queries = lax.dynamic_slice_in_dim(b_query, block_start, query_span, 0).astype(jnp.float32)
        block_keys = lax.dynamic_slice_in_dim(pad_keys, block_start, query_span + WINDOW, 0)
        block_values = lax.dynamic_slice_in_dim(pad_values, block_start, query_span + WINDOW, 0)
        scores = jnp.einsum('qhgd,khd->hgqk', queries, block_keys) * score_scale
        query_pos = block_start + jnp.arange(query_span, dtype=jnp.int32)
        near_pos = block_start - WINDOW + jnp.arange(query_span + WINDOW, dtype=jnp.int32)
        distance = query_pos[:, None] - near_pos[None, :]
        allowed = (distance >= 0) & (distance < WINDOW) & (near_pos[None, :] >= 0)
        scores = jnp.where(allowed, scores, mask_fill)
        row_top = jnp.maximum(lax.optimization_barrier(jnp.max(scores, axis=-1)), sink_term)
        weights = jnp.where(allowed, jnp.exp(scores - row_top[..., None]), 0.0)
        row_total = lax.optimization_barrier(jnp.sum(weights, axis=-1)) + jnp.exp(sink_term - row_top)
        probs = weights / row_total[..., None]
        block_out = jnp.einsum('hgqk,khd->qhgd', rounded(probs), block_values)
        return block_out.reshape(query_span, B_HEADS * HEAD_DIM).astype(jnp.bfloat16)
    b_heads = lax.map(windowed, jnp.arange(span_count, dtype=jnp.int32)).reshape(length, B_HEADS * HEAD_DIM)
    heads_local = A_HEADS // N_TP
    cols_local = B_HEADS * HEAD_DIM // N_TP
    summed = jnp.zeros((length, D), jnp.float32)
    for group_index in range(N_TP):
        a_part = a_heads[group_index * heads_local:(group_index + 1) * heads_local].astype(jnp.float32)
        a_weight = a_out_w[group_index * heads_local * VALUE_DIM:(group_index + 1) * heads_local * VALUE_DIM]
        a_weight = a_weight.reshape(heads_local, VALUE_DIM, D).astype(jnp.float32)
        b_part = b_heads[:, group_index * cols_local:(group_index + 1) * cols_local]
        b_weight = b_out_w[group_index * cols_local:(group_index + 1) * cols_local]
        partial_sum = jnp.einsum('hqe,hen->qn', a_part, a_weight) + jnp.dot(b_part, b_weight, preferred_element_type=jnp.float32)
        summed = summed + rounded(partial_sum)
    return summed.astype(jnp.bfloat16)
```

```python
import functools

import jax
import jax.numpy as jnp
from jax import lax
from jax.experimental import pallas as pl
from jax.experimental.pallas import tpu as pltpu
from jax.sharding import PartitionSpec as P

HEAD_DIM = 64
VALUE_DIM = 128
WINDOW = 128

norm_eps = 0.0001
head_scale = 0.8
mask_fill = -1e30

MESH = pl.DeviceIdType.MESH
NT = (((1,), (1,)), ((), ()))
LOG2E = 1.4426950408889634
VMEM = pltpu.VMEM
F32 = jnp.float32
BF16 = jnp.bfloat16


def remote(src, dst, send_sem, recv_sem, row, col):
    return pltpu.make_async_remote_copy(
        src_ref=src,
        dst_ref=dst,
        send_sem=send_sem,
        recv_sem=recv_sem,
        device_id=(row, col),
        device_id_type=MESH,
    )


def soft_chunk(items, score, lookup, mx, ls, acc):
    def weights(i, pieces):
        before = mx[i]
        top = before
        for piece in pieces:
            top = jnp.maximum(top, jnp.max(piece, axis=0, keepdims=True))
        shrink = jnp.exp2(before - top)
        mx[i] = top
        return shrink, [jnp.exp2(piece - top).astype(BF16) for piece in pieces]

    def collect(i, shrink, pieces):
        got = jnp.dot(lookup, jnp.concatenate(pieces, axis=0), preferred_element_type=F32)
        acc[i] = acc[i] * shrink + got[:VALUE_DIM]
        ls[i] = ls[i] * shrink + got[VALUE_DIM : VALUE_DIM + 1]

    now = score(items[0])
    held = None
    for at, i in enumerate(items):
        later = score(items[at + 1]) if at + 1 < len(items) else None
        current = weights(i, now)
        if held is not None:
            collect(items[at - 1], *held)
        held, now = current, later
    collect(items[-1], *held)


def attention_kernel(
    q_in, kv_in, bq_in, bkv_in, lam_in, gain_in, sink_in,
    a_out, b_out,
    kv, q_raw, q_mul, near, lam, acc, mx, ls, stage, back,
    a2a_s, a2a_r, zs, zr, rs, rr, ds, dr, q_s, q_r, small_s, small_r, ret_s, ret_r,
):
    s, t = lax.axis_index("sp"), lax.axis_index("tp")
    z, y = s // 4, s % 4
    x, c = t // 2, t % 2
    other = 2 * x + 1 - c
    up, down = (z + 1) % 4, (z + 3) % 4
    far = (z + 2) % 4
    mate = 3 - z
    side = z + 1 - 2 * (z % 2)
    quarter = 2 * c + z // 2
    order = (y, y + 1 - 2 * (y % 2), 3 - y, (y + 2) % 4)

    barrier = pltpu.get_barrier_semaphore()

    def greet(row, col):
        pl.semaphore_signal(barrier, inc=1, device_id=(row, col), device_id_type=MESH)

    for j in range(4):
        for core in range(2):
            if j == 0:
                @pl.when(core != c)
                def _(core=core):
                    greet(4 * z + y, 2 * x + core)
            else:
                greet(4 * z + (y + j) % 4, 2 * x + core)
            greet(4 * mate + (y + j) % 4, 2 * x + core)
    greet(4 * side + y, t)
    rim_up = (y == 3) & (z % 2 == 0)
    rim_down = (y == 0) & (z % 2 == 1)

    @pl.when(rim_up)
    def _():
        greet(s + 1, t)

    @pl.when(rim_down)
    def _():
        greet(s - 1, t)

    pl.semaphore_wait(barrier, 16 + jnp.where(rim_up | rim_down, 1, 0))

    def kv_send(head, part):
        return remote(
            kv_in.at[head, part], kv.at[part, z, y], a2a_s.at[head, part], a2a_r.at[y],
            4 * z + 2 * c + head, 2 * x + part,
        )

    def kv_local(head, part):
        return (2 * c + head == y) & (part == c)

    def q_send(head, k, core):
        goal = z if k == 0 else mate
        return remote(
            q_in.at[head, pl.ds(128 * (2 * core + goal // 2), 128)], q_raw.at[z // 2, y],
            q_s.at[head, k, core], q_r.at[z // 2, y],
            4 * goal + 2 * c + head, 2 * x + core,
        )

    def q_local(head, k, core):
        return (2 * c + head == y) & (core == c) & (k == 0)

    for head in range(2):
        for part in range(2):
            @pl.when(~kv_local(head, part))
            def _(head=head, part=part):
                kv_send(head, part).start()

    lam_send = remote(lam_in, lam.at[c], small_s.at[0], small_r.at[0], s, other)
    lam_send.start()
    near_send = remote(
        bkv_in.at[pl.ds(384, 128)], near.at[pl.ds(0, 128)], small_s.at[1], small_r.at[1],
        jnp.minimum(s + 1, 15), t,
    )

    @pl.when(s < 15)
    def _():
        near_send.start()

    for head in range(2):
        for k in range(2):
            for core in range(2):
                @pl.when(~q_local(head, k, core))
                def _(head=head, k=k, core=core):
                    q_send(head, k, core).start()

    for head in range(2):
        @pl.when(2 * c + head == y)
        def _(head=head):
            kv[c, z, y] = kv_in[head, c]
            q_raw[z // 2, y] = q_in[head, pl.ds(128 * quarter, 128)]

    lam[c] = lam_in[...]

    def half(which):
        return pl.ds(256 * which, 256)

    def z_send(row, which, upward):
        return remote(
            kv.at[c, z, row, half(which)], kv.at[c, z, row, half(which)],
            zs.at[row, which, 0 if upward else 1], zr.at[row, which, 0 if upward else 1],
            4 * (up if upward else down) + y, t,
        )

    def z_wait(row, which, upward):
        level = down if upward else up
        return remote(
            kv.at[c, level, row, half(which)], kv.at[c, level, row, half(which)],
            zs.at[row, which, 0 if upward else 1], zr.at[row, which, 0 if upward else 1],
            4 * (up if upward else down) + y, t,
        )

    def relay_send(row, upward):
        level, which = (down, 0) if upward else (up, 1)
        return remote(
            kv.at[c, level, row, half(which)], kv.at[c, level, row, half(which)],
            rs.at[row, which], rr.at[row, which],
            4 * (up if upward else down) + y, t,
        )

    def relay_wait(row, which):
        return remote(
            kv.at[c, far, row, half(which)], kv.at[c, far, row, half(which)],
            rs.at[row, which], rr.at[row, which],
            4 * (up if which == 0 else down) + y, t,
        )

    def cross_send(level, row):
        return remote(
            kv.at[c, level, row], kv.at[c, level, row],
            ds.at[level, row], dr.at[level, row], s, other,
        )

    def cross_wait(level, row):
        return remote(
            kv.at[1 - c, level, row], kv.at[1 - c, level, row],
            ds.at[level, row], dr.at[level, row], s, other,
        )

    def a2a_wait(row):
        return remote(
            kv.at[c, z, row], kv.at[c, z, row], a2a_s.at[0, 0], a2a_r.at[row], s, other
        )

    def spread(row):
        z_send(row, 0, True).start()
        z_send(row, 1, False).start()
        z_send(row, 1, True).start()
        z_send(row, 0, False).start()
        cross_send(z, row).start()

    @pl.when(y // 2 != c)
    def _():
        a2a_wait(y).wait_recv()

    spread(order[0])
    acc[...] = jnp.zeros_like(acc)
    ls[...] = jnp.zeros_like(ls)
    mx[...] = jnp.full_like(mx, mask_fill)
    near[pl.ds(128, 512)] = bkv_in[...]

    @pl.when(s == 0)
    def _():
        near[pl.ds(0, 128)] = jnp.zeros((128, 128), BF16)

    a2a_wait(order[1]).wait_recv()
    spread(order[1])

    @pl.when(s > 0)
    def _():
        near_send.wait_recv()

    lane = lax.broadcasted_iota(jnp.int32, (1, 128), 1)

    def windowed(block, carry):
        start = pl.multiple_of(block * 128, 128)
        span = near[pl.ds(start, 256)]
        span32 = span.astype(F32)
        turned = jnp.concatenate([span32[:, HEAD_DIM:], span32[:, :HEAD_DIM]], axis=1)
        keys = jnp.where(lane < HEAD_DIM, span32, turned).astype(BF16)
        values = jnp.transpose(span32)[HEAD_DIM:].astype(BF16)
        parts = []
        sinks = []
        for j in range(4):
            own = bq_in[pl.ds(start, 128), 128 * (j // 2) : 128 * (j // 2 + 1)]
            mine = (lane >= HEAD_DIM) if j % 2 else (lane < HEAD_DIM)
            parts.append(jnp.where(mine, own.astype(F32), 0.0).astype(BF16))
            sinks.append(jnp.full((1, 128), sink_in[j] * LOG2E, F32))
        queries = jnp.concatenate(parts, axis=0)
        sink = jnp.concatenate(sinks, axis=1)
        scores = lax.dot_general(keys, queries, NT, preferred_element_type=F32)
        scores = scores * (LOG2E * HEAD_DIM ** (-0.5))
        key_at = lax.broadcasted_iota(jnp.int32, (256, 512), 0)
        query_at = lax.broadcasted_iota(jnp.int32, (256, 512), 1) % 128
        first = jnp.where((s == 0) & (block == 0), 128, 0)
        allowed = (key_at > query_at) & (key_at <= query_at + WINDOW) & (key_at >= first)
        scores = jnp.where(allowed, scores, mask_fill)
        top = jnp.maximum(jnp.max(scores, axis=0, keepdims=True), sink)
        weights = jnp.exp2(scores - top)
        total = jnp.sum(weights, axis=0, keepdims=True) + jnp.exp2(sink - top)
        found = jnp.dot(values, weights.astype(BF16), preferred_element_type=F32) / total
        tall = jnp.concatenate([found[:, 128 * j : 128 * (j + 1)] for j in range(4)], axis=0)
        b_out[pl.ds(start, 128)] = jnp.transpose(tall).astype(BF16)
        return carry

    lax.fori_loop(0, 4, windowed, 0)

    a2a_wait(order[2]).wait_recv()
    spread(order[2])
    a2a_wait(order[3]).wait_recv()
    spread(order[3])

    for pair in range(2):
        for row in range(4):
            @pl.when(~((pair == z // 2) & (row == y) & (y // 2 == c)))
            def _(pair=pair, row=row):
                remote(
                    q_raw.at[pair, row], q_raw.at[pair, row], q_s.at[0, 0, 0],
                    q_r.at[pair, row], s, other,
                ).wait_recv()

    for pair in range(2):
        for row in range(4):
            wide = q_raw[pair, row].astype(F32) * (LOG2E * HEAD_DIM ** (-0.5))
            high = wide.astype(BF16).astype(F32)
            low = wide - high
            for m in range(2):
                mine = (lane >= HEAD_DIM) if m else (lane < HEAD_DIM)
                i = pair * 4 + (row // 2) * 2 + m
                rows = slice(128 * (row % 2), 128 * (row % 2) + 128)
                q_mul[i, rows, 0:128] = jnp.where(mine, high, 0.0).astype(BF16)
                q_mul[i, rows, 128:256] = jnp.where(mine, low, 0.0).astype(BF16)

    def relay(row):
        z_wait(row, 0, True).wait_recv()
        relay_send(row, True).start()
        z_wait(row, 1, False).wait_recv()
        relay_send(row, False).start()
        z_wait(row, 1, True).wait_recv()
        cross_send(down, row).start()
        z_wait(row, 0, False).wait_recv()
        cross_send(up, row).start()

    def relay_far(row):
        relay_wait(row, 0).wait_recv()
        relay_wait(row, 1).wait_recv()
        cross_send(far, row).start()

    def load_pair(level, pair):
        keys = kv[0, level, pl.ds(2 * pair, 2)].reshape(1024, 128)
        held = kv[1, level, pl.ds(2 * pair, 2)].reshape(1024, 128)
        lookup = jnp.concatenate([held[128 * k : 128 * (k + 1)] for k in range(8)], axis=1)
        lookup = jnp.concatenate([lookup, jnp.ones((16, 1024), BF16)], axis=0)
        return jnp.concatenate([keys, keys], axis=1), lookup

    apart = lax.broadcasted_iota(jnp.int32, (256, 256), 0)
    column = lax.broadcasted_iota(jnp.int32, (256, 256), 1)
    apart = apart - (column % 128) - 512 * (column // 128)

    def attend(level, pair, sel):
        mark = jnp.where(sel == 0, jnp.minimum(z, mate), jnp.maximum(z, mate))

        @pl.when(level < mark)
        def _():
            keys, lookup = load_pair(level, pair)

            def score(i):
                return [
                    lax.dot_general(
                        keys[256 * k : 256 * (k + 1)], q_mul[i], NT, preferred_element_type=F32
                    )
                    for k in range(4)
                ]

            soft_chunk([sel * 4 + k for k in range(4)], score, lookup, mx, ls, acc)

        @pl.when(level == mark)
        def _():
            def group(g, carry):
                keys, lookup = load_pair(level, pair)
                base = 1024 * g + 128 * quarter - 1024 * pair

                def score(i):
                    return [
                        jnp.where(
                            apart <= base - 256 * k,
                            lax.dot_general(
                                keys[256 * k : 256 * (k + 1)], q_mul[i], NT,
                                preferred_element_type=F32,
                            ),
                            mask_fill,
                        )
                        for k in range(4)
                    ]

                first = sel * 4 + g * 2
                soft_chunk([first, first + 1], score, lookup, mx, ls, acc)
                return carry

            lax.fori_loop(pair, 2, group, 0)

    def step(it, carry):
        @pl.when((it >= 1) & (it <= 4))
        def _():
            j = it - 1
            row = jnp.where(
                j == 0, order[0], jnp.where(j == 1, order[1], jnp.where(j == 2, order[2], order[3]))
            )
            relay(row)

        @pl.when(it == 5)
        def _():
            relay_far(order[0])
            relay_far(order[1])

        @pl.when(it == 6)
        def _():
            relay_far(order[2])

        @pl.when(it == 7)
        def _():
            relay_far(order[3])

        below = (it == 2) | (it == 4)
        above = (it == 3) | (it == 5)
        level = jnp.where(it < 2, z, jnp.where(below, down, jnp.where(above, up, far)))
        near_pair = (it == 0) | (it == 2) | (it == 3) | (it == 6)
        pair = jnp.where(near_pair, y // 2, 1 - y // 2)
        cross_wait(level, 2 * pair).wait_recv()
        cross_wait(level, 2 * pair + 1).wait_recv()

        def one(sel, inner):
            attend(level, pair, sel)
            return inner

        lax.fori_loop(0, 2, one, 0)
        return carry

    lax.fori_loop(0, 8, step, 0)

    lam_send.wait_recv()
    mixing = lam[y // 2, y % 2, 0:1, :]
    gain = gain_in[...] * head_scale

    def ret_send(pair, row):
        goal = jnp.minimum(z, mate) if pair == 0 else jnp.maximum(z, mate)
        return remote(
            stage.at[pair, row], back.at[y % 2, pl.ds(128 * quarter, 128)],
            ret_s.at[pair, row], ret_r.at[y % 2, quarter],
            4 * goal + row, 2 * x + y // 2,
        )

    def ret_local(pair, row):
        return (pair == z // 2) & (row == y) & (y // 2 == c)

    for pair in range(2):
        for g in range(2):
            i = pair * 4 + g * 2
            first = acc[i] / ls[i]
            second = acc[i + 1] / ls[i + 1]
            gap = first - mixing * second
            square = jnp.mean(gap * gap, axis=0, keepdims=True)
            done = gap * lax.rsqrt(square + norm_eps) * gain
            rows = jnp.transpose(done).astype(BF16)
            for k in range(2):
                row = 2 * g + k
                stage[pair, row] = rows[128 * k : 128 * (k + 1)]

                @pl.when(~ret_local(pair, row))
                def _(pair=pair, row=row):
                    ret_send(pair, row).start()

                @pl.when(ret_local(pair, row))
                def _(pair=pair, row=row):
                    back[y % 2, pl.ds(128 * quarter, 128)] = stage[pair, row]

    for head in range(2):
        for part in range(2):
            @pl.when(~kv_local(head, part))
            def _(head=head, part=part):
                kv_send(head, part).wait_send()
        for k in range(2):
            for core in range(2):
                @pl.when(~q_local(head, k, core))
                def _(head=head, k=k, core=core):
                    q_send(head, k, core).wait_send()
    lam_send.wait_send()

    @pl.when(s < 15)
    def _():
        near_send.wait_send()

    def drain(row, carry):
        for which in range(2):
            for upward in (True, False):
                z_send(row, which, upward).wait_send()
        relay_send(row, True).wait_send()
        relay_send(row, False).wait_send()
        for level in range(4):
            cross_send(level, row).wait_send()
        return carry

    lax.fori_loop(0, 4, drain, 0)
    for head in range(2):
        for part in range(4):
            mine = (2 * c + head == y) & (part == quarter)

            @pl.when(~mine)
            def _(head=head, part=part):
                spot = back.at[head, pl.ds(128 * part, 128)]
                remote(spot, spot, ret_s.at[0, 0], ret_r.at[head, part], s, other).wait_recv()

    a_out[...] = back[...]
    for pair in range(2):
        for row in range(4):
            @pl.when(~ret_local(pair, row))
            def _(pair=pair, row=row):
                ret_send(pair, row).wait_send()


def attention(q_in, kv_in, bq_in, bkv_in, lam_in, gain_in, sink_in):
    vmem = pl.BlockSpec(memory_space=VMEM)
    dma = pltpu.SemaphoreType.DMA
    return pl.pallas_call(
        attention_kernel,
        out_shape=(
            jax.ShapeDtypeStruct((2, 512, 128), BF16),
            jax.ShapeDtypeStruct((512, 256), BF16),
        ),
        in_specs=[vmem] * 6 + [pl.BlockSpec(memory_space=pltpu.SMEM)],
        out_specs=(vmem, vmem),
        scratch_shapes=[
            VMEM((2, 4, 4, 512, 128), BF16),
            VMEM((2, 4, 128, 128), BF16),
            VMEM((8, 256, 256), BF16),
            VMEM((640, 128), BF16),
            VMEM((2, 2, 8, 256), F32),
            VMEM((8, 128, 256), F32),
            VMEM((8, 1, 256), F32),
            VMEM((8, 1, 256), F32),
            VMEM((2, 4, 128, 128), BF16),
            VMEM((2, 512, 128), BF16),
            dma((2, 2)), dma((4,)),
            dma((4, 2, 2)), dma((4, 2, 2)),
            dma((4, 2)), dma((4, 2)),
            dma((4, 4)), dma((4, 4)),
            dma((2, 2, 2)), dma((2, 4)),
            dma((2,)), dma((2,)),
            dma((2, 4)), dma((2, 4)),
        ],
        compiler_params=pltpu.CompilerParams(
            collective_id=1, has_side_effects=True, vmem_limit_bytes=50 * 2**20
        ),
        name="attention",
    )(q_in, kv_in, bq_in, bkv_in, lam_in, gain_in, sink_in)


def shards(
    inputs,
    a_query_w,
    a_key_w,
    a_value_w,
    b_query_w,
    b_key_w,
    b_value_w,
    head_lambda,
    head_gain,
    sink_logit,
    a_out_w,
    b_out_w,
):
    rows = lax.all_gather(inputs, "tp", axis=0, tiled=True)

    def project(matrix):
        return jnp.dot(rows, matrix, preferred_element_type=F32).astype(BF16)

    q = project(a_query_w).reshape(512, 2, 128).transpose(1, 0, 2)
    k = project(a_key_w).reshape(512, 2, 128).transpose(1, 0, 2)
    v = project(a_value_w).reshape(4, 128, 2, 128).transpose(2, 0, 3, 1).reshape(2, 512, 128)
    kv = jnp.stack([k, v], axis=1)
    bq = project(b_query_w)
    bkv = jnp.concatenate([project(b_key_w), project(b_value_w)], axis=1)
    lam = jnp.broadcast_to(head_lambda[:, None, None], (2, 8, 256))
    a_heads, b_heads = attention(q, kv, bq, bkv, lam, head_gain[:, None], sink_logit)
    a_weight = a_out_w.reshape(2, VALUE_DIM, 4096)
    return lax.psum_scatter(
        (
            jnp.einsum("hqe,hen->qn", a_heads, a_weight, preferred_element_type=F32)
            + jnp.dot(b_heads, b_out_w, preferred_element_type=F32)
        ).astype(BF16),
        "tp",
        scatter_dimension=0,
        tiled=True,
    )


def solution(mesh):
    return jax.shard_map(
        shards,
        mesh=mesh,
        in_specs=(
            P(("sp", "tp"), None),
            P(None, "tp"),
            P(None, "tp"),
            P(None, "tp"),
            P(None, "tp"),
            P(None, "tp"),
            P(None, "tp"),
            P("tp"),
            P(),
            P("tp"),
            P("tp", None),
            P("tp", None),
        ),
        out_specs=P(("sp", "tp"), None),
        check_vma=False,
    )
```

```python
import functools

import jax
import jax.numpy as jnp
from jax import lax
from jax.experimental import pallas as pl
from jax.experimental.pallas import tpu as pltpu
from jax.sharding import PartitionSpec as P

HEAD_DIM = 64
VALUE_DIM = 128
WINDOW = 128

norm_eps = 0.0001
head_scale = 0.8
mask_fill = -1e30

MESH = pl.DeviceIdType.MESH
NT = (((1,), (1,)), ((), ()))
LOG2E = 1.4426950408889634
VMEM = pltpu.VMEM
F32 = jnp.float32
BF16 = jnp.bfloat16


def remote(src, dst, send_sem, recv_sem, row, col):
    return pltpu.make_async_remote_copy(
        src_ref=src,
        dst_ref=dst,
        send_sem=send_sem,
        recv_sem=recv_sem,
        device_id=(row, col),
        device_id_type=MESH,
    )


def soft_chunk(items, score, lookup, mx, ls, acc):
    def weights(i, pieces):
        before = mx[i]
        top = before
        for piece in pieces:
            top = jnp.maximum(top, jnp.max(piece, axis=0, keepdims=True))
        shrink = jnp.exp2(before - top)
        mx[i] = top
        return shrink, [jnp.exp2(piece - top).astype(BF16) for piece in pieces]

    def collect(i, shrink, pieces):
        got = jnp.dot(lookup, jnp.concatenate(pieces, axis=0), preferred_element_type=F32)
        acc[i] = acc[i] * shrink + got[:VALUE_DIM]
        ls[i] = ls[i] * shrink + got[VALUE_DIM : VALUE_DIM + 1]

    now = score(items[0])
    held = None
    for at, i in enumerate(items):
        later = score(items[at + 1]) if at + 1 < len(items) else None
        current = weights(i, now)
        if held is not None:
            collect(items[at - 1], *held)
        held, now = current, later
    collect(items[-1], *held)


def attention_kernel(
    q_in, kv_in, bq_in, bkv_in, lam_in, gain_in, sink_in,
    a_out, b_out,
    kv, q_raw, q_mul, near, lam, acc, mx, ls, stage, back,
    a2a_s, a2a_r, zs, zr, rs, rr, ds, dr, q_s, q_r, small_s, small_r, ret_s, ret_r,
):
    s, t = lax.axis_index("sp"), lax.axis_index("tp")
    z, y = s // 4, s % 4
    x, c = t // 2, t % 2
    other = 2 * x + 1 - c
    up, down = (z + 1) % 4, (z + 3) % 4
    far = (z + 2) % 4
    mate = 3 - z
    side = z + 1 - 2 * (z % 2)
    quarter = 2 * c + z // 2
    order = (y, y + 1 - 2 * (y % 2), 3 - y, (y + 2) % 4)

    barrier = pltpu.get_barrier_semaphore()

    def greet(row, col):
        pl.semaphore_signal(barrier, inc=1, device_id=(row, col), device_id_type=MESH)

    for j in range(4):
        for core in range(2):
            if j == 0:
                @pl.when(core != c)
                def _(core=core):
                    greet(4 * z + y, 2 * x + core)
            else:
                greet(4 * z + (y + j) % 4, 2 * x + core)
            greet(4 * mate + (y + j) % 4, 2 * x + core)
    greet(4 * side + y, t)
    rim_up = (y == 3) & (z % 2 == 0)
    rim_down = (y == 0) & (z % 2 == 1)

    @pl.when(rim_up)
    def _():
        greet(s + 1, t)

    @pl.when(rim_down)
    def _():
        greet(s - 1, t)

    pl.semaphore_wait(barrier, 16 + jnp.where(rim_up | rim_down, 1, 0))

    def kv_send(head, part):
        return remote(
            kv_in.at[head, part], kv.at[part, z, y], a2a_s.at[head, part], a2a_r.at[y],
            4 * z + 2 * c + head, 2 * x + part,
        )

    def kv_local(head, part):
        return (2 * c + head == y) & (part == c)

    def q_send(head, k, core):
        goal = z if k == 0 else mate
        return remote(
            q_in.at[head, pl.ds(128 * (2 * core + goal // 2), 128)], q_raw.at[z // 2, y],
            q_s.at[head, k, core], q_r.at[z // 2, y],
            4 * goal + 2 * c + head, 2 * x + core,
        )

    def q_local(head, k, core):
        return (2 * c + head == y) & (core == c) & (k == 0)

    for head in range(2):
        for part in range(2):
            @pl.when(~kv_local(head, part))
            def _(head=head, part=part):
                kv_send(head, part).start()

    lam_send = remote(lam_in, lam.at[c], small_s.at[0], small_r.at[0], s, other)
    lam_send.start()
    near_send = remote(
        bkv_in.at[pl.ds(384, 128)], near.at[pl.ds(0, 128)], small_s.at[1], small_r.at[1],
        jnp.minimum(s + 1, 15), t,
    )

    @pl.when(s < 15)
    def _():
        near_send.start()

    for head in range(2):
        for k in range(2):
            for core in range(2):
                @pl.when(~q_local(head, k, core))
                def _(head=head, k=k, core=core):
                    q_send(head, k, core).start()

    for head in range(2):
        @pl.when(2 * c + head == y)
        def _(head=head):
            kv[c, z, y] = kv_in[head, c]
            q_raw[z // 2, y] = q_in[head, pl.ds(128 * quarter, 128)]

    lam[c] = lam_in[...]

    def half(which):
        return pl.ds(256 * which, 256)

    def z_send(row, which, upward):
        return remote(
            kv.at[c, z, row, half(which)], kv.at[c, z, row, half(which)],
            zs.at[row, which, 0 if upward else 1], zr.at[row, which, 0 if upward else 1],
            4 * (up if upward else down) + y, t,
        )

    def z_wait(row, which, upward):
        level = down if upward else up
        return remote(
            kv.at[c, level, row, half(which)], kv.at[c, level, row, half(which)],
            zs.at[row, which, 0 if upward else 1], zr.at[row, which, 0 if upward else 1],
            4 * (up if upward else down) + y, t,
        )

    def relay_send(row, upward):
        level, which = (down, 0) if upward else (up, 1)
        return remote(
            kv.at[c, level, row, half(which)], kv.at[c, level, row, half(which)],
            rs.at[row, which], rr.at[row, which],
            4 * (up if upward else down) + y, t,
        )

    def relay_wait(row, which):
        return remote(
            kv.at[c, far, row, half(which)], kv.at[c, far, row, half(which)],
            rs.at[row, which], rr.at[row, which],
            4 * (up if which == 0 else down) + y, t,
        )

    def cross_send(level, row):
        return remote(
            kv.at[c, level, row], kv.at[c, level, row],
            ds.at[level, row], dr.at[level, row], s, other,
        )

    def cross_wait(level, row):
        return remote(
            kv.at[1 - c, level, row], kv.at[1 - c, level, row],
            ds.at[level, row], dr.at[level, row], s, other,
        )

    def a2a_wait(row):
        return remote(
            kv.at[c, z, row], kv.at[c, z, row], a2a_s.at[0, 0], a2a_r.at[row], s, other
        )

    def spread(row):
        z_send(row, 0, True).start()
        z_send(row, 1, False).start()
        z_send(row, 1, True).start()
        z_send(row, 0, False).start()
        cross_send(z, row).start()

    @pl.when(y // 2 != c)
    def _():
        a2a_wait(y).wait_recv()

    spread(order[0])
    acc[...] = jnp.zeros_like(acc)
    ls[...] = jnp.zeros_like(ls)
    mx[...] = jnp.full_like(mx, mask_fill)
    near[pl.ds(128, 512)] = bkv_in[...]

    @pl.when(s == 0)
    def _():
        near[pl.ds(0, 128)] = jnp.zeros((128, 128), BF16)

    a2a_wait(order[1]).wait_recv()
    spread(order[1])

    @pl.when(s > 0)
    def _():
        near_send.wait_recv()

    lane = lax.broadcasted_iota(jnp.int32, (1, 128), 1)

    def windowed(block, carry):
        start = pl.multiple_of(block * 128, 128)
        span = near[pl.ds(start, 256)]
        span32 = span.astype(F32)
        turned = jnp.concatenate([span32[:, HEAD_DIM:], span32[:, :HEAD_DIM]], axis=1)
        keys = jnp.where(lane < HEAD_DIM, span32, turned).astype(BF16)
        values = jnp.transpose(span32)[HEAD_DIM:].astype(BF16)
        parts = []
        sinks = []
        for j in range(4):
            own = bq_in[pl.ds(start, 128), 128 * (j // 2) : 128 * (j // 2 + 1)]
            mine = (lane >= HEAD_DIM) if j % 2 else (lane < HEAD_DIM)
            parts.append(jnp.where(mine, own.astype(F32), 0.0).astype(BF16))
            sinks.append(jnp.full((1, 128), sink_in[j] * LOG2E, F32))
        queries = jnp.concatenate(parts, axis=0)
        sink = jnp.concatenate(sinks, axis=1)
        scores = lax.dot_general(keys, queries, NT, preferred_element_type=F32)
        scores = scores * (LOG2E * HEAD_DIM ** (-0.5))
        key_at = lax.broadcasted_iota(jnp.int32, (256, 512), 0)
        query_at = lax.broadcasted_iota(jnp.int32, (256, 512), 1) % 128
        first = jnp.where((s == 0) & (block == 0), 128, 0)
        allowed = (key_at > query_at) & (key_at <= query_at + WINDOW) & (key_at >= first)
        scores = jnp.where(allowed, scores, mask_fill)
        top = jnp.maximum(jnp.max(scores, axis=0, keepdims=True), sink)
        weights = jnp.exp2(scores - top)
        total = jnp.sum(weights, axis=0, keepdims=True) + jnp.exp2(sink - top)
        found = jnp.dot(values, weights.astype(BF16), preferred_element_type=F32) / total
        tall = jnp.concatenate([found[:, 128 * j : 128 * (j + 1)] for j in range(4)], axis=0)
        b_out[pl.ds(start, 128)] = jnp.transpose(tall).astype(BF16)
        return carry

    lax.fori_loop(0, 4, windowed, 0)

    a2a_wait(order[2]).wait_recv()
    spread(order[2])
    a2a_wait(order[3]).wait_recv()
    spread(order[3])

    for pair in range(2):
        for row in range(4):
            @pl.when(~((pair == z // 2) & (row == y) & (y // 2 == c)))
            def _(pair=pair, row=row):
                remote(
                    q_raw.at[pair, row], q_raw.at[pair, row], q_s.at[0, 0, 0],
                    q_r.at[pair, row], s, other,
                ).wait_recv()

    for pair in range(2):
        for row in range(4):
            wide = q_raw[pair, row].astype(F32) * (LOG2E * HEAD_DIM ** (-0.5))
            high = wide.astype(BF16).astype(F32)
            low = wide - high
            for m in range(2):
                mine = (lane >= HEAD_DIM) if m else (lane < HEAD_DIM)
                i = pair * 4 + (row // 2) * 2 + m
                rows = slice(128 * (row % 2), 128 * (row % 2) + 128)
                q_mul[i, rows, 0:128] = jnp.where(mine, high, 0.0).astype(BF16)
                q_mul[i, rows, 128:256] = jnp.where(mine, low, 0.0).astype(BF16)

    def relay(row):
        z_wait(row, 0, True).wait_recv()
        relay_send(row, True).start()
        z_wait(row, 1, False).wait_recv()
        relay_send(row, False).start()
        z_wait(row, 1, True).wait_recv()
        cross_send(down, row).start()
        z_wait(row, 0, False).wait_recv()
        cross_send(up, row).start()

    def relay_far(row):
        relay_wait(row, 0).wait_recv()
        relay_wait(row, 1).wait_recv()
        cross_send(far, row).start()

    def load_pair(level, pair):
        keys = kv[0, level, pl.ds(2 * pair, 2)].reshape(1024, 128)
        held = kv[1, level, pl.ds(2 * pair, 2)].reshape(1024, 128)
        lookup = jnp.concatenate([held[128 * k : 128 * (k + 1)] for k in range(8)], axis=1)
        lookup = jnp.concatenate([lookup, jnp.ones((16, 1024), BF16)], axis=0)
        return jnp.concatenate([keys, keys], axis=1), lookup

    apart = lax.broadcasted_iota(jnp.int32, (256, 256), 0)
    column = lax.broadcasted_iota(jnp.int32, (256, 256), 1)
    apart = apart - (column % 128) - 512 * (column // 128)

    def attend(level, pair, sel):
        mark = jnp.where(sel == 0, jnp.minimum(z, mate), jnp.maximum(z, mate))

        @pl.when(level < mark)
        def _():
            keys, lookup = load_pair(level, pair)

            def score(i):
                return [
                    lax.dot_general(
                        keys[256 * k : 256 * (k + 1)], q_mul[i], NT, preferred_element_type=F32
                    )
                    for k in range(4)
                ]

            soft_chunk([sel * 4 + k for k in range(4)], score, lookup, mx, ls, acc)

        @pl.when(level == mark)
        def _():
            def group(g, carry):
                keys, lookup = load_pair(level, pair)
                base = 1024 * g + 128 * quarter - 1024 * pair

                def score(i):
                    return [
                        jnp.where(
                            apart <= base - 256 * k,
                            lax.dot_general(
                                keys[256 * k : 256 * (k + 1)], q_mul[i], NT,
                                preferred_element_type=F32,
                            ),
                            mask_fill,
                        )
                        for k in range(4)
                    ]

                first = sel * 4 + g * 2
                soft_chunk([first, first + 1], score, lookup, mx, ls, acc)
                return carry

            lax.fori_loop(pair, 2, group, 0)

    def step(it, carry):
        @pl.when((it >= 1) & (it <= 4))
        def _():
            j = it - 1
            row = jnp.where(
                j == 0, order[0], jnp.where(j == 1, order[1], jnp.where(j == 2, order[2], order[3]))
            )
            relay(row)

        @pl.when(it == 5)
        def _():
            relay_far(order[0])
            relay_far(order[1])

        @pl.when(it == 6)
        def _():
            relay_far(order[2])

        @pl.when(it == 7)
        def _():
            relay_far(order[3])

        below = (it == 2) | (it == 4)
        above = (it == 3) | (it == 5)
        level = jnp.where(it < 2, z, jnp.where(below, down, jnp.where(above, up, far)))
        near_pair = (it == 0) | (it == 2) | (it == 3) | (it == 6)
        pair = jnp.where(near_pair, y // 2, 1 - y // 2)
        cross_wait(level, 2 * pair).wait_recv()
        cross_wait(level, 2 * pair + 1).wait_recv()

        def one(sel, inner):
            attend(level, pair, sel)
            return inner

        lax.fori_loop(0, 2, one, 0)
        return carry

    lax.fori_loop(0, 8, step, 0)

    lam_send.wait_recv()
    mixing = lam[y // 2, y % 2, 0:1, :]
    gain = gain_in[...] * head_scale

    def ret_send(pair, row):
        goal = jnp.minimum(z, mate) if pair == 0 else jnp.maximum(z, mate)
        return remote(
            stage.at[pair, row], back.at[y % 2, pl.ds(128 * quarter, 128)],
            ret_s.at[pair, row], ret_r.at[y % 2, quarter],
            4 * goal + row, 2 * x + y // 2,
        )

    def ret_local(pair, row):
        return (pair == z // 2) & (row == y) & (y // 2 == c)

    for pair in range(2):
        for g in range(2):
            i = pair * 4 + g * 2
            first = acc[i] / ls[i]
            second = acc[i + 1] / ls[i + 1]
            gap = first - mixing * second
            square = jnp.mean(gap * gap, axis=0, keepdims=True)
            done = gap * lax.rsqrt(square + norm_eps) * gain
            rows = jnp.transpose(done).astype(BF16)
            for k in range(2):
                row = 2 * g + k
                stage[pair, row] = rows[128 * k : 128 * (k + 1)]

                @pl.when(~ret_local(pair, row))
                def _(pair=pair, row=row):
                    ret_send(pair, row).start()

                @pl.when(ret_local(pair, row))
                def _(pair=pair, row=row):
                    back[y % 2, pl.ds(128 * quarter, 128)] = stage[pair, row]

    for head in range(2):
        for part in range(2):
            @pl.when(~kv_local(head, part))
            def _(head=head, part=part):
                kv_send(head, part).wait_send()
        for k in range(2):
            for core in range(2):
                @pl.when(~q_local(head, k, core))
                def _(head=head, k=k, core=core):
                    q_send(head, k, core).wait_send()
    lam_send.wait_send()

    @pl.when(s < 15)
    def _():
        near_send.wait_send()

    def drain(row, carry):
        for which in range(2):
            for upward in (True, False):
                z_send(row, which, upward).wait_send()
        relay_send(row, True).wait_send()
        relay_send(row, False).wait_send()
        for level in range(4):
            cross_send(level, row).wait_send()
        return carry

    lax.fori_loop(0, 4, drain, 0)
    for head in range(2):
        for part in range(4):
            mine = (2 * c + head == y) & (part == quarter)

            @pl.when(~mine)
            def _(head=head, part=part):
                spot = back.at[head, pl.ds(128 * part, 128)]
                remote(spot, spot, ret_s.at[0, 0], ret_r.at[head, part], s, other).wait_recv()

    a_out[...] = back[...]
    for pair in range(2):
        for row in range(4):
            @pl.when(~ret_local(pair, row))
            def _(pair=pair, row=row):
                ret_send(pair, row).wait_send()


def attention(q_in, kv_in, bq_in, bkv_in, lam_in, gain_in, sink_in):
    vmem = pl.BlockSpec(memory_space=VMEM)
    dma = pltpu.SemaphoreType.DMA
    return pl.pallas_call(
        attention_kernel,
        out_shape=(
            jax.ShapeDtypeStruct((2, 512, 128), BF16),
            jax.ShapeDtypeStruct((512, 256), BF16),
        ),
        in_specs=[vmem] * 6 + [pl.BlockSpec(memory_space=pltpu.SMEM)],
        out_specs=(vmem, vmem),
        scratch_shapes=[
            VMEM((2, 4, 4, 512, 128), BF16),
            VMEM((2, 4, 128, 128), BF16),
            VMEM((8, 256, 256), BF16),
            VMEM((640, 128), BF16),
            VMEM((2, 2, 8, 256), F32),
            VMEM((8, 128, 256), F32),
            VMEM((8, 1, 256), F32),
            VMEM((8, 1, 256), F32),
            VMEM((2, 4, 128, 128), BF16),
            VMEM((2, 512, 128), BF16),
            dma((2, 2)), dma((4,)),
            dma((4, 2, 2)), dma((4, 2, 2)),
            dma((4, 2)), dma((4, 2)),
            dma((4, 4)), dma((4, 4)),
            dma((2, 2, 2)), dma((2, 4)),
            dma((2,)), dma((2,)),
            dma((2, 4)), dma((2, 4)),
        ],
        compiler_params=pltpu.CompilerParams(
            collective_id=1, has_side_effects=True, vmem_limit_bytes=50 * 2**20
        ),
        name="attention",
    )(q_in, kv_in, bq_in, bkv_in, lam_in, gain_in, sink_in)


NC = 8
CW = 512


def output_kernel(
    a_in, b_in, aw_in, bw_in, out,
    weights, part, crossed, chip, far_l, far_r, got_l, got_r, relayed,
    w_s, cr_s, cr_r, fs, fr, gs, gr,
):
    s, t = lax.axis_index("sp"), lax.axis_index("tp")
    x, c = t // 2, t % 2
    xr, xl, xf = (x + 1) % 4, (x + 3) % 4, (x + 2) % 4
    other, right, left = 2 * x + 1 - c, 2 * xr + c, 2 * xl + c

    def fetch(n, which):
        columns = pl.ds(pl.multiple_of(n * CW, CW), CW)
        source = aw_in if which == 0 else bw_in
        return pltpu.make_async_copy(
            source.at[:, columns], weights.at[n, pl.ds(256 * which, 256)], w_s.at[n, which]
        )

    for n in range(NC):
        fetch(n, 0).start()
        fetch(n, 1).start()
    barrier = pltpu.get_barrier_semaphore()
    for col in (other, right, left):
        pl.semaphore_signal(barrier, inc=1, device_id=(s, col), device_id_type=MESH)
    pl.semaphore_wait(barrier, 3)

    heads = jnp.concatenate([a_in[0], a_in[1], b_in[...]], axis=1)
    first, second = pl.ds(0, 32), pl.ds(32, 32)

    def cross(n):
        return remote(part.at[n, 1 - c], crossed.at[n], cr_s.at[n], cr_r.at[n], s, other)

    def far_send(n, way):
        rows = first if way == 0 else second
        return remote(
            chip.at[n, xf, rows], (far_l if way == 0 else far_r).at[n],
            fs.at[n, way], fr.at[n, way], s, right if way == 0 else left,
        )

    def near_send(n, way):
        rows = second if way == 0 else first
        return remote(
            chip.at[n, xr if way == 0 else xl, rows], (got_l if way == 0 else got_r).at[n, rows],
            gs.at[n, way, 0], gr.at[n, way, 0], s, right if way == 0 else left,
        )

    def sum_send(n, way):
        rows = first if way == 0 else second
        return remote(
            relayed.at[n, way], (got_l if way == 0 else got_r).at[n, rows],
            gs.at[n, way, 1], gr.at[n, way, 1], s, right if way == 0 else left,
        )

    def multiply(n):
        fetch(n, 0).wait()
        fetch(n, 1).wait()
        partial = jnp.dot(heads, weights[n], preferred_element_type=F32).astype(BF16)
        for col in range(8):
            part[n, col % 2, col // 2] = partial[64 * col : 64 * (col + 1)]
        cross(n).start()

    def join(n):
        cross(n).wait_recv()
        chip[n] = (part[n, c].astype(F32) + crossed[n].astype(F32)).astype(BF16)
        far_send(n, 0).start()
        far_send(n, 1).start()
        near_send(n, 0).start()
        near_send(n, 1).start()

    def pass_on(n, carry):
        far_send(n, 0).wait_recv()
        relayed[n, 0] = (chip[n, xr, first].astype(F32) + far_l[n].astype(F32)).astype(BF16)
        sum_send(n, 0).start()
        far_send(n, 1).wait_recv()
        relayed[n, 1] = (chip[n, xl, second].astype(F32) + far_r[n].astype(F32)).astype(BF16)
        sum_send(n, 1).start()
        return carry

    multiply(0)

    def run(n, carry):
        multiply(n)
        join(n - 1)
        return carry

    lax.fori_loop(1, NC, run, 0)
    join(NC - 1)
    lax.fori_loop(0, NC, pass_on, 0)

    for n in range(NC):
        for way in range(2):
            near_send(n, way).wait_recv()
            sum_send(n, way).wait_recv()
        total = chip[n, x].astype(F32) + got_l[n].astype(F32) + got_r[n].astype(F32)
        out[:, n * CW : (n + 1) * CW] = total.astype(BF16)

    def drain(n, carry):
        cross(n).wait_send()
        for way in range(2):
            far_send(n, way).wait_send()
            near_send(n, way).wait_send()
            sum_send(n, way).wait_send()
        return carry

    lax.fori_loop(0, NC, drain, 0)


def output(a_heads, b_heads, a_out_w, b_out_w):
    vmem = pl.BlockSpec(memory_space=VMEM)
    hbm = pl.BlockSpec(memory_space=pl.ANY)
    dma = pltpu.SemaphoreType.DMA
    return pl.pallas_call(
        output_kernel,
        out_shape=jax.ShapeDtypeStruct((64, 4096), BF16),
        in_specs=[vmem, vmem, hbm, hbm],
        out_specs=vmem,
        scratch_shapes=[
            VMEM((NC, 512, CW), BF16),
            VMEM((NC, 2, 4, 64, CW), BF16),
            VMEM((NC, 4, 64, CW), BF16),
            VMEM((NC, 4, 64, CW), BF16),
            VMEM((NC, 32, CW), BF16),
            VMEM((NC, 32, CW), BF16),
            VMEM((NC, 64, CW), BF16),
            VMEM((NC, 64, CW), BF16),
            VMEM((NC, 2, 32, CW), BF16),
            dma((NC, 2)), dma((NC,)), dma((NC,)),
            dma((NC, 2)), dma((NC, 2)), dma((NC, 2, 2)), dma((NC, 2, 2)),
        ],
        compiler_params=pltpu.CompilerParams(
            collective_id=2, has_side_effects=True, vmem_limit_bytes=50 * 2**20
        ),
        name="output",
    )(a_heads, b_heads, a_out_w, b_out_w)


KC = 4
KW = 1024
WIDTHS = (256, 256, 256, 256, 64, 64)


def project_kernel(
    x_in, w0, w1, w2, w3, w4, w5, q_out, kv_out, bq_out, bkv_out,
    rows, m0, m1, m2, m3, m4, m5, t0, t1, t2, t3, t4, t5,
    w_s, os, orr, rs, rr, ds, dr,
):
    s, t = lax.axis_index("sp"), lax.axis_index("tp")
    x, c = t // 2, t % 2
    xr, xl, xf = (x + 1) % 4, (x + 3) % 4, (x + 2) % 4
    other, right, left = 2 * x + 1 - c, 2 * xr + c, 2 * xl + c
    beyond = 2 * xf + c
    sources = (w0, w1, w2, w3, w4, w5)
    mats = (m0, m1, m2, m3, m4, m5)
    sums = (t0, t1, t2, t3, t4, t5)

    def fetch(k, i):
        return pltpu.make_async_copy(
            sources[i].at[pl.ds(pl.multiple_of(k * KW, KW), KW)], mats[i].at[k], w_s.at[k, i]
        )

    for k in range(KC):
        for i in range(6):
            fetch(k, i).start()
    barrier = pltpu.get_barrier_semaphore()
    for col in (other, right, left):
        pl.semaphore_signal(barrier, inc=1, device_id=(s, col), device_id_type=MESH)
    pl.semaphore_wait(barrier, 3)

    halves = (pl.ds(0, 32), pl.ds(32, 32))

    def columns(k):
        return pl.ds(pl.multiple_of(k * KW, KW), KW)

    def own_send(k, way, which):
        return remote(
            x_in.at[halves[which], columns(k)], rows.at[k, t, halves[which]],
            os.at[k, way, which], orr.at[k, way, which], s, right if way == 0 else left,
        )

    def own_wait(k, way, which):
        spot = rows.at[k, left if way == 0 else right, halves[which]]
        return remote(
            spot, spot, os.at[k, way, which], orr.at[k, way, which],
            s, right if way == 0 else left,
        )

    def relay_send(k, way):
        spot = rows.at[k, left if way == 0 else right, halves[way]]
        return remote(
            spot, spot, rs.at[k, way], rr.at[k, way], s, right if way == 0 else left
        )

    def relay_wait(k, way):
        spot = rows.at[k, beyond, halves[way]]
        return remote(
            spot, spot, rs.at[k, way], rr.at[k, way], s, right if way == 0 else left
        )

    def own_cross(k):
        return remote(
            x_in.at[:, columns(k)], rows.at[k, t], ds.at[k, x], dr.at[k, x], s, other
        )

    def cross(k, chip):
        spot = rows.at[k, 2 * chip + c]
        return remote(spot, spot, ds.at[k, chip], dr.at[k, chip], s, other)

    def cross_wait(k, chip):
        spot = rows.at[k, 2 * chip + 1 - c]
        return remote(spot, spot, ds.at[k, chip], dr.at[k, chip], s, other)

    for k in range(KC):
        own_send(k, 0, 0).start()
        own_send(k, 1, 1).start()
        own_send(k, 0, 1).start()
        own_send(k, 1, 0).start()
        own_cross(k).start()
    for k in range(KC):
        rows[k, t] = x_in[:, k * KW : (k + 1) * KW]
    for total in sums:
        total[...] = jnp.zeros_like(total)

    def pass_on(k, carry):
        own_wait(k, 0, 0).wait_recv()
        relay_send(k, 0).start()
        own_wait(k, 1, 1).wait_recv()
        relay_send(k, 1).start()
        own_wait(k, 0, 1).wait_recv()
        cross(k, xl).start()
        own_wait(k, 1, 0).wait_recv()
        cross(k, xr).start()
        return carry

    lax.fori_loop(0, KC, pass_on, 0)

    def multiply(k, carry):
        relay_wait(k, 0).wait_recv()
        relay_wait(k, 1).wait_recv()
        cross(k, xf).start()
        for i in range(6):
            fetch(k, i).wait()
        for chip in (x, xl, xr, xf):
            cross_wait(k, chip).wait_recv()
        block = rows[k].reshape(512, KW)
        for i in range(6):
            sums[i][...] += jnp.dot(block, mats[i][k], preferred_element_type=F32)
        return carry

    lax.fori_loop(0, KC, multiply, 0)

    for head in range(2):
        lanes = slice(128 * head, 128 * (head + 1))
        q_out[head] = t0[:, lanes].astype(BF16)
        kv_out[head, 0] = t1[:, lanes].astype(BF16)
        for j in range(4):
            turned = jnp.transpose(t2[128 * j : 128 * (j + 1), lanes])
            kv_out[head, 1, 128 * j : 128 * (j + 1)] = turned.astype(BF16)
    bq_out[...] = t3[...].astype(BF16)
    bkv_out[...] = jnp.concatenate([t4[...], t5[...]], axis=1).astype(BF16)

    def drain(k, carry):
        for way in range(2):
            own_send(k, way, 0).wait_send()
            own_send(k, way, 1).wait_send()
            relay_send(k, way).wait_send()
        own_cross(k).wait_send()
        for chip in (xl, xr, xf):
            cross(k, chip).wait_send()
        return carry

    lax.fori_loop(0, KC, drain, 0)


def project(inputs, *matrices):
    vmem = pl.BlockSpec(memory_space=VMEM)
    hbm = pl.BlockSpec(memory_space=pl.ANY)
    dma = pltpu.SemaphoreType.DMA
    return pl.pallas_call(
        project_kernel,
        out_shape=(
            jax.ShapeDtypeStruct((2, 512, 128), BF16),
            jax.ShapeDtypeStruct((2, 2, 512, 128), BF16),
            jax.ShapeDtypeStruct((512, 256), BF16),
            jax.ShapeDtypeStruct((512, 128), BF16),
        ),
        in_specs=[vmem] + [hbm] * 6,
        out_specs=(vmem,) * 4,
        scratch_shapes=[VMEM((KC, 8, 64, KW), BF16)]
        + [VMEM((KC, KW, width), BF16) for width in WIDTHS]
        + [VMEM((512, width), F32) for width in WIDTHS]
        + [
            dma((KC, 6)),
            dma((KC, 2, 2)), dma((KC, 2, 2)), dma((KC, 2)), dma((KC, 2)),
            dma((KC, 4)), dma((KC, 4)),
        ],
        compiler_params=pltpu.CompilerParams(
            collective_id=0, has_side_effects=True, vmem_limit_bytes=50 * 2**20
        ),
        name="project",
    )(inputs, *matrices)


def shards(
    inputs,
    a_query_w,
    a_key_w,
    a_value_w,
    b_query_w,
    b_key_w,
    b_value_w,
    head_lambda,
    head_gain,
    sink_logit,
    a_out_w,
    b_out_w,
):
    q, kv, bq, bkv = project(
        inputs, a_query_w, a_key_w, a_value_w, b_query_w, b_key_w, b_value_w
    )
    lam = jnp.broadcast_to(head_lambda[:, None, None], (2, 8, 256))
    a_heads, b_heads = attention(q, kv, bq, bkv, lam, head_gain[:, None], sink_logit)
    return output(a_heads, b_heads, a_out_w, b_out_w)


def solution(mesh):
    return jax.shard_map(
        shards,
        mesh=mesh,
        in_specs=(
            P(("sp", "tp"), None),
            P(None, "tp"),
            P(None, "tp"),
            P(None, "tp"),
            P(None, "tp"),
            P(None, "tp"),
            P(None, "tp"),
            P("tp"),
            P(),
            P("tp"),
            P("tp", None),
            P("tp", None),
        ),
        out_specs=P(("sp", "tp"), None),
        check_vma=False,
    )
```

```python
import functools

import jax
import jax.numpy as jnp
from jax import lax
from jax.experimental import pallas as pl
from jax.experimental.pallas import tpu as pltpu
from jax.sharding import PartitionSpec as P

HEAD_DIM = 64
VALUE_DIM = 128
WINDOW = 128

norm_eps = 0.0001
head_scale = 0.8
mask_fill = -1e30

MESH = pl.DeviceIdType.MESH
NT = (((1,), (1,)), ((), ()))
LOG2E = 1.4426950408889634
VMEM = pltpu.VMEM
F32 = jnp.float32
BF16 = jnp.bfloat16


def remote(src, dst, send_sem, recv_sem, row, col):
    return pltpu.make_async_remote_copy(
        src_ref=src,
        dst_ref=dst,
        send_sem=send_sem,
        recv_sem=recv_sem,
        device_id=(row, col),
        device_id_type=MESH,
    )


def soft_chunk(items, score, lookup, mx, ls, acc):
    def weights(i, pieces):
        before = mx[i]
        top = before
        for piece in pieces:
            top = jnp.maximum(top, jnp.max(piece, axis=0, keepdims=True))
        shrink = jnp.exp2(before - top)
        mx[i] = top
        return shrink, [jnp.exp2(piece - top).astype(BF16) for piece in pieces]

    def collect(i, shrink, pieces):
        got = jnp.dot(lookup, jnp.concatenate(pieces, axis=0), preferred_element_type=F32)
        acc[i] = acc[i] * shrink + got[:VALUE_DIM]
        ls[i] = ls[i] * shrink + got[VALUE_DIM : VALUE_DIM + 1]

    now = score(items[0])
    held = None
    for at, i in enumerate(items):
        later = score(items[at + 1]) if at + 1 < len(items) else None
        current = weights(i, now)
        if held is not None:
            collect(items[at - 1], *held)
        held, now = current, later
    collect(items[-1], *held)


NC = 8
CW = 512
GROUPS = 4


def layer_kernel(
    x_in, wq_in, wk_in, wv_in, wbq_in, wbk_in, wbv_in, lam_in, gain_in, sink_in, aw_in, bw_in,
    out,
    rows, wq, wk, wv, wbq, wbkv, q_own, kv_own, bq_own,
    kv, q_raw, q_mul, near, lam, acc, mx, ls, stage, back, b_heads,
    weights, part, crossed, chip, far_l, far_r, got_l, got_r, relayed,
    pw_s, os, orr, xs, xr_s, xds, xdr,
    a2a_s, a2a_r, zs, zr, rs, rr, ds, dr, q_s, q_r, small_s, small_r, ret_s, ret_r,
    w_s, cr_s, cr_r, fs, fr, gs, gr,
):
    s, t = lax.axis_index("sp"), lax.axis_index("tp")
    z, y = s // 4, s % 4
    x, c = t // 2, t % 2
    xr, xl, xf = (x + 1) % 4, (x + 3) % 4, (x + 2) % 4
    other, right, left = 2 * x + 1 - c, 2 * xr + c, 2 * xl + c
    beyond = 2 * xf + c
    up, down = (z + 1) % 4, (z + 3) % 4
    far = (z + 2) % 4
    mate = 3 - z
    side = z + 1 - 2 * (z % 2)
    quarter = 2 * c + z // 2
    lane = lax.broadcasted_iota(jnp.int32, (1, 128), 1)

    loads = [
        pltpu.make_async_copy(wk_in, wk, pw_s.at[0]),
        pltpu.make_async_copy(wv_in, wv, pw_s.at[1]),
        pltpu.make_async_copy(wq_in, wq, pw_s.at[2]),
        pltpu.make_async_copy(wbq_in, wbq, pw_s.at[3]),
        pltpu.make_async_copy(wbk_in, wbkv.at[pl.ds(0, 64)], pw_s.at[4]),
        pltpu.make_async_copy(wbv_in, wbkv.at[pl.ds(64, 64)], pw_s.at[5]),
    ]
    for load in loads:
        load.start()

    def fetch(n, which):
        columns = pl.ds(pl.multiple_of(n * CW, CW), CW)
        source = aw_in if which == 0 else bw_in
        return pltpu.make_async_copy(
            source.at[:, columns], weights.at[n, pl.ds(256 * which, 256)], w_s.at[n, which]
        )

    for n in range(NC):
        fetch(n, 0).start()
        fetch(n, 1).start()

    barrier = pltpu.get_barrier_semaphore()

    def greet(row, col):
        pl.semaphore_signal(barrier, inc=1, device_id=(row, col), device_id_type=MESH)

    for j in range(4):
        for core in range(2):
            if j == 0:
                @pl.when(core != c)
                def _(core=core):
                    greet(4 * z + y, 2 * x + core)
            else:
                greet(4 * z + (y + j) % 4, 2 * x + core)
            greet(4 * mate + (y + j) % 4, 2 * x + core)
    greet(4 * side + y, t)
    greet(s, right)
    greet(s, left)
    rim_up = (y == 3) & (z % 2 == 0)
    rim_down = (y == 0) & (z % 2 == 1)

    @pl.when(rim_up)
    def _():
        greet(s + 1, t)

    @pl.when(rim_down)
    def _():
        greet(s - 1, t)

    pl.semaphore_wait(barrier, 18 + jnp.where(rim_up | rim_down, 1, 0))

    halves = (pl.ds(0, 2048), pl.ds(2048, 2048))
    every = pl.ds(0, 16)

    def mine16(g):
        return pl.ds(pl.multiple_of(16 * g, 16), 16)

    def own_send(g, way, which):
        return remote(
            x_in.at[mine16(g), halves[which]], rows.at[g, t, every, halves[which]],
            os.at[g, way, which], orr.at[g, way, which], s, right if way == 0 else left,
        )

    def own_wait(g, way, which):
        spot = rows.at[g, left if way == 0 else right, every, halves[which]]
        return remote(
            spot, spot, os.at[g, way, which], orr.at[g, way, which],
            s, right if way == 0 else left,
        )

    def xrelay_send(g, way):
        spot = rows.at[g, left if way == 0 else right, every, halves[way]]
        return remote(
            spot, spot, xs.at[g, way], xr_s.at[g, way], s, right if way == 0 else left
        )

    def xrelay_wait(g, way):
        spot = rows.at[g, beyond, every, halves[way]]
        return remote(
            spot, spot, xs.at[g, way], xr_s.at[g, way], s, right if way == 0 else left
        )

    def own_cross(g):
        return remote(x_in.at[mine16(g)], rows.at[g, t], xds.at[g, x], xdr.at[g, x], s, other)

    def xcross(g, where):
        spot = rows.at[g, 2 * where + c]
        return remote(spot, spot, xds.at[g, where], xdr.at[g, where], s, other)

    def xcross_wait(g, where):
        spot = rows.at[g, 2 * where + 1 - c]
        return remote(spot, spot, xds.at[g, where], xdr.at[g, where], s, other)

    def own_start(g):
        own_send(g, 0, 0).start()
        own_send(g, 1, 1).start()
        own_send(g, 0, 1).start()
        own_send(g, 1, 0).start()
        own_cross(g).start()

    def kv_send(g, head, part_of):
        return remote(
            kv_own.at[head, part_of, g], kv.at[part_of, z, g, y],
            a2a_s.at[g, head, part_of], a2a_r.at[g, y],
            4 * z + 2 * c + head, 2 * x + part_of,
        )

    def kv_local(head, part_of):
        return (2 * c + head == y) & (part_of == c)

    def a2a_wait(g, row):
        spot = kv.at[c, z, g, row]
        return remote(spot, spot, a2a_s.at[0, 0, 0], a2a_r.at[g, row], s, other)

    def z_send(g, way):
        spot = kv.at[c, z, g]
        return remote(spot, spot, zs.at[g, way], zr.at[g, way], 4 * (up, down)[way] + y, t)

    def z_wait(g, way):
        spot = kv.at[c, (down, up)[way], g]
        return remote(spot, spot, zs.at[g, way], zr.at[g, way], 4 * (up, down)[way] + y, t)

    def relay_send(g, way):
        spot = kv.at[c, (down, up)[way], g, pl.ds(2 * way, 2)]
        return remote(spot, spot, rs.at[g, way], rr.at[g, way], 4 * (up, down)[way] + y, t)

    def relay_wait(g, way):
        spot = kv.at[c, far, g, pl.ds(2 * way, 2)]
        return remote(spot, spot, rs.at[g, way], rr.at[g, way], 4 * (up, down)[way] + y, t)

    def cross_send(level, g):
        spot = kv.at[c, level, g]
        return remote(spot, spot, ds.at[level, g], dr.at[level, g], s, other)

    def cross_wait(level, g):
        spot = kv.at[1 - c, level, g]
        return remote(spot, spot, ds.at[level, g], dr.at[level, g], s, other)

    def spread(g):
        for j in range(4):
            row = (y + j) % 4
            if j == 0:
                @pl.when(y // 2 != c)
                def _():
                    a2a_wait(g, y).wait_recv()
            else:
                a2a_wait(g, row).wait_recv()
        z_send(g, 0).start()
        z_send(g, 1).start()
        cross_send(z, g).start()

    def zrelay(g):
        z_wait(g, 0).wait_recv()
        relay_send(g, 0).start()
        cross_send(down, g).start()
        z_wait(g, 1).wait_recv()
        relay_send(g, 1).start()
        cross_send(up, g).start()

    def zfar(g):
        relay_wait(g, 0).wait_recv()
        relay_wait(g, 1).wait_recv()
        cross_send(far, g).start()

    own_start(0)
    own_start(1)
    lam_send = remote(lam_in, lam.at[c], small_s.at[0], small_r.at[0], s, other)
    lam_send.start()
    for g in range(GROUPS):
        rows[g, t] = x_in[16 * g : 16 * (g + 1)]
    lam[c] = lam_in[...]
    acc[...] = jnp.zeros_like(acc)
    ls[...] = jnp.zeros_like(ls)
    mx[...] = jnp.full_like(mx, mask_fill)

    @pl.when(s == 0)
    def _():
        near[pl.ds(0, 128)] = jnp.zeros((128, 128), BF16)

    def gather(g, carry):
        own_wait(g, 0, 0).wait_recv()
        xrelay_send(g, 0).start()
        own_wait(g, 1, 1).wait_recv()
        xrelay_send(g, 1).start()

        @pl.when(g < GROUPS - 2)
        def _():
            own_start(g + 2)

        own_wait(g, 0, 1).wait_recv()
        xcross(g, xl).start()
        own_wait(g, 1, 0).wait_recv()
        xcross(g, xr).start()

        @pl.when(g >= 1)
        def _():
            spread(g - 1)

        @pl.when(g >= 2)
        def _():
            zrelay(g - 2)

        xrelay_wait(g, 0).wait_recv()
        xrelay_wait(g, 1).wait_recv()
        xcross(g, xf).start()

        @pl.when(g == 0)
        def _():
            for load in loads[:2]:
                load.wait()

        for where in (x, xl, xr, xf):
            xcross_wait(g, where).wait_recv()
        block = rows[g].reshape(128, 4096)
        keys = jnp.dot(block, wk[...], preferred_element_type=F32)
        values = jnp.dot(block, wv[...], preferred_element_type=F32)
        for head in range(2):
            lanes = slice(128 * head, 128 * (head + 1))
            kv_own[head, 0, g] = keys[:, lanes].astype(BF16)
            kv_own[head, 1, g] = jnp.transpose(values[:, lanes]).astype(BF16)

            @pl.when(2 * c + head == y)
            def _(head=head):
                kv[c, z, g, y] = kv_own[head, c, g]

            for part_of in range(2):
                @pl.when(~kv_local(head, part_of))
                def _(head=head, part_of=part_of):
                    kv_send(g, head, part_of).start()

        @pl.when(g == 0)
        def _():
            for load in loads[2:]:
                load.wait()

        queries = jnp.dot(block, wq[...], preferred_element_type=F32).astype(BF16)
        b_queries = jnp.dot(block, wbq[...], preferred_element_type=F32).astype(BF16)
        b_pair = lax.dot_general(block, wbkv[...], NT, preferred_element_type=F32).astype(BF16)
        for d in range(8):
            spot = pl.ds(pl.multiple_of(64 * d + 16 * g, 16), 16)
            take = slice(16 * d, 16 * (d + 1))
            q_own[0, spot] = queries[take, :128]
            q_own[1, spot] = queries[take, 128:]
            bq_own[spot] = b_queries[take]
            near[pl.ds(pl.multiple_of(128 + 64 * d + 16 * g, 16), 16)] = b_pair[take]
        return carry

    lax.fori_loop(0, GROUPS, gather, 0)

    def q_send(head, k, core):
        goal = z if k == 0 else mate
        return remote(
            q_own.at[head, pl.ds(128 * (2 * core + goal // 2), 128)], q_raw.at[z // 2, y],
            q_s.at[head, k, core], q_r.at[z // 2, y],
            4 * goal + 2 * c + head, 2 * x + core,
        )

    def q_local(head, k, core):
        return (2 * c + head == y) & (core == c) & (k == 0)

    for head in range(2):
        for k in range(2):
            for core in range(2):
                @pl.when(~q_local(head, k, core))
                def _(head=head, k=k, core=core):
                    q_send(head, k, core).start()

        @pl.when(2 * c + head == y)
        def _(head=head):
            q_raw[z // 2, y] = q_own[head, pl.ds(128 * quarter, 128)]

    rim_send = remote(
        near.at[pl.ds(512, 128)], near.at[pl.ds(0, 128)], small_s.at[1], small_r.at[1],
        jnp.minimum(s + 1, 15), t,
    )

    @pl.when(s < 15)
    def _():
        rim_send.start()

    spread(3)
    zrelay(2)
    zfar(0)
    zfar(1)

    @pl.when(s > 0)
    def _():
        rim_send.wait_recv()

    def windowed(block, carry):
        start = pl.multiple_of(block * 128, 128)
        span = near[pl.ds(start, 256)]
        span32 = span.astype(F32)
        turned = jnp.concatenate([span32[:, HEAD_DIM:], span32[:, :HEAD_DIM]], axis=1)
        keys = jnp.where(lane < HEAD_DIM, span32, turned).astype(BF16)
        values = jnp.transpose(span32)[HEAD_DIM:].astype(BF16)
        parts = []
        sinks = []
        for j in range(4):
            own = bq_own[pl.ds(start, 128), 128 * (j // 2) : 128 * (j // 2 + 1)]
            mine = (lane >= HEAD_DIM) if j % 2 else (lane < HEAD_DIM)
            parts.append(jnp.where(mine, own.astype(F32), 0.0).astype(BF16))
            sinks.append(jnp.full((1, 128), sink_in[j] * LOG2E, F32))
        queries = jnp.concatenate(parts, axis=0)
        sink = jnp.concatenate(sinks, axis=1)
        scores = lax.dot_general(keys, queries, NT, preferred_element_type=F32)
        scores = scores * (LOG2E * HEAD_DIM ** (-0.5))
        key_at = lax.broadcasted_iota(jnp.int32, (256, 512), 0)
        query_at = lax.broadcasted_iota(jnp.int32, (256, 512), 1) % 128
        first = jnp.where((s == 0) & (block == 0), 128, 0)
        allowed = (key_at > query_at) & (key_at <= query_at + WINDOW) & (key_at >= first)
        scores = jnp.where(allowed, scores, mask_fill)
        top = jnp.maximum(jnp.max(scores, axis=0, keepdims=True), sink)
        weights = jnp.exp2(scores - top)
        total = jnp.sum(weights, axis=0, keepdims=True) + jnp.exp2(sink - top)
        found = jnp.dot(values, weights.astype(BF16), preferred_element_type=F32) / total
        tall = jnp.concatenate([found[:, 128 * j : 128 * (j + 1)] for j in range(4)], axis=0)
        b_heads[pl.ds(start, 128)] = jnp.transpose(tall).astype(BF16)
        return carry

    lax.fori_loop(0, 4, windowed, 0)

    for pair in range(2):
        for row in range(4):
            @pl.when(~((pair == z // 2) & (row == y) & (y // 2 == c)))
            def _(pair=pair, row=row):
                remote(
                    q_raw.at[pair, row], q_raw.at[pair, row], q_s.at[0, 0, 0],
                    q_r.at[pair, row], s, other,
                ).wait_recv()

    for pair in range(2):
        for row in range(4):
            wide = q_raw[pair, row].astype(F32) * (LOG2E * HEAD_DIM ** (-0.5))
            high = wide.astype(BF16).astype(F32)
            low = wide - high
            for m in range(2):
                mine = (lane >= HEAD_DIM) if m else (lane < HEAD_DIM)
                i = pair * 4 + (row // 2) * 2 + m
                span = slice(128 * (row % 2), 128 * (row % 2) + 128)
                q_mul[i, span, 0:128] = jnp.where(mine, high, 0.0).astype(BF16)
                q_mul[i, span, 128:256] = jnp.where(mine, low, 0.0).astype(BF16)

    def unit(level, pair):
        keys = kv[0, level, pl.ds(2 * pair, 2)].reshape(1024, 128)
        held = kv[1, level, pl.ds(2 * pair, 2)].reshape(1024, 128)
        lookup = jnp.concatenate([held[128 * k : 128 * (k + 1)] for k in range(8)], axis=1)
        lookup = jnp.concatenate([lookup, jnp.ones((16, 1024), BF16)], axis=0)
        return jnp.concatenate([keys, keys], axis=1), lookup

    def small_unit(level, pair, two):
        rows_of = (pl.ds(2 * pair, 2), pl.ds(2 * two, 2))
        keys = kv[0, level, rows_of[0], rows_of[1]].reshape(512, 128)
        held = kv[1, level, rows_of[0], rows_of[1]].reshape(512, 128)
        lookup = jnp.concatenate([held[128 * k : 128 * (k + 1)] for k in range(4)], axis=1)
        lookup = jnp.concatenate([lookup, jnp.ones((16, 512), BF16)], axis=0)
        return jnp.concatenate([keys, keys], axis=1), lookup

    key_at = lax.broadcasted_iota(jnp.int32, (256, 256), 0)
    query_at = lax.broadcasted_iota(jnp.int32, (256, 256), 1)
    apart = 512 * (key_at // 128) + 64 * ((key_at % 128) // 16) + key_at % 16
    apart = apart - (query_at % 128) - 512 * (query_at // 128)

    def attend(level, pair, sel):
        mark = jnp.where(sel == 0, jnp.minimum(z, mate), jnp.maximum(z, mate))

        @pl.when(level < mark)
        def _():
            keys, lookup = unit(level, pair)

            def score(i):
                return [
                    lax.dot_general(
                        keys[256 * k : 256 * (k + 1)], q_mul[i], NT, preferred_element_type=F32
                    )
                    for k in range(4)
                ]

            soft_chunk([sel * 4 + k for k in range(4)], score, lookup, mx, ls, acc)

        @pl.when(level == mark)
        def _():
            def group(at, carry):
                g = jnp.minimum(at, 1)
                two = at // 2
                keys, lookup = small_unit(level, pair, two)
                base = 1024 * (g - two) + 128 * quarter - 32 * pair

                def score(i):
                    return [
                        jnp.where(
                            apart <= base - 16 * k,
                            lax.dot_general(
                                keys[256 * k : 256 * (k + 1)], q_mul[i], NT,
                                preferred_element_type=F32,
                            ),
                            mask_fill,
                        )
                        for k in range(2)
                    ]

                first = sel * 4 + g * 2
                soft_chunk([first, first + 1], score, lookup, mx, ls, acc)
                return carry

            lax.fori_loop(0, 3, group, 0)

    def step(it, carry):
        @pl.when(it == 2)
        def _():
            zfar(2)

        @pl.when(it == 3)
        def _():
            zrelay(3)

        @pl.when(it == 6)
        def _():
            zfar(3)

        level = jnp.where(
            (it == 0) | (it == 3), z,
            jnp.where((it == 1) | (it == 5), down, jnp.where((it == 2) | (it == 6), up, far)),
        )
        pair = jnp.where((it == 3) | (it >= 5), 1, 0)
        cross_wait(level, 2 * pair).wait_recv()
        cross_wait(level, 2 * pair + 1).wait_recv()

        def one(sel, inner):
            attend(level, pair, sel)
            return inner

        lax.fori_loop(0, 2, one, 0)
        return carry

    lax.fori_loop(0, 8, step, 0)

    lam_send.wait_recv()
    mixing = lam[y // 2, y % 2, 0:1, :]
    gain = gain_in[...] * head_scale

    def ret_send(pair, row):
        goal = jnp.minimum(z, mate) if pair == 0 else jnp.maximum(z, mate)
        return remote(
            stage.at[pair, row], back.at[y % 2, pl.ds(128 * quarter, 128)],
            ret_s.at[pair, row], ret_r.at[y % 2, quarter],
            4 * goal + row, 2 * x + y // 2,
        )

    def ret_local(pair, row):
        return (pair == z // 2) & (row == y) & (y // 2 == c)

    for pair in range(2):
        for g in range(2):
            i = pair * 4 + g * 2
            first_mean = acc[i] / ls[i]
            second_mean = acc[i + 1] / ls[i + 1]
            gap = first_mean - mixing * second_mean
            square = jnp.mean(gap * gap, axis=0, keepdims=True)
            done = gap * lax.rsqrt(square + norm_eps) * gain
            tall = jnp.transpose(done).astype(BF16)
            for k in range(2):
                row = 2 * g + k
                stage[pair, row] = tall[128 * k : 128 * (k + 1)]

                @pl.when(~ret_local(pair, row))
                def _(pair=pair, row=row):
                    ret_send(pair, row).start()

                @pl.when(ret_local(pair, row))
                def _(pair=pair, row=row):
                    back[y % 2, pl.ds(128 * quarter, 128)] = stage[pair, row]

    for head in range(2):
        for k in range(4):
            mine = (2 * c + head == y) & (k == quarter)

            @pl.when(~mine)
            def _(head=head, k=k):
                spot = back.at[head, pl.ds(128 * k, 128)]
                remote(spot, spot, ret_s.at[0, 0], ret_r.at[head, k], s, other).wait_recv()

    heads = jnp.concatenate([back[0], back[1], b_heads[...]], axis=1)
    first, second = pl.ds(0, 32), pl.ds(32, 32)

    def cross(n):
        return remote(part.at[n, 1 - c], crossed.at[n], cr_s.at[n], cr_r.at[n], s, other)

    def far_send(n, way):
        rows = first if way == 0 else second
        return remote(
            chip.at[n, xf, rows], (far_l if way == 0 else far_r).at[n],
            fs.at[n, way], fr.at[n, way], s, right if way == 0 else left,
        )

    def near_send(n, way):
        rows = second if way == 0 else first
        return remote(
            chip.at[n, xr if way == 0 else xl, rows], (got_l if way == 0 else got_r).at[n, rows],
            gs.at[n, way, 0], gr.at[n, way, 0], s, right if way == 0 else left,
        )

    def sum_send(n, way):
        rows = first if way == 0 else second
        return remote(
            relayed.at[n, way], (got_l if way == 0 else got_r).at[n, rows],
            gs.at[n, way, 1], gr.at[n, way, 1], s, right if way == 0 else left,
        )

    def multiply(n):
        fetch(n, 0).wait()
        fetch(n, 1).wait()
        partial = jnp.dot(heads, weights[n], preferred_element_type=F32).astype(BF16)
        for col in range(8):
            part[n, col % 2, col // 2] = partial[64 * col : 64 * (col + 1)]
        cross(n).start()

    def join(n):
        cross(n).wait_recv()
        chip[n] = (part[n, c].astype(F32) + crossed[n].astype(F32)).astype(BF16)
        far_send(n, 0).start()
        far_send(n, 1).start()
        near_send(n, 0).start()
        near_send(n, 1).start()

    def pass_on(n, carry):
        far_send(n, 0).wait_recv()
        relayed[n, 0] = (chip[n, xr, first].astype(F32) + far_l[n].astype(F32)).astype(BF16)
        sum_send(n, 0).start()
        far_send(n, 1).wait_recv()
        relayed[n, 1] = (chip[n, xl, second].astype(F32) + far_r[n].astype(F32)).astype(BF16)
        sum_send(n, 1).start()
        return carry

    multiply(0)

    def run(n, carry):
        multiply(n)
        join(n - 1)
        return carry

    lax.fori_loop(1, NC, run, 0)
    join(NC - 1)
    lax.fori_loop(0, NC, pass_on, 0)

    for n in range(NC):
        for way in range(2):
            near_send(n, way).wait_recv()
            sum_send(n, way).wait_recv()
        total = chip[n, x].astype(F32) + got_l[n].astype(F32) + got_r[n].astype(F32)
        out[:, n * CW : (n + 1) * CW] = total.astype(BF16)

    def drain(n, carry):
        cross(n).wait_send()
        for way in range(2):
            far_send(n, way).wait_send()
            near_send(n, way).wait_send()
            sum_send(n, way).wait_send()
        return carry

    lax.fori_loop(0, NC, drain, 0)

    for g in range(GROUPS):
        for head in range(2):
            for part_of in range(2):
                @pl.when(~kv_local(head, part_of))
                def _(g=g, head=head, part_of=part_of):
                    kv_send(g, head, part_of).wait_send()
    for head in range(2):
        for k in range(2):
            for core in range(2):
                @pl.when(~q_local(head, k, core))
                def _(head=head, k=k, core=core):
                    q_send(head, k, core).wait_send()
    lam_send.wait_send()

    @pl.when(s < 15)
    def _():
        rim_send.wait_send()

    def drain_rows(g, carry):
        for way in range(2):
            own_send(g, way, 0).wait_send()
            own_send(g, way, 1).wait_send()
            xrelay_send(g, way).wait_send()
            z_send(g, way).wait_send()
            relay_send(g, way).wait_send()
        own_cross(g).wait_send()
        for where in (xl, xr, xf):
            xcross(g, where).wait_send()
        for level in range(4):
            cross_send(level, g).wait_send()
        return carry

    lax.fori_loop(0, GROUPS, drain_rows, 0)
    for pair in range(2):
        for row in range(4):
            @pl.when(~ret_local(pair, row))
            def _(pair=pair, row=row):
                ret_send(pair, row).wait_send()


def layer(*operands):
    vmem = pl.BlockSpec(memory_space=VMEM)
    hbm = pl.BlockSpec(memory_space=pl.ANY)
    dma = pltpu.SemaphoreType.DMA
    return pl.pallas_call(
        layer_kernel,
        out_shape=jax.ShapeDtypeStruct((64, 4096), BF16),
        in_specs=[vmem] + [hbm] * 6 + [vmem, vmem, pl.BlockSpec(memory_space=pltpu.SMEM)] + [hbm] * 2,
        out_specs=vmem,
        scratch_shapes=[
            VMEM((4, 8, 16, 4096), BF16),
            VMEM((4096, 256), BF16), VMEM((4096, 256), BF16),
            VMEM((4096, 256), BF16), VMEM((4096, 256), BF16), VMEM((128, 4096), BF16),
            VMEM((2, 512, 128), BF16), VMEM((2, 2, 4, 128, 128), BF16), VMEM((512, 256), BF16),
            VMEM((2, 4, 4, 4, 128, 128), BF16),
            VMEM((2, 4, 128, 128), BF16),
            VMEM((8, 256, 256), BF16),
            VMEM((640, 128), BF16),
            VMEM((2, 2, 8, 256), F32),
            VMEM((8, 128, 256), F32),
            VMEM((8, 1, 256), F32),
            VMEM((8, 1, 256), F32),
            VMEM((2, 4, 128, 128), BF16),
            VMEM((2, 512, 128), BF16),
            VMEM((512, 256), BF16),
            VMEM((NC, 512, CW), BF16),
            VMEM((NC, 2, 4, 64, CW), BF16),
            VMEM((NC, 4, 64, CW), BF16),
            VMEM((NC, 4, 64, CW), BF16),
            VMEM((NC, 32, CW), BF16),
            VMEM((NC, 32, CW), BF16),
            VMEM((NC, 64, CW), BF16),
            VMEM((NC, 64, CW), BF16),
            VMEM((NC, 2, 32, CW), BF16),
            dma((6,)), dma((4, 2, 2)), dma((4, 2, 2)), dma((4, 2)), dma((4, 2)),
            dma((4, 4)), dma((4, 4)),
            dma((4, 2, 2)), dma((4, 4)),
            dma((4, 2)), dma((4, 2)),
            dma((4, 2)), dma((4, 2)),
            dma((4, 4)), dma((4, 4)),
            dma((2, 2, 2)), dma((2, 4)),
            dma((2,)), dma((2,)),
            dma((2, 4)), dma((2, 4)),
            dma((NC, 2)), dma((NC,)), dma((NC,)),
            dma((NC, 2)), dma((NC, 2)), dma((NC, 2, 2)), dma((NC, 2, 2)),
        ],
        compiler_params=pltpu.CompilerParams(
            collective_id=0, has_side_effects=True, vmem_limit_bytes=58 * 2**20
        ),
        name="layer",
    )(*operands)


def shards(
    inputs,
    a_query_w,
    a_key_w,
    a_value_w,
    b_query_w,
    b_key_w,
    b_value_w,
    head_lambda,
    head_gain,
    sink_logit,
    a_out_w,
    b_out_w,
):
    lam = jnp.broadcast_to(head_lambda[:, None, None], (2, 8, 256))
    return layer(
        inputs, a_query_w, a_key_w, a_value_w, b_query_w, b_key_w.T, b_value_w.T,
        lam, head_gain[:, None], sink_logit, a_out_w, b_out_w,
    )


def solution(mesh):
    return jax.shard_map(
        shards,
        mesh=mesh,
        in_specs=(
            P(("sp", "tp"), None),
            P(None, "tp"),
            P(None, "tp"),
            P(None, "tp"),
            P(None, "tp"),
            P(None, "tp"),
            P(None, "tp"),
            P("tp"),
            P(),
            P("tp"),
            P("tp", None),
            P("tp", None),
        ),
        out_specs=P(("sp", "tp"), None),
        check_vma=False,
    )
```

```python
import functools

import jax
import jax.numpy as jnp
from jax import lax
from jax.experimental import pallas as pl
from jax.experimental.pallas import tpu as pltpu
from jax.sharding import PartitionSpec as P

HEAD_DIM = 64
VALUE_DIM = 128
WINDOW = 128

norm_eps = 0.0001
head_scale = 0.8
mask_fill = -1e30

MESH = pl.DeviceIdType.MESH
NT = (((1,), (1,)), ((), ()))
LOG2E = 1.4426950408889634
VMEM = pltpu.VMEM
F32 = jnp.float32
BF16 = jnp.bfloat16


def remote(src, dst, send_sem, recv_sem, row, col):
    return pltpu.make_async_remote_copy(
        src_ref=src,
        dst_ref=dst,
        send_sem=send_sem,
        recv_sem=recv_sem,
        device_id=(row, col),
        device_id_type=MESH,
    )


def soft_chunk(items, score, lookup, mx, ls, acc):
    def weights(i, pieces):
        before = mx[i]
        top = before
        for piece in pieces:
            top = jnp.maximum(top, jnp.max(piece, axis=0, keepdims=True))
        shrink = jnp.exp2(before - top)
        mx[i] = top
        return shrink, [jnp.exp2(piece - top).astype(BF16) for piece in pieces]

    def collect(i, shrink, pieces):
        got = jnp.dot(lookup, jnp.concatenate(pieces, axis=0), preferred_element_type=F32)
        acc[i] = acc[i] * shrink + got[:VALUE_DIM]
        ls[i] = ls[i] * shrink + got[VALUE_DIM : VALUE_DIM + 1]

    now = score(items[0])
    held = None
    for at, i in enumerate(items):
        later = score(items[at + 1]) if at + 1 < len(items) else None
        current = weights(i, now)
        if held is not None:
            collect(items[at - 1], *held)
        held, now = current, later
    collect(items[-1], *held)


NC = 8
CW = 512
GROUPS = 4


def layer_kernel(
    x_hbm, wq_in, wk_in, wv_in, wbq_in, wbk_in, wbv_in, lam_in, gain_in, sink_in, aw_in, bw_in,
    out,
    x_in, rows, wq, wk, wv, wbq, wbkv, q_own, kv_own, bq_own,
    kv, q_raw, q_mul, near, lam, acc, mx, ls, stage, back, b_heads,
    weights, part, crossed, chip, far_l, far_r, got_l, got_r, relayed,
    x_s, pw_s, os, orr, xs, xr_s, xds, xdr,
    a2a_s, a2a_r, zs, zr, rs, rr, ds, dr, q_s, q_r, small_s, small_r, ret_s, ret_r,
    w_s, cr_s, cr_r, fs, fr, gs, ss, gr,
):
    s, t = lax.axis_index("sp"), lax.axis_index("tp")
    z, y = s // 4, s % 4
    x, c = t // 2, t % 2
    xr, xl, xf = (x + 1) % 4, (x + 3) % 4, (x + 2) % 4
    other, right, left = 2 * x + 1 - c, 2 * xr + c, 2 * xl + c
    beyond = 2 * xf + c
    up, down = (z + 1) % 4, (z + 3) % 4
    far = (z + 2) % 4
    mate = 3 - z
    side = z + 1 - 2 * (z % 2)
    quarter = 2 * c + z // 2
    lane = lax.broadcasted_iota(jnp.int32, (1, 128), 1)

    x_load = pltpu.make_async_copy(x_hbm, x_in, x_s)
    x_load.start()
    mixed = y // 2 == c
    loads = [
        pltpu.make_async_copy(wq_in, wq, pw_s.at[2]),
        pltpu.make_async_copy(wk_in, wk, pw_s.at[0]),
        pltpu.make_async_copy(wv_in, wv, pw_s.at[1]),
        pltpu.make_async_copy(wbq_in, wbq, pw_s.at[3]),
        pltpu.make_async_copy(wbk_in, wbkv.at[pl.ds(0, 64)], pw_s.at[4]),
        pltpu.make_async_copy(wbv_in, wbkv.at[pl.ds(64, 64)], pw_s.at[5]),
    ]

    def fetch(n, which):
        columns = pl.ds(pl.multiple_of(n * CW, CW), CW)
        source = aw_in if which == 0 else bw_in
        return pltpu.make_async_copy(
            source.at[:, columns], weights.at[n, pl.ds(256 * which, 256)], w_s
        )

    barrier = pltpu.get_barrier_semaphore()

    def greet(row, col):
        pl.semaphore_signal(barrier, inc=1, device_id=(row, col), device_id_type=MESH)

    for j in range(4):
        for core in range(2):
            if j == 0:
                @pl.when(core != c)
                def _(core=core):
                    greet(4 * z + y, 2 * x + core)
            else:
                greet(4 * z + (y + j) % 4, 2 * x + core)
            greet(4 * mate + (y + j) % 4, 2 * x + core)
    greet(4 * side + y, t)
    greet(s, right)
    greet(s, left)
    rim_up = (y == 3) & (z % 2 == 0)
    rim_down = (y == 0) & (z % 2 == 1)

    @pl.when(rim_up)
    def _():
        greet(s + 1, t)

    @pl.when(rim_down)
    def _():
        greet(s - 1, t)

    x_load.wait()
    for load in loads:
        load.start()
    pl.semaphore_wait(barrier, 18 + jnp.where(rim_up | rim_down, 1, 0))

    halves = (pl.ds(0, 2048), pl.ds(2048, 2048))
    every = pl.ds(0, 16)

    def mine16(g):
        return pl.ds(pl.multiple_of(16 * g, 16), 16)

    def own_send(g, way, which):
        return remote(
            x_in.at[mine16(g), halves[which]], rows.at[g, t, every, halves[which]],
            os, orr.at[g, way, which], s, right if way == 0 else left,
        )

    def own_wait(g, way, which):
        spot = rows.at[g, left if way == 0 else right, every, halves[which]]
        return remote(
            spot, spot, os, orr.at[g, way, which],
            s, right if way == 0 else left,
        )

    def xrelay_send(g, way):
        spot = rows.at[g, left if way == 0 else right, every, halves[way]]
        return remote(spot, spot, xs, xr_s.at[g], s, right if way == 0 else left)

    def xrelay_wait(g):
        spot = rows.at[g, beyond]
        return remote(spot, spot, xs, xr_s.at[g], s, right)

    def own_cross(g):
        return remote(x_in.at[mine16(g)], rows.at[g, t], xds, xdr.at[g], s, other)

    def xcross(g, where):
        spot = rows.at[g, 2 * where + c]
        return remote(spot, spot, xds, xdr.at[g], s, other)

    def xcross_wait(g):
        spot = rows.at[g, pl.ds(0, 4)]
        return remote(spot, spot, xds, xdr.at[g], s, other)

    def own_start(g):
        own_send(g, 0, 0).start()
        own_send(g, 1, 1).start()
        own_send(g, 0, 1).start()
        own_send(g, 1, 0).start()
        own_cross(g).start()

    def kv_send(g, head, part_of):
        return remote(
            kv_own.at[head, part_of, g], kv.at[part_of, z, g, y],
            a2a_s, a2a_r.at[g],
            4 * z + 2 * c + head, 2 * x + part_of,
        )

    def kv_local(head, part_of):
        return (2 * c + head == y) & (part_of == c)

    def a2a_wait(g, count):
        spot = kv.at[c, z, g, pl.ds(0, count)]
        return remote(spot, spot, a2a_s, a2a_r.at[g], s, other)

    def z_send(g, way):
        spot = kv.at[c, z, g]
        return remote(spot, spot, zs, zr.at[g, way], 4 * (up, down)[way] + y, t)

    def z_wait(g, way):
        spot = kv.at[c, (down, up)[way], g]
        return remote(spot, spot, zs, zr.at[g, way], 4 * (up, down)[way] + y, t)

    def relay_send(g, way):
        spot = kv.at[c, (down, up)[way], g, pl.ds(2 * way, 2)]
        return remote(spot, spot, rs, rr.at[g], 4 * (up, down)[way] + y, t)

    def relay_wait(g):
        spot = kv.at[c, far, g]
        return remote(spot, spot, rs, rr.at[g], 4 * up + y, t)

    def cross_send(level, g):
        spot = kv.at[c, level, g]
        return remote(spot, spot, ds, dr.at[level, g // 2], s, other)

    def cross_wait(level, pair):
        spot = kv.at[1 - c, level, pl.ds(2 * pair, 2)]
        return remote(spot, spot, ds, dr.at[level, pair], s, other)

    def spread(g):
        @pl.when(mixed)
        def _():
            a2a_wait(g, 3).wait_recv()

        @pl.when(~mixed)
        def _():
            a2a_wait(g, 4).wait_recv()

        z_send(g, 0).start()
        z_send(g, 1).start()
        cross_send(z, g).start()

    def zrelay(g):
        z_wait(g, 0).wait_recv()
        relay_send(g, 0).start()
        cross_send(down, g).start()
        z_wait(g, 1).wait_recv()
        relay_send(g, 1).start()
        cross_send(up, g).start()

    def zfar(g):
        relay_wait(g).wait_recv()
        cross_send(far, g).start()

    own_start(0)
    own_start(1)
    lam_send = remote(lam.at[c], lam.at[c], small_s.at[0], small_r.at[0], s, other)
    for g in range(GROUPS):
        rows[g, t] = x_in[16 * g : 16 * (g + 1)]
    for head in range(2):
        lam[c, head] = jnp.full((8, 256), lam_in[head], F32)
    acc[...] = jnp.zeros_like(acc)
    ls[...] = jnp.zeros_like(ls)
    mx[...] = jnp.full_like(mx, mask_fill)

    @pl.when(s == 0)
    def _():
        near[pl.ds(0, 128)] = jnp.zeros((128, 128), BF16)

    def near_rows(g):
        own_wait(g, 0, 0).wait_recv()
        xrelay_send(g, 0).start()
        own_wait(g, 1, 1).wait_recv()
        xrelay_send(g, 1).start()

        @pl.when(g < GROUPS - 2)
        def _():
            own_start(g + 2)

        own_wait(g, 0, 1).wait_recv()
        xcross(g, xl).start()
        own_wait(g, 1, 0).wait_recv()
        xcross(g, xr).start()

    near_rows(0)

    def gather(g, carry):
        @pl.when(g < GROUPS - 1)
        def _():
            near_rows(g + 1)

        xrelay_wait(g).wait_recv()
        xcross(g, xf).start()

        @pl.when(g >= 2)
        def _():
            spread(g - 2)

        @pl.when(g == 0)
        def _():
            for load in loads[:3]:
                load.wait()

        xcross_wait(g).wait_recv()
        block = rows[g].reshape(128, 4096)
        queries = jnp.dot(block, wq[...], preferred_element_type=F32).astype(BF16)
        q_own[0, g] = queries[:, :128]
        q_own[1, g] = queries[:, 128:]
        send_queries(g)
        keys = jnp.dot(block, wk[...], preferred_element_type=F32)
        values = jnp.dot(block, wv[...], preferred_element_type=F32)
        for head in range(2):
            lanes = slice(128 * head, 128 * (head + 1))
            kv_own[head, 0, g] = keys[:, lanes].astype(BF16)
            kv_own[head, 1, g] = jnp.transpose(values[:, lanes]).astype(BF16)

            @pl.when(2 * c + head == y)
            def _(head=head):
                kv[c, z, g, y] = kv_own[head, c, g]

            for part_of in range(2):
                @pl.when(~kv_local(head, part_of))
                def _(head=head, part_of=part_of):
                    kv_send(g, head, part_of).start()

        @pl.when(g == 0)
        def _():
            for load in loads[3:]:
                load.wait()
            for n in range(NC):
                fetch(n, 0).start()
                fetch(n, 1).start()

        @pl.when(g == GROUPS - 1)
        def _():
            spread(2)

        b_queries = jnp.dot(block, wbq[...], preferred_element_type=F32).astype(BF16)
        b_pair = lax.dot_general(block, wbkv[...], NT, preferred_element_type=F32).astype(BF16)
        for d in range(8):
            spot = pl.ds(pl.multiple_of(64 * d + 16 * g, 16), 16)
            take = slice(16 * d, 16 * (d + 1))
            bq_own[spot] = b_queries[take]
            near[pl.ds(pl.multiple_of(128 + 64 * d + 16 * g, 16), 16)] = b_pair[take]
        return carry

    def q_send(g, head, k, core):
        goal = z if k == 0 else mate
        return remote(
            q_own.at[head, g, pl.ds(32 * (2 * core + goal // 2), 32)],
            q_raw.at[4 * (z // 2) + y, g], q_s, q_r,
            4 * goal + 2 * c + head, 2 * x + core,
        )

    def q_local(head, k, core):
        return (2 * c + head == y) & (core == c) & (k == 0)

    def send_queries(g):
        for head in range(2):
            for k in range(2):
                for core in range(2):
                    @pl.when(~q_local(head, k, core))
                    def _(head=head, k=k, core=core):
                        q_send(g, head, k, core).start()

            @pl.when(2 * c + head == y)
            def _(head=head):
                q_raw[4 * (z // 2) + y, g] = q_own[head, g, pl.ds(32 * quarter, 32)]

    def q_all(count):
        spot = q_raw.at[pl.ds(0, count)]
        return remote(spot, spot, q_s, q_r, s, other)

    lam_send.start()
    lax.fori_loop(0, GROUPS, gather, 0)

    rim_send = remote(
        near.at[pl.ds(512, 128)], near.at[pl.ds(0, 128)], small_s.at[1], small_r.at[1],
        jnp.minimum(s + 1, 15), t,
    )

    @pl.when(s < 15)
    def _():
        rim_send.start()

    zrelay(0)
    zrelay(1)


    def windowed(block, carry):
        start = pl.multiple_of(block * 128, 128)
        span = near[pl.ds(start, 256)]
        span32 = span.astype(F32)
        turned = jnp.concatenate([span32[:, HEAD_DIM:], span32[:, :HEAD_DIM]], axis=1)
        keys = jnp.where(lane < HEAD_DIM, span32, turned).astype(BF16)
        values = jnp.transpose(span32)[HEAD_DIM:].astype(BF16)
        parts = []
        sinks = []
        for j in range(4):
            own = bq_own[pl.ds(start, 128), 128 * (j // 2) : 128 * (j // 2 + 1)]
            mine = (lane >= HEAD_DIM) if j % 2 else (lane < HEAD_DIM)
            parts.append(jnp.where(mine, own.astype(F32), 0.0).astype(BF16))
            sinks.append(jnp.full((1, 128), sink_in[j] * LOG2E, F32))
        queries = jnp.concatenate(parts, axis=0)
        sink = jnp.concatenate(sinks, axis=1)
        scores = lax.dot_general(keys, queries, NT, preferred_element_type=F32)
        scores = scores * (LOG2E * HEAD_DIM ** (-0.5))
        key_at = lax.broadcasted_iota(jnp.int32, (256, 512), 0)
        query_at = lax.broadcasted_iota(jnp.int32, (256, 512), 1) % 128
        first = jnp.where((s == 0) & (block == 0), 128, 0)
        allowed = (key_at > query_at) & (key_at <= query_at + WINDOW) & (key_at >= first)
        scores = jnp.where(allowed, scores, mask_fill)
        top = jnp.maximum(jnp.max(scores, axis=0, keepdims=True), sink)
        weights = jnp.exp2(scores - top)
        total = jnp.sum(weights, axis=0, keepdims=True) + jnp.exp2(sink - top)
        found = jnp.dot(values, weights.astype(BF16), preferred_element_type=F32) / total
        tall = jnp.concatenate([found[:, 128 * j : 128 * (j + 1)] for j in range(4)], axis=0)
        b_heads[pl.ds(start, 128)] = jnp.transpose(tall).astype(BF16)
        return carry

    lax.fori_loop(1, 4, windowed, 0)

    spread(3)
    @pl.when(mixed)
    def _():
        q_all(7).wait_recv()

    @pl.when(~mixed)
    def _():
        q_all(8).wait_recv()

    for pair in range(2):
        for row in range(4):
            raw = q_raw[4 * pair + row].astype(F32)
            raw = jnp.concatenate(
                [raw[g, 16 * d : 16 * (d + 1)] for d in range(2) for g in range(4)], axis=0
            )
            wide = raw * (LOG2E * HEAD_DIM ** (-0.5))
            high = wide.astype(BF16).astype(F32)
            low = wide - high
            for m in range(2):
                mine = (lane >= HEAD_DIM) if m else (lane < HEAD_DIM)
                i = pair * 4 + (row // 2) * 2 + m
                span = slice(128 * (row % 2), 128 * (row % 2) + 128)
                q_mul[i, span, 0:128] = jnp.where(mine, high, 0.0).astype(BF16)
                q_mul[i, span, 128:256] = jnp.where(mine, low, 0.0).astype(BF16)

    def unit(level, pair):
        keys = kv[0, level, pl.ds(2 * pair, 2)].reshape(1024, 128)
        held = kv[1, level, pl.ds(2 * pair, 2)].reshape(1024, 128)
        lookup = jnp.concatenate([held[128 * k : 128 * (k + 1)] for k in range(8)], axis=1)
        lookup = jnp.concatenate([lookup, jnp.ones((16, 1024), BF16)], axis=0)
        return jnp.concatenate([keys, keys], axis=1), lookup

    def small_unit(level, pair, two):
        rows_of = (pl.ds(2 * pair, 2), pl.ds(2 * two, 2))
        keys = kv[0, level, rows_of[0], rows_of[1]].reshape(512, 128)
        held = kv[1, level, rows_of[0], rows_of[1]].reshape(512, 128)
        lookup = jnp.concatenate([held[128 * k : 128 * (k + 1)] for k in range(4)], axis=1)
        lookup = jnp.concatenate([lookup, jnp.ones((16, 512), BF16)], axis=0)
        return jnp.concatenate([keys, keys], axis=1), lookup

    key_at = lax.broadcasted_iota(jnp.int32, (256, 256), 0)
    query_at = lax.broadcasted_iota(jnp.int32, (256, 256), 1)
    apart = 512 * (key_at // 128) + 64 * ((key_at % 128) // 16) + key_at % 16
    apart = apart - (query_at % 128) - 512 * (query_at // 128)

    def attend(level, pair, sel):
        mark = jnp.where(sel == 0, jnp.minimum(z, mate), jnp.maximum(z, mate))

        @pl.when(level < mark)
        def _():
            keys, lookup = unit(level, pair)

            def score(i):
                return [
                    lax.dot_general(
                        keys[256 * k : 256 * (k + 1)], q_mul[i], NT, preferred_element_type=F32
                    )
                    for k in range(4)
                ]

            soft_chunk([sel * 4 + k for k in range(4)], score, lookup, mx, ls, acc)

        @pl.when(level == mark)
        def _():
            def group(at, carry):
                g = jnp.minimum(at, 1)
                two = at // 2
                keys, lookup = small_unit(level, pair, two)
                base = 1024 * (g - two) + 128 * quarter - 32 * pair

                def score(i):
                    return [
                        jnp.where(
                            apart <= base - 16 * k,
                            lax.dot_general(
                                keys[256 * k : 256 * (k + 1)], q_mul[i], NT,
                                preferred_element_type=F32,
                            ),
                            mask_fill,
                        )
                        for k in range(2)
                    ]

                first = sel * 4 + g * 2
                soft_chunk([first, first + 1], score, lookup, mx, ls, acc)
                return carry

            lax.fori_loop(0, 3, group, 0)

    def step(it, carry):
        @pl.when(it == 1)
        def _():
            zfar(0)

        @pl.when(it == 2)
        def _():
            zfar(1)
            zrelay(2)

        @pl.when(it == 3)
        def _():
            @pl.when(s > 0)
            def _():
                rim_send.wait_recv()

            windowed(0, 0)

        @pl.when(it == 4)
        def _():
            zrelay(3)
            zfar(2)

        @pl.when(it == 6)
        def _():
            zfar(3)

        turn = it % 4
        level = jnp.where(
            turn == 0, z, jnp.where(turn == 1, down, jnp.where(turn == 2, up, far))
        )
        pair = it // 4
        cross_wait(level, pair).wait_recv()

        def one(sel, inner):
            attend(level, pair, sel)
            return inner

        lax.fori_loop(0, 2, one, 0)
        return carry

    lax.fori_loop(0, 8, step, 0)

    lam_send.wait_recv()
    mixing = lam[y // 2, y % 2, 0:1, :]
    gain = gain_in[...] * head_scale

    def ret_send(pair, row):
        goal = jnp.minimum(z, mate) if pair == 0 else jnp.maximum(z, mate)
        return remote(
            stage.at[4 * pair + row], back.at[4 * (y % 2) + quarter], ret_s, ret_r,
            4 * goal + row, 2 * x + y // 2,
        )

    def ret_local(pair, row):
        return (pair == z // 2) & (row == y) & (y // 2 == c)

    for pair in range(2):
        for g in range(2):
            i = pair * 4 + g * 2
            first_mean = acc[i] / ls[i]
            second_mean = acc[i + 1] / ls[i + 1]
            gap = first_mean - mixing * second_mean
            square = jnp.mean(gap * gap, axis=0, keepdims=True)
            done = gap * lax.rsqrt(square + norm_eps)
            tall = (jnp.transpose(done) * gain).astype(BF16)
            for k in range(2):
                row = 2 * g + k
                stage[4 * pair + row] = tall[128 * k : 128 * (k + 1)]

                @pl.when(~ret_local(pair, row))
                def _(pair=pair, row=row):
                    ret_send(pair, row).start()

                @pl.when(ret_local(pair, row))
                def _(pair=pair, row=row):
                    back[4 * (y % 2) + quarter] = stage[4 * pair + row]

    def ret_all(count):
        spot = back.at[pl.ds(0, count)]
        return remote(spot, spot, ret_s, ret_r, s, other)

    @pl.when(mixed)
    def _():
        ret_all(7).wait_recv()

    @pl.when(~mixed)
    def _():
        ret_all(8).wait_recv()

    heads = jnp.concatenate(
        [back[0:4].reshape(512, 128), back[4:8].reshape(512, 128), b_heads[...]], axis=1
    )
    first, second = pl.ds(0, 32), pl.ds(32, 32)

    def cross(n):
        return remote(part.at[n, 1 - c], crossed.at[n], cr_s, cr_r.at[n], s, other)

    def far_send(n, way):
        rows = first if way == 0 else second
        return remote(
            chip.at[n, xf, rows], (far_l if way == 0 else far_r).at[n],
            fs, fr.at[n], s, right if way == 0 else left,
        )

    def near_send(n, way):
        rows = second if way == 0 else first
        return remote(
            chip.at[n, xr if way == 0 else xl, rows], (got_l if way == 0 else got_r).at[n, rows],
            gs, gr.at[n], s, right if way == 0 else left,
        )

    def sum_send(n, way):
        rows = first if way == 0 else second
        return remote(
            relayed.at[n, way], (got_l if way == 0 else got_r).at[n, rows],
            ss, gr.at[n], s, right if way == 0 else left,
        )

    def multiply(n):
        partial = jnp.dot(heads, weights[n], preferred_element_type=F32).astype(BF16)
        for col in range(8):
            part[n, col % 2, col // 2] = partial[64 * col : 64 * (col + 1)]
        cross(n).start()

    def join(n):
        cross(n).wait_recv()
        chip[n] = (part[n, c].astype(F32) + crossed[n].astype(F32)).astype(BF16)
        far_send(n, 0).start()
        far_send(n, 1).start()
        near_send(n, 0).start()
        near_send(n, 1).start()

    def pass_on(n, carry):
        remote(relayed.at[n], relayed.at[n], fs, fr.at[n], s, right).wait_recv()
        relayed[n, 0] = (chip[n, xr, first].astype(F32) + far_l[n].astype(F32)).astype(BF16)
        sum_send(n, 0).start()
        relayed[n, 1] = (chip[n, xl, second].astype(F32) + far_r[n].astype(F32)).astype(BF16)
        sum_send(n, 1).start()
        return carry

    remote(weights, weights, gs, w_s, s, other).wait_recv()
    multiply(0)

    def run(n, carry):
        multiply(n)
        join(n - 1)
        return carry

    lax.fori_loop(1, NC, run, 0)
    join(NC - 1)
    def drained(spot, sem):
        remote(spot, spot, sem, q_r, s, other).wait_send()

    drained(rows.at[0], os)
    drained(x_in, xs)
    drained(rows.at[pl.ds(0, 2)], xds)
    drained(kv.at[0, pl.ds(0, 2)], zs)
    drained(kv.at[0, 0], rs)
    drained(kv.at[0], ds)
    lam_send.wait_send()

    @pl.when(s < 15)
    def _():
        rim_send.wait_send()

    @pl.when(mixed)
    def _():
        drained(kv.at[0, 0, pl.ds(0, 3)], a2a_s)
        q_all(7).wait_send()
        ret_all(7).wait_send()

    @pl.when(~mixed)
    def _():
        drained(kv.at[0, 0], a2a_s)
        q_all(8).wait_send()
        ret_all(8).wait_send()

    lax.fori_loop(0, NC, pass_on, 0)

    drained(crossed, cr_s)
    drained(relayed, fs)
    drained(relayed, gs)
    for n in range(NC):
        spot = chip.at[n, pl.ds(0, 2)]
        remote(spot, spot, ss, gr.at[n], s, other).wait_recv()
        total = chip[n, x].astype(F32) + got_l[n].astype(F32) + got_r[n].astype(F32)
        out[:, n * CW : (n + 1) * CW] = total.astype(BF16)
    drained(relayed, ss)


def layer(*operands):
    vmem = pl.BlockSpec(memory_space=VMEM)
    hbm = pl.BlockSpec(memory_space=pltpu.HBM)
    smem = pl.BlockSpec(memory_space=pltpu.SMEM)
    dma = pltpu.SemaphoreType.DMA
    return pl.pallas_call(
        layer_kernel,
        out_shape=jax.ShapeDtypeStruct((64, 4096), BF16),
        in_specs=[hbm] * 7 + [smem, vmem, smem] + [hbm] * 2,
        out_specs=vmem,
        scratch_shapes=[
            VMEM((64, 4096), BF16),
            VMEM((4, 8, 16, 4096), BF16),
            VMEM((4096, 256), BF16), VMEM((4096, 256), BF16),
            VMEM((4096, 256), BF16), VMEM((4096, 256), BF16), VMEM((128, 4096), BF16),
            VMEM((2, 4, 128, 128), BF16), VMEM((2, 2, 4, 128, 128), BF16), VMEM((512, 256), BF16),
            VMEM((2, 4, 4, 4, 128, 128), BF16),
            VMEM((8, 4, 32, 128), BF16),
            VMEM((8, 256, 256), BF16),
            VMEM((640, 128), BF16),
            VMEM((2, 2, 8, 256), F32),
            VMEM((8, 128, 256), F32),
            VMEM((8, 1, 256), F32),
            VMEM((8, 1, 256), F32),
            VMEM((8, 128, 128), BF16),
            VMEM((8, 128, 128), BF16),
            VMEM((512, 256), BF16),
            VMEM((NC, 512, CW), BF16),
            VMEM((NC, 2, 4, 64, CW), BF16),
            VMEM((NC, 4, 64, CW), BF16),
            VMEM((NC, 4, 64, CW), BF16),
            VMEM((NC, 32, CW), BF16),
            VMEM((NC, 32, CW), BF16),
            VMEM((NC, 64, CW), BF16),
            VMEM((NC, 64, CW), BF16),
            VMEM((NC, 2, 32, CW), BF16),
            dma, dma((6,)), dma, dma((4, 2, 2)), dma, dma((4,)), dma, dma((4,)),
            dma, dma((4,)), dma, dma((4, 2)), dma, dma((4,)), dma, dma((4, 2)),
            dma, dma, dma((2,)), dma((2,)), dma, dma,
            dma, dma, dma((NC,)), dma, dma((NC,)), dma, dma, dma((NC,)),
        ],
        compiler_params=pltpu.CompilerParams(
            collective_id=0, has_side_effects=True, vmem_limit_bytes=56 * 2**20
        ),
        name="layer",
    )(*operands)


def shards(
    inputs,
    a_query_w,
    a_key_w,
    a_value_w,
    b_query_w,
    b_key_w,
    b_value_w,
    head_lambda,
    head_gain,
    sink_logit,
    a_out_w,
    b_out_w,
):
    return layer(
        inputs, a_query_w, a_key_w, a_value_w, b_query_w, b_key_w.T, b_value_w.T,
        head_lambda, head_gain[None], sink_logit, a_out_w, b_out_w,
    )


def solution(mesh):
    return jax.shard_map(
        shards,
        mesh=mesh,
        in_specs=(
            P(("sp", "tp"), None),
            P(None, "tp"),
            P(None, "tp"),
            P(None, "tp"),
            P(None, "tp"),
            P(None, "tp"),
            P(None, "tp"),
            P("tp"),
            P(),
            P("tp"),
            P("tp", None),
            P("tp", None),
        ),
        out_specs=P(("sp", "tp"), None),
        check_vma=False,
    )
```

```python
import functools

import jax
import jax.numpy as jnp
from jax import lax
from jax.experimental import pallas as pl
from jax.experimental.pallas import tpu as pltpu
from jax.sharding import PartitionSpec as P

HEAD_DIM = 64
VALUE_DIM = 128
WINDOW = 128

norm_eps = 0.0001
head_scale = 0.8
mask_fill = -1e30

MESH = pl.DeviceIdType.MESH
NT = (((1,), (1,)), ((), ()))
LOG2E = 1.4426950408889634
VMEM = pltpu.VMEM
F32 = jnp.float32
BF16 = jnp.bfloat16


def remote(src, dst, send_sem, recv_sem, row, col):
    return pltpu.make_async_remote_copy(
        src_ref=src,
        dst_ref=dst,
        send_sem=send_sem,
        recv_sem=recv_sem,
        device_id=(row, col),
        device_id_type=MESH,
    )


def soft_chunk(items, mx, ls, acc):
    def weights(i, pieces):
        before = mx[i]
        top = before
        for piece in pieces:
            top = jnp.maximum(top, jnp.max(piece, axis=0, keepdims=True))
        shrink = jnp.exp2(before - top)
        mx[i] = top
        return shrink, [jnp.exp2(piece - top).astype(BF16) for piece in pieces]

    def collect(i, lookup, shrink, pieces):
        got = jnp.dot(lookup, jnp.concatenate(pieces, axis=0), preferred_element_type=F32)
        acc[i] = acc[i] * shrink + got[:VALUE_DIM]
        ls[i] = ls[i] * shrink + got[VALUE_DIM : VALUE_DIM + 1]

    now = items[0][1]()
    held = None
    for at, (i, _, lookup) in enumerate(items):
        later = items[at + 1][1]() if at + 1 < len(items) else None
        current = (i, lookup, *weights(i, now))
        if held is not None:
            collect(*held)
        held, now = current, later
    collect(*held)


NC = 8
CW = 512
GROUPS = 4


def layer_kernel(
    x_hbm, wq_in, wk_in, wv_in, wbq_in, wbk_in, wbv_in, lam_in, gain_in, sink_in, aw_in, bw_in,
    out,
    out_v, x_in, rows, wa, wbq, wbkv, q_own, kv_own, bq_own,
    kv, q_raw, q_mul, near, lam, acc, mx, ls, stage, back, b_heads,
    weights, part, crossed, chip, far_l, far_r, got_l, got_r, relayed,
    out_s, x_s, pw_s, os, orr, xs, xr_s, xds, xdr,
    a2a_s, a2a_r, zs, zr, rs, rr, ds, dr, q_s, q_r, small_s, small_r, ret_s, ret_r,
    w_s, cr_s, cr_r, fs, fr, gs, ss, gr,
):
    s, t = lax.axis_index("sp"), lax.axis_index("tp")
    z, y = s // 4, s % 4
    x, c = t // 2, t % 2
    xr, xl, xf = (x + 1) % 4, (x + 3) % 4, (x + 2) % 4
    other, right, left = 2 * x + 1 - c, 2 * xr + c, 2 * xl + c
    beyond = 2 * xf + c
    up, down = (z + 1) % 4, (z + 3) % 4
    far = (z + 2) % 4
    mate = 3 - z
    side = z + 1 - 2 * (z % 2)
    quarter = 2 * c + z // 2
    lane = lax.broadcasted_iota(jnp.int32, (1, 128), 1)

    x_load = pltpu.make_async_copy(x_hbm, x_in, x_s)
    x_load.start()
    mixed = y // 2 == c
    loads = [
        pltpu.make_async_copy(wq_in, wa.at[:, pl.ds(0, 256)], pw_s.at[2]),
        pltpu.make_async_copy(wk_in, wa.at[:, pl.ds(256, 256)], pw_s.at[0]),
        pltpu.make_async_copy(wv_in, wa.at[:, pl.ds(512, 256)], pw_s.at[1]),
        pltpu.make_async_copy(wbq_in, wbq, pw_s.at[3]),
        pltpu.make_async_copy(wbk_in, wbkv.at[pl.ds(0, 64)], pw_s.at[4]),
        pltpu.make_async_copy(wbv_in, wbkv.at[pl.ds(64, 64)], pw_s.at[5]),
    ]

    def fetch(n, which):
        columns = pl.ds(pl.multiple_of(n * CW, CW), CW)
        source = aw_in if which == 0 else bw_in
        return pltpu.make_async_copy(
            source.at[:, columns], weights.at[n, pl.ds(256 * which, 256)], w_s
        )

    barrier = pltpu.get_barrier_semaphore()

    def greet(row, col):
        pl.semaphore_signal(barrier, inc=1, device_id=(row, col), device_id_type=MESH)

    for j in range(4):
        for core in range(2):
            if j == 0:
                @pl.when(core != c)
                def _(core=core):
                    greet(4 * z + y, 2 * x + core)
            else:
                greet(4 * z + (y + j) % 4, 2 * x + core)
            greet(4 * mate + (y + j) % 4, 2 * x + core)
    greet(4 * side + y, t)
    greet(s, right)
    greet(s, left)
    rim_up = (y == 3) & (z % 2 == 0)
    rim_down = (y == 0) & (z % 2 == 1)

    @pl.when(rim_up)
    def _():
        greet(s + 1, t)

    @pl.when(rim_down)
    def _():
        greet(s - 1, t)

    x_load.wait()
    for load in loads:
        load.start()
    pl.semaphore_wait(barrier, 18 + jnp.where(rim_up | rim_down, 1, 0))

    halves = (pl.ds(0, 2048), pl.ds(2048, 2048))
    every = pl.ds(0, 16)

    def mine16(g):
        return pl.ds(pl.multiple_of(16 * g, 16), 16)

    def own_send(g, way, which):
        return remote(
            x_in.at[mine16(g), halves[which]], rows.at[g, t, every, halves[which]],
            os, orr.at[g, way, which], s, right if way == 0 else left,
        )

    def own_wait(g, way, which):
        spot = rows.at[g, left if way == 0 else right, every, halves[which]]
        return remote(
            spot, spot, os, orr.at[g, way, which],
            s, right if way == 0 else left,
        )

    def xrelay_send(g, way):
        spot = rows.at[g, left if way == 0 else right, every, halves[way]]
        return remote(spot, spot, xs, xr_s.at[g], s, right if way == 0 else left)

    def xrelay_wait(g):
        spot = rows.at[g, beyond]
        return remote(spot, spot, xs, xr_s.at[g], s, right)

    def own_cross(g):
        return remote(x_in.at[mine16(g)], rows.at[g, t], xds, xdr.at[g], s, other)

    def xcross(g, where):
        spot = rows.at[g, 2 * where + c]
        return remote(spot, spot, xds, xdr.at[g], s, other)

    def xcross_wait(g):
        spot = rows.at[g, pl.ds(0, 4)]
        return remote(spot, spot, xds, xdr.at[g], s, other)

    def own_start(g):
        own_send(g, 0, 0).start()
        own_send(g, 1, 1).start()
        own_send(g, 0, 1).start()
        own_send(g, 1, 0).start()
        own_cross(g).start()

    def kv_send(g, head, part_of):
        return remote(
            kv_own.at[head, part_of, g], kv.at[part_of, z, g, y],
            a2a_s, a2a_r.at[g],
            4 * z + 2 * c + head, 2 * x + part_of,
        )

    def kv_local(head, part_of):
        return (2 * c + head == y) & (part_of == c)

    def a2a_wait(g, count):
        spot = kv.at[c, z, g, pl.ds(0, count)]
        return remote(spot, spot, a2a_s, a2a_r.at[g], s, other)

    def z_send(g, way):
        spot = kv.at[c, z, g]
        return remote(spot, spot, zs, zr.at[g, way], 4 * (up, down)[way] + y, t)

    def z_wait(g, way):
        spot = kv.at[c, (down, up)[way], g]
        return remote(spot, spot, zs, zr.at[g, way], 4 * (up, down)[way] + y, t)

    def relay_send(g, way):
        spot = kv.at[c, (down, up)[way], g, pl.ds(2 * way, 2)]
        return remote(spot, spot, rs, rr.at[g], 4 * (up, down)[way] + y, t)

    def relay_wait(g):
        spot = kv.at[c, far, g]
        return remote(spot, spot, rs, rr.at[g], 4 * up + y, t)

    def cross_send(level, g):
        spot = kv.at[c, level, g]
        return remote(spot, spot, ds, dr.at[level, g // 2], s, other)

    def cross_wait(level, pair):
        spot = kv.at[1 - c, level, pl.ds(2 * pair, 2)]
        return remote(spot, spot, ds, dr.at[level, pair], s, other)

    def spread(g):
        @pl.when(mixed)
        def _():
            a2a_wait(g, 3).wait_recv()

        @pl.when(~mixed)
        def _():
            a2a_wait(g, 4).wait_recv()

        z_send(g, 0).start()
        z_send(g, 1).start()
        cross_send(z, g).start()

    def zrelay(g):
        z_wait(g, 0).wait_recv()
        relay_send(g, 0).start()
        cross_send(down, g).start()
        z_wait(g, 1).wait_recv()
        relay_send(g, 1).start()
        cross_send(up, g).start()

    def zfar(g):
        relay_wait(g).wait_recv()
        cross_send(far, g).start()

    own_start(0)
    own_start(1)
    lam_send = remote(lam.at[c], lam.at[c], small_s.at[0], small_r.at[0], s, other)
    for g in range(GROUPS):
        rows[g, t] = x_in[16 * g : 16 * (g + 1)]
    for head in range(2):
        lam[c, head] = jnp.full((8, 256), lam_in[head], F32)
    acc[...] = jnp.zeros_like(acc)
    ls[...] = jnp.zeros_like(ls)
    mx[...] = jnp.full_like(mx, mask_fill)

    @pl.when(s == 0)
    def _():
        near[pl.ds(0, 128)] = jnp.zeros((128, 128), BF16)

    def near_rows(g):
        own_wait(g, 0, 0).wait_recv()
        xrelay_send(g, 0).start()
        own_wait(g, 1, 1).wait_recv()
        xrelay_send(g, 1).start()

        @pl.when(g == 0)
        def _():
            own_start(2)
            own_start(3)

        own_wait(g, 0, 1).wait_recv()
        xcross(g, xl).start()
        own_wait(g, 1, 0).wait_recv()
        xcross(g, xr).start()

    near_rows(0)
    near_rows(1)

    def far_rows(g):
        xrelay_wait(g).wait_recv()
        xcross(g, xf).start()

    def project_b(at, count):
        block = rows[at : at + count].reshape(128 * count, 4096)
        b_queries = jnp.dot(block, wbq[...], preferred_element_type=F32).astype(BF16)
        b_pair = lax.dot_general(block, wbkv[...], NT, preferred_element_type=F32).astype(BF16)
        for k in range(count):
            for d in range(8):
                first_row = 64 * d + 16 * (at + k)
                take = slice(128 * k + 16 * d, 128 * k + 16 * (d + 1))
                bq_own[first_row : first_row + 16] = b_queries[take]
                near[first_row + 128 : first_row + 144] = b_pair[take]

    def gather(g, carry):
        @pl.when(g == 0)
        def _():
            far_rows(0)
            near_rows(2)

        @pl.when(g == 1)
        def _():
            near_rows(3)
            far_rows(1)
            far_rows(2)
            spread(0)

        @pl.when(g == 2)
        def _():
            far_rows(3)

        @pl.when(g == 0)
        def _():
            for load in loads[:3]:
                load.wait()

        xcross_wait(g).wait_recv()
        block = rows[g].reshape(128, 4096)
        found = jnp.dot(block, wa[...], preferred_element_type=F32)
        q_own[0, g] = found[:, :128].astype(BF16)
        q_own[1, g] = found[:, 128:256].astype(BF16)
        keys, values = found[:, 256:512], found[:, 512:]
        for head in range(2):
            lanes = slice(128 * head, 128 * (head + 1))
            kv_own[head, 0, g] = keys[:, lanes].astype(BF16)
            kv_own[head, 1, g] = jnp.transpose(values[:, lanes]).astype(BF16)

            @pl.when(2 * c + head == y)
            def _(head=head):
                kv[c, z, g, y] = kv_own[head, c, g]

            for part_of in range(2):
                @pl.when(~kv_local(head, part_of))
                def _(head=head, part_of=part_of):
                    kv_send(g, head, part_of).start()

        send_queries(g)

        @pl.when(g == 0)
        def _():
            for n in range(NC):
                fetch(n, 0).start()
                fetch(n, 1).start()
            for load in loads[3:]:
                load.wait()
            project_b(0, 1)

        return carry

    def q_send(g, head, k, core):
        goal = z if k == 0 else mate
        return remote(
            q_own.at[head, g, pl.ds(32 * (2 * core + goal // 2), 32)],
            q_raw.at[4 * (z // 2) + y, g], q_s, q_r,
            4 * goal + 2 * c + head, 2 * x + core,
        )

    def q_local(head, k, core):
        return (2 * c + head == y) & (core == c) & (k == 0)

    def send_queries(g):
        for head in range(2):
            for k in range(2):
                for core in range(2):
                    @pl.when(~q_local(head, k, core))
                    def _(head=head, k=k, core=core):
                        q_send(g, head, k, core).start()

            @pl.when(2 * c + head == y)
            def _(head=head):
                q_raw[4 * (z // 2) + y, g] = q_own[head, g, pl.ds(32 * quarter, 32)]

    def q_all(count):
        spot = q_raw.at[pl.ds(0, count)]
        return remote(spot, spot, q_s, q_r, s, other)

    lam_send.start()
    lax.fori_loop(0, GROUPS, gather, 0)
    zrelay(0)
    project_b(1, 1)
    spread(1)
    project_b(2, 2)
    spread(2)

    rim_send = remote(
        near.at[pl.ds(512, 128)], near.at[pl.ds(0, 128)], small_s.at[1], small_r.at[1],
        jnp.minimum(s + 1, 15), t,
    )

    @pl.when(s < 15)
    def _():
        rim_send.start()

    def windowed(block, carry):
        start = pl.multiple_of(block * 128, 128)
        span = near[pl.ds(start, 256)]
        span32 = span.astype(F32)
        turned = jnp.concatenate([span32[:, HEAD_DIM:], span32[:, :HEAD_DIM]], axis=1)
        keys = jnp.where(lane < HEAD_DIM, span32, turned).astype(BF16)
        values = jnp.transpose(span32)[HEAD_DIM:].astype(BF16)
        parts = []
        sinks = []
        for j in range(4):
            own = bq_own[pl.ds(start, 128), 128 * (j // 2) : 128 * (j // 2 + 1)]
            mine = (lane >= HEAD_DIM) if j % 2 else (lane < HEAD_DIM)
            parts.append(jnp.where(mine, own.astype(F32), 0.0).astype(BF16))
            sinks.append(jnp.full((1, 128), sink_in[j] * LOG2E, F32))
        queries = jnp.concatenate(parts, axis=0)
        sink = jnp.concatenate(sinks, axis=1)
        scores = lax.dot_general(keys, queries, NT, preferred_element_type=F32)
        scores = scores * (LOG2E * HEAD_DIM ** (-0.5))
        key_at = lax.broadcasted_iota(jnp.int32, (256, 512), 0)
        query_at = lax.broadcasted_iota(jnp.int32, (256, 512), 1) % 128
        first = jnp.where((s == 0) & (block == 0), 128, 0)
        allowed = (key_at > query_at) & (key_at <= query_at + WINDOW) & (key_at >= first)
        scores = jnp.where(allowed, scores, mask_fill)
        top = jnp.maximum(jnp.max(scores, axis=0, keepdims=True), sink)
        weights = jnp.exp2(scores - top)
        total = jnp.sum(weights, axis=0, keepdims=True) + jnp.exp2(sink - top)
        found = jnp.dot(values, weights.astype(BF16), preferred_element_type=F32) / total
        tall = jnp.concatenate([found[:, 128 * j : 128 * (j + 1)] for j in range(4)], axis=0)
        b_heads[pl.ds(start, 128)] = jnp.transpose(tall).astype(BF16)
        return carry

    windowed(1, 0)
    spread(3)

    @pl.when(mixed)
    def _():
        q_all(7).wait_recv()

    @pl.when(~mixed)
    def _():
        q_all(8).wait_recv()

    for pair in range(2):
        for row in range(4):
            raw = q_raw[4 * pair + row].astype(F32)
            raw = jnp.concatenate(
                [raw[g, 16 * d : 16 * (d + 1)] for d in range(2) for g in range(4)], axis=0
            )
            wide = raw * (LOG2E * HEAD_DIM ** (-0.5))
            high = wide.astype(BF16).astype(F32)
            both = jnp.transpose(jnp.concatenate([high, wide - high], axis=1))
            tall = lax.broadcasted_iota(jnp.int32, (256, 1), 0) % 128
            for m in range(2):
                mine = (tall >= HEAD_DIM) if m else (tall < HEAD_DIM)
                i = pair * 4 + (row // 2) * 2 + m
                span = slice(128 * (row % 2), 128 * (row % 2) + 128)
                q_mul[i, :, span] = jnp.where(mine, both, 0.0).astype(BF16)

    def unit(level, pair):
        keys = kv[0, level, pl.ds(2 * pair, 2)].reshape(1024, 128)
        held = kv[1, level, pl.ds(2 * pair, 2)].reshape(1024, 128)
        lookup = jnp.concatenate([held[128 * k : 128 * (k + 1)] for k in range(8)], axis=1)
        lookup = jnp.concatenate([lookup, jnp.ones((16, 1024), BF16)], axis=0)
        return jnp.concatenate([keys, keys], axis=1), lookup

    def small_unit(level, pair, two):
        rows_of = (pl.ds(2 * pair, 2), pl.ds(2 * two, 2))
        keys = kv[0, level, rows_of[0], rows_of[1]].reshape(512, 128)
        held = kv[1, level, rows_of[0], rows_of[1]].reshape(512, 128)
        lookup = jnp.concatenate([held[128 * k : 128 * (k + 1)] for k in range(4)], axis=1)
        lookup = jnp.concatenate([lookup, jnp.ones((16, 512), BF16)], axis=0)
        return jnp.concatenate([keys, keys], axis=1), lookup

    key_at = lax.broadcasted_iota(jnp.int32, (256, 256), 0)
    query_at = lax.broadcasted_iota(jnp.int32, (256, 256), 1)
    apart = 512 * (key_at // 128) + 64 * ((key_at % 128) // 16) + key_at % 16
    apart = apart - (query_at % 128) - 512 * (query_at // 128)

    def attend(level, pair, sel):
        mark = jnp.where(sel == 0, jnp.minimum(z, mate), jnp.maximum(z, mate))

        def score(keys, i):
            return [
                jnp.dot(keys[256 * k : 256 * (k + 1)], q_mul[i], preferred_element_type=F32)
                for k in range(2)
            ]

        @pl.when(level < mark)
        def _():
            keys, lookup = unit(level, pair)
            items = []
            for h in range(2):
                span = slice(512 * h, 512 * (h + 1))
                for k in range(4):
                    i = sel * 4 + k
                    items.append(
                        (i, functools.partial(score, keys[span], i), lookup[:, span])
                    )
            soft_chunk(items, mx, ls, acc)

        @pl.when(level == mark)
        def _():
            base = 128 * quarter - 32 * pair

            def hidden(keys, i):
                return [
                    jnp.where(apart <= base - 16 * k, piece, mask_fill)
                    for k, piece in enumerate(score(keys, i))
                ]

            items = []
            low = small_unit(level, pair, 0)
            high = small_unit(level, pair, 1)
            for g, (keys, lookup), rule in ((0, low, hidden), (1, low, score), (1, high, hidden)):
                for m in range(2):
                    i = sel * 4 + g * 2 + m
                    items.append((i, functools.partial(rule, keys, i), lookup))
            soft_chunk(items, mx, ls, acc)

    def step(it, carry):
        @pl.when(it == 1)
        def _():
            zrelay(1)
            zfar(0)

        @pl.when((it == 2) | (it == 3))
        def _():
            windowed(it, 0)
            zrelay(it)

        @pl.when(it == 3)
        def _():
            zfar(1)

        @pl.when(it == 4)
        def _():
            @pl.when(s > 0)
            def _():
                rim_send.wait_recv()

            windowed(0, 0)

        @pl.when(it == 5)
        def _():
            zfar(2)

        @pl.when(it == 6)
        def _():
            zfar(3)

        level = jnp.where(
            it < 2, z,
            jnp.where(
                (it == 2) | (it == 5), down, jnp.where((it == 3) | (it == 6), up, far)
            ),
        )
        pair = jnp.where((it == 1) | (it >= 5), 1, 0)
        cross_wait(level, pair).wait_recv()

        def one(sel, inner):
            attend(level, pair, sel)
            return inner

        lax.fori_loop(0, 2, one, 0)
        return carry

    lax.fori_loop(0, 8, step, 0)

    lam_send.wait_recv()
    mixing = lam[y // 2, y % 2, 0:1, :]
    gain = gain_in[...] * head_scale

    def ret_send(pair, row):
        goal = jnp.minimum(z, mate) if pair == 0 else jnp.maximum(z, mate)
        return remote(
            stage.at[4 * pair + row], back.at[4 * (y % 2) + quarter], ret_s, ret_r,
            4 * goal + row, 2 * x + y // 2,
        )

    def ret_local(pair, row):
        return (pair == z // 2) & (row == y) & (y // 2 == c)

    for pair in range(2):
        for g in range(2):
            i = pair * 4 + g * 2
            first_mean = acc[i] / ls[i]
            second_mean = acc[i + 1] / ls[i + 1]
            gap = first_mean - mixing * second_mean
            square = jnp.mean(gap * gap, axis=0, keepdims=True)
            done = gap * lax.rsqrt(square + norm_eps)
            tall = (jnp.transpose(done) * gain).astype(BF16)
            for k in range(2):
                row = 2 * g + k
                stage[4 * pair + row] = tall[128 * k : 128 * (k + 1)]

                @pl.when(~ret_local(pair, row))
                def _(pair=pair, row=row):
                    ret_send(pair, row).start()

                @pl.when(ret_local(pair, row))
                def _(pair=pair, row=row):
                    back[4 * (y % 2) + quarter] = stage[4 * pair + row]

    def ret_all(count):
        spot = back.at[pl.ds(0, count)]
        return remote(spot, spot, ret_s, ret_r, s, other)

    @pl.when(mixed)
    def _():
        ret_all(7).wait_recv()

    @pl.when(~mixed)
    def _():
        ret_all(8).wait_recv()

    heads = jnp.concatenate(
        [back[0:4].reshape(512, 128), back[4:8].reshape(512, 128), b_heads[...]], axis=1
    )
    first, second = pl.ds(0, 32), pl.ds(32, 32)

    def cross(n):
        return remote(part.at[n, 1 - c], crossed.at[n], cr_s, cr_r.at[n], s, other)

    def far_send(n, way):
        rows = first if way == 0 else second
        return remote(
            chip.at[n, xf, rows], (far_l if way == 0 else far_r).at[n],
            fs, fr.at[n], s, right if way == 0 else left,
        )

    def near_send(n, way):
        rows = second if way == 0 else first
        return remote(
            chip.at[n, xr if way == 0 else xl, rows], (got_l if way == 0 else got_r).at[n, rows],
            gs, gr.at[n], s, right if way == 0 else left,
        )

    def sum_send(n, way):
        rows = first if way == 0 else second
        return remote(
            relayed.at[n, way], (got_l if way == 0 else got_r).at[n, rows],
            ss, gr.at[n], s, right if way == 0 else left,
        )

    def multiply(n):
        partial = jnp.dot(heads, weights[n], preferred_element_type=F32).astype(BF16)
        for col in range(8):
            part[n, col % 2, col // 2] = partial[64 * col : 64 * (col + 1)]
        cross(n).start()

    def join(n):
        cross(n).wait_recv()
        chip[n] = (part[n, c].astype(F32) + crossed[n].astype(F32)).astype(BF16)
        far_send(n, 0).start()
        far_send(n, 1).start()
        near_send(n, 0).start()
        near_send(n, 1).start()

    def pass_on(n, carry):
        remote(relayed.at[n], relayed.at[n], fs, fr.at[n], s, right).wait_recv()
        relayed[n, 0] = (chip[n, xr, first].astype(F32) + far_l[n].astype(F32)).astype(BF16)
        sum_send(n, 0).start()
        relayed[n, 1] = (chip[n, xl, second].astype(F32) + far_r[n].astype(F32)).astype(BF16)
        sum_send(n, 1).start()
        return carry

    remote(weights, weights, gs, w_s, s, other).wait_recv()
    multiply(0)

    def run(n, carry):
        multiply(n)
        join(n - 1)
        return carry

    lax.fori_loop(1, NC, run, 0)
    join(NC - 1)
    def drained(spot, sem):
        remote(spot, spot, sem, q_r, s, other).wait_send()

    drained(rows.at[0], os)
    drained(x_in, xs)
    drained(rows.at[pl.ds(0, 2)], xds)
    drained(kv.at[0, pl.ds(0, 2)], zs)
    drained(kv.at[0, 0], rs)
    drained(kv.at[0], ds)
    lam_send.wait_send()

    @pl.when(s < 15)
    def _():
        rim_send.wait_send()

    @pl.when(mixed)
    def _():
        drained(kv.at[0, 0, pl.ds(0, 3)], a2a_s)
        q_all(7).wait_send()
        ret_all(7).wait_send()

    @pl.when(~mixed)
    def _():
        drained(kv.at[0, 0], a2a_s)
        q_all(8).wait_send()
        ret_all(8).wait_send()

    lax.fori_loop(0, NC, pass_on, 0)

    drained(crossed, cr_s)
    drained(relayed, fs)
    drained(relayed, gs)
    for n in range(NC):
        spot = chip.at[n, pl.ds(0, 2)]
        remote(spot, spot, ss, gr.at[n], s, other).wait_recv()
        total = chip[n, x].astype(F32) + got_l[n].astype(F32) + got_r[n].astype(F32)
        out_v[n] = total.astype(BF16)
        pltpu.make_async_copy(out_v.at[n], out.at[:, pl.ds(n * CW, CW)], out_s).start()
    drained(relayed, ss)
    pltpu.make_async_copy(x_in, out, out_s).wait()


def layer(*operands):
    vmem = pl.BlockSpec(memory_space=VMEM)
    hbm = pl.BlockSpec(memory_space=pltpu.HBM)
    smem = pl.BlockSpec(memory_space=pltpu.SMEM)
    dma = pltpu.SemaphoreType.DMA
    return pl.pallas_call(
        layer_kernel,
        out_shape=jax.ShapeDtypeStruct((64, 4096), BF16),
        in_specs=[hbm] * 7 + [smem, vmem, smem] + [hbm] * 2,
        out_specs=hbm,
        scratch_shapes=[
            VMEM((NC, 64, CW), BF16),
            VMEM((64, 4096), BF16),
            VMEM((4, 8, 16, 4096), BF16),
            VMEM((4096, 768), BF16), VMEM((4096, 256), BF16), VMEM((128, 4096), BF16),
            VMEM((2, 4, 128, 128), BF16), VMEM((2, 2, 4, 128, 128), BF16), VMEM((512, 256), BF16),
            VMEM((2, 4, 4, 4, 128, 128), BF16),
            VMEM((8, 4, 32, 128), BF16),
            VMEM((8, 256, 256), BF16),
            VMEM((640, 128), BF16),
            VMEM((2, 2, 8, 256), F32),
            VMEM((8, 128, 256), F32),
            VMEM((8, 1, 256), F32),
            VMEM((8, 1, 256), F32),
            VMEM((8, 128, 128), BF16),
            VMEM((8, 128, 128), BF16),
            VMEM((512, 256), BF16),
            VMEM((NC, 512, CW), BF16),
            VMEM((NC, 2, 4, 64, CW), BF16),
            VMEM((NC, 4, 64, CW), BF16),
            VMEM((NC, 4, 64, CW), BF16),
            VMEM((NC, 32, CW), BF16),
            VMEM((NC, 32, CW), BF16),
            VMEM((NC, 64, CW), BF16),
            VMEM((NC, 64, CW), BF16),
            VMEM((NC, 2, 32, CW), BF16),
            dma, dma, dma((6,)), dma, dma((4, 2, 2)), dma, dma((4,)), dma, dma((4,)),
            dma, dma((4,)), dma, dma((4, 2)), dma, dma((4,)), dma, dma((4, 2)),
            dma, dma, dma((2,)), dma((2,)), dma, dma,
            dma, dma, dma((NC,)), dma, dma((NC,)), dma, dma, dma((NC,)),
        ],
        compiler_params=pltpu.CompilerParams(
            collective_id=0, has_side_effects=True, vmem_limit_bytes=56 * 2**20
        ),
        name="layer",
    )(*operands)


def shards(
    inputs,
    a_query_w,
    a_key_w,
    a_value_w,
    b_query_w,
    b_key_w,
    b_value_w,
    head_lambda,
    head_gain,
    sink_logit,
    a_out_w,
    b_out_w,
):
    return layer(
        inputs, a_query_w, a_key_w, a_value_w, b_query_w, b_key_w.T, b_value_w.T,
        head_lambda, head_gain[None], sink_logit, a_out_w, b_out_w,
    )


def solution(mesh):
    return jax.shard_map(
        shards,
        mesh=mesh,
        in_specs=(
            P(("sp", "tp"), None),
            P(None, "tp"),
            P(None, "tp"),
            P(None, "tp"),
            P(None, "tp"),
            P(None, "tp"),
            P(None, "tp"),
            P("tp"),
            P(),
            P("tp"),
            P("tp", None),
            P("tp", None),
        ),
        out_specs=P(("sp", "tp"), None),
        check_vma=False,
    )
```

```python
import functools

import jax
import jax.numpy as jnp
from jax import lax
from jax.experimental import pallas as pl
from jax.experimental.pallas import tpu as pltpu
from jax.sharding import PartitionSpec as P

HEAD_DIM = 64
VALUE_DIM = 128
WINDOW = 128

norm_eps = 0.0001
head_scale = 0.8
mask_fill = -1e30

MESH = pl.DeviceIdType.MESH
NT = (((1,), (1,)), ((), ()))
LOG2E = 1.4426950408889634
VMEM = pltpu.VMEM
F32 = jnp.float32
BF16 = jnp.bfloat16


def remote(src, dst, send_sem, recv_sem, row, col):
    return pltpu.make_async_remote_copy(
        src_ref=src,
        dst_ref=dst,
        send_sem=send_sem,
        recv_sem=recv_sem,
        device_id=(row, col),
        device_id_type=MESH,
    )


def soft_chunk(items, mx, ls, acc):
    def weights(i, pieces):
        before = mx[i]
        top = before
        for piece in pieces:
            top = jnp.maximum(top, jnp.max(piece, axis=0, keepdims=True))
        shrink = jnp.exp2(before - top)
        mx[i] = top
        return shrink, [jnp.exp2(piece - top).astype(BF16) for piece in pieces]

    def collect(i, lookup, shrink, pieces):
        got = jnp.dot(lookup, jnp.concatenate(pieces, axis=0), preferred_element_type=F32)
        acc[i] = acc[i] * shrink + got[:VALUE_DIM]
        ls[i] = ls[i] * shrink + got[VALUE_DIM : VALUE_DIM + 1]

    now = items[0][1]()
    held = None
    for at, (i, _, lookup) in enumerate(items):
        later = items[at + 1][1]() if at + 1 < len(items) else None
        current = (i, lookup, *weights(i, now))
        if held is not None:
            collect(*held)
        held, now = current, later
    collect(*held)


NC = 8
CW = 512
GROUPS = 4


def layer_kernel(
    x_hbm, wq_in, wk_in, wv_in, wbq_in, wbk_in, wbv_in, lam_in, gain_in, sink_in, aw_in, bw_in,
    out,
    out_v, x_in, rows, wa, wbq, wbkv, q_own, kv_own, bq_own,
    kv, q_raw, q_mul, near, lam, acc, mx, ls, stage, back, b_heads,
    weights, part, crossed, chip, far_l, far_r, got_l, got_r, relayed,
    out_s, x_s, pw_s, os, orr, xs, xr_s, xds, xdr,
    a2a_s, a2a_r, zs, zr, rs, rr, ds, dr, q_s, q_r, small_s, small_r, ret_s, ret_r,
    w_s, cr_s, cr_r, fs, fr, gs, ss, gr,
):
    s, t = lax.axis_index("sp"), lax.axis_index("tp")
    z, y = s // 4, s % 4
    x, c = t // 2, t % 2
    xr, xl, xf = (x + 1) % 4, (x + 3) % 4, (x + 2) % 4
    other, right, left = 2 * x + 1 - c, 2 * xr + c, 2 * xl + c
    beyond = 2 * xf + c
    up, down = (z + 1) % 4, (z + 3) % 4
    far = (z + 2) % 4
    mate = 3 - z
    side = z + 1 - 2 * (z % 2)
    quarter = 2 * c + z // 2
    most = jnp.maximum(z, mate)
    lane = lax.broadcasted_iota(jnp.int32, (1, 128), 1)

    x_load = pltpu.make_async_copy(x_hbm, x_in, x_s)
    x_load.start()
    mixed = y // 2 == c
    loads = [
        pltpu.make_async_copy(wq_in, wa.at[:, pl.ds(0, 256)], pw_s.at[2]),
        pltpu.make_async_copy(wk_in, wa.at[:, pl.ds(256, 256)], pw_s.at[0]),
        pltpu.make_async_copy(wv_in, wa.at[:, pl.ds(512, 256)], pw_s.at[1]),
        pltpu.make_async_copy(wbq_in, wbq, pw_s.at[3]),
        pltpu.make_async_copy(wbk_in, wbkv.at[pl.ds(0, 64)], pw_s.at[4]),
        pltpu.make_async_copy(wbv_in, wbkv.at[pl.ds(64, 64)], pw_s.at[5]),
    ]

    def fetch(n, which):
        columns = pl.ds(pl.multiple_of(n * CW, CW), CW)
        source = aw_in if which == 0 else bw_in
        return pltpu.make_async_copy(
            source.at[:, columns], weights.at[n, pl.ds(256 * which, 256)], w_s
        )

    barrier = pltpu.get_barrier_semaphore()

    def greet(row, col):
        pl.semaphore_signal(barrier, inc=1, device_id=(row, col), device_id_type=MESH)

    for j in range(4):
        for core in range(2):
            if j == 0:
                @pl.when(core != c)
                def _(core=core):
                    greet(4 * z + y, 2 * x + core)
            else:
                greet(4 * z + (y + j) % 4, 2 * x + core)
            greet(4 * mate + (y + j) % 4, 2 * x + core)
    greet(4 * side + y, t)
    greet(s, right)
    greet(s, left)
    rim_up = (y == 3) & (z % 2 == 0)
    rim_down = (y == 0) & (z % 2 == 1)

    @pl.when(rim_up)
    def _():
        greet(s + 1, t)

    @pl.when(rim_down)
    def _():
        greet(s - 1, t)

    x_load.wait()
    for load in loads:
        load.start()
    pl.semaphore_wait(barrier, 18 + jnp.where(rim_up | rim_down, 1, 0))

    halves = (pl.ds(0, 2048), pl.ds(2048, 2048))
    every = pl.ds(0, 16)

    def mine16(g):
        return pl.ds(pl.multiple_of(16 * g, 16), 16)

    def own_send(g, way, which):
        return remote(
            x_in.at[mine16(g), halves[which]], rows.at[g, t, every, halves[which]],
            os, orr.at[g, way, which], s, right if way == 0 else left,
        )

    def own_wait(g, way, which):
        spot = rows.at[g, left if way == 0 else right, every, halves[which]]
        return remote(
            spot, spot, os, orr.at[g, way, which],
            s, right if way == 0 else left,
        )

    def xrelay_send(g, way):
        spot = rows.at[g, left if way == 0 else right, every, halves[way]]
        return remote(spot, spot, xs, xr_s.at[g], s, right if way == 0 else left)

    def xrelay_wait(g):
        spot = rows.at[g, beyond]
        return remote(spot, spot, xs, xr_s.at[g], s, right)

    def own_cross(g):
        return remote(x_in.at[mine16(g)], rows.at[g, t], xds, xdr.at[g], s, other)

    def xcross(g, where):
        spot = rows.at[g, 2 * where + c]
        return remote(spot, spot, xds, xdr.at[g], s, other)

    def xcross_wait(g):
        spot = rows.at[g, pl.ds(0, 4)]
        return remote(spot, spot, xds, xdr.at[g], s, other)

    def own_start(g):
        own_send(g, 0, 0).start()
        own_send(g, 1, 1).start()
        own_send(g, 0, 1).start()
        own_send(g, 1, 0).start()
        own_cross(g).start()

    def kv_send(g, head, part_of):
        return remote(
            kv_own.at[head, part_of, g], kv.at[part_of, z, g, y],
            a2a_s, a2a_r.at[g],
            4 * z + 2 * c + head, 2 * x + part_of,
        )

    def kv_local(head, part_of):
        return (2 * c + head == y) & (part_of == c)

    def a2a_wait(g, count):
        spot = kv.at[c, z, g, pl.ds(0, count)]
        return remote(spot, spot, a2a_s, a2a_r.at[g], s, other)

    def z_send(g, way):
        spot = kv.at[c, z, g]
        return remote(spot, spot, zs, zr.at[g, way], 4 * (up, down)[way] + y, t)

    def z_wait(g, way):
        spot = kv.at[c, (down, up)[way], g]
        return remote(spot, spot, zs, zr.at[g, way], 4 * (up, down)[way] + y, t)

    def relay_send(g, way):
        spot = kv.at[c, (down, up)[way], g, pl.ds(2 * way, 2)]
        return remote(spot, spot, rs, rr.at[g], 4 * (up, down)[way] + y, t)

    def relay_whole(g):
        spot = kv.at[c, up, g]
        return remote(spot, spot, rs, rr.at[g], 4 * down + y, t)

    def relay_wait(g):
        spot = kv.at[c, far, g]
        return remote(spot, spot, rs, rr.at[g], 4 * up + y, t)

    def cross_send(level, g):
        spot = kv.at[c, level, g]
        return remote(spot, spot, ds, dr.at[level, g // 2], s, other)

    def cross_wait(level, pair):
        spot = kv.at[1 - c, level, pl.ds(2 * pair, 2)]
        return remote(spot, spot, ds, dr.at[level, pair], s, other)

    def spread(g):
        @pl.when(mixed)
        def _():
            a2a_wait(g, 3).wait_recv()

        @pl.when(~mixed)
        def _():
            a2a_wait(g, 4).wait_recv()

        z_send(g, 0).start()

        @pl.when(z < 3)
        def _():
            z_send(g, 1).start()

        cross_send(z, g).start()

    def zrelay(g):
        z_wait(g, 0).wait_recv()

        @pl.when(z >= 2)
        def _():
            relay_send(g, 0).start()

        cross_send(down, g).start()

        @pl.when(z != 2)
        def _():
            z_wait(g, 1).wait_recv()

            @pl.when(z == 3)
            def _():
                relay_whole(g).start()

            @pl.when(z < 2)
            def _():
                relay_send(g, 1).start()

            cross_send(up, g).start()

    def zfar(g):
        @pl.when(z != 1)
        def _():
            relay_wait(g).wait_recv()
            cross_send(far, g).start()

    own_start(0)
    own_start(1)
    lam_send = remote(lam.at[c], lam.at[c], small_s.at[0], small_r.at[0], s, other)
    for g in range(GROUPS):
        rows[g, t] = x_in[16 * g : 16 * (g + 1)]
    for head in range(2):
        lam[c, head] = jnp.full((8, 256), lam_in[head], F32)
    acc[...] = jnp.zeros_like(acc)
    ls[...] = jnp.zeros_like(ls)
    mx[...] = jnp.full_like(mx, mask_fill)

    @pl.when(s == 0)
    def _():
        near[pl.ds(0, 128)] = jnp.zeros((128, 128), BF16)

    def near_rows(g):
        own_wait(g, 0, 0).wait_recv()
        xrelay_send(g, 0).start()
        own_wait(g, 1, 1).wait_recv()
        xrelay_send(g, 1).start()

        @pl.when(g < GROUPS - 2)
        def _():
            own_start(g + 2)

        own_wait(g, 0, 1).wait_recv()
        xcross(g, xl).start()
        own_wait(g, 1, 0).wait_recv()
        xcross(g, xr).start()

    near_rows(0)
    near_rows(1)

    def far_rows(g):
        xrelay_wait(g).wait_recv()
        xcross(g, xf).start()

    def project_b(at, count):
        block = rows[at : at + count].reshape(128 * count, 4096)
        b_queries = jnp.dot(block, wbq[...], preferred_element_type=F32).astype(BF16)
        b_pair = lax.dot_general(block, wbkv[...], NT, preferred_element_type=F32).astype(BF16)
        for k in range(count):
            for d in range(8):
                first_row = 64 * d + 16 * (at + k)
                take = slice(128 * k + 16 * d, 128 * k + 16 * (d + 1))
                bq_own[first_row : first_row + 16] = b_queries[take]
                near[first_row + 128 : first_row + 144] = b_pair[take]

    def gather(g, carry):
        @pl.when(g == 0)
        def _():
            far_rows(0)
            near_rows(2)

        @pl.when(g == 1)
        def _():
            far_rows(1)

        @pl.when(g == 2)
        def _():
            near_rows(3)
            spread(0)
            far_rows(2)

        @pl.when(g == 3)
        def _():
            spread(1)
            far_rows(3)

        @pl.when(g == 0)
        def _():
            for load in loads[:3]:
                load.wait()

        xcross_wait(g).wait_recv()
        block = rows[g].reshape(128, 4096)
        found = jnp.dot(block, wa[...], preferred_element_type=F32)
        q_own[0, g] = found[:, :128].astype(BF16)
        q_own[1, g] = found[:, 128:256].astype(BF16)
        keys, values = found[:, 256:512], found[:, 512:]
        for head in range(2):
            lanes = slice(128 * head, 128 * (head + 1))
            kv_own[head, 0, g] = keys[:, lanes].astype(BF16)
            kv_own[head, 1, g] = jnp.transpose(values[:, lanes]).astype(BF16)

            @pl.when(2 * c + head == y)
            def _(head=head):
                kv[c, z, g, y] = kv_own[head, c, g]

            for part_of in range(2):
                @pl.when(~kv_local(head, part_of))
                def _(head=head, part_of=part_of):
                    kv_send(g, head, part_of).start()

        send_queries(g)

        @pl.when(g == 0)
        def _():
            for n in range(NC):
                fetch(n, 0).start()
                fetch(n, 1).start()
            for load in loads[3:]:
                load.wait()
            project_b(0, 1)

        return carry

    def q_send(g, head, k, core):
        goal = z if k == 0 else mate
        return remote(
            q_own.at[head, g, pl.ds(32 * (2 * core + goal // 2), 32)],
            q_raw.at[4 * (z // 2) + y, g], q_s, q_r,
            4 * goal + 2 * c + head, 2 * x + core,
        )

    def q_local(head, k, core):
        return (2 * c + head == y) & (core == c) & (k == 0)

    def send_queries(g):
        for head in range(2):
            for k in range(2):
                for core in range(2):
                    @pl.when(~q_local(head, k, core))
                    def _(head=head, k=k, core=core):
                        q_send(g, head, k, core).start()

            @pl.when(2 * c + head == y)
            def _(head=head):
                q_raw[4 * (z // 2) + y, g] = q_own[head, g, pl.ds(32 * quarter, 32)]

    def q_all(count):
        spot = q_raw.at[pl.ds(0, count)]
        return remote(spot, spot, q_s, q_r, s, other)

    lam_send.start()
    lax.fori_loop(0, GROUPS, gather, 0)
    project_b(1, 1)
    spread(2)
    project_b(2, 2)
    zrelay(0)

    rim_send = remote(
        near.at[pl.ds(512, 128)], near.at[pl.ds(0, 128)], small_s.at[1], small_r.at[1],
        jnp.minimum(s + 1, 15), t,
    )

    @pl.when(s < 15)
    def _():
        rim_send.start()

    def windowed(block, carry):
        start = pl.multiple_of(block * 128, 128)
        span = near[pl.ds(start, 256)]
        span32 = span.astype(F32)
        turned = jnp.concatenate([span32[:, HEAD_DIM:], span32[:, :HEAD_DIM]], axis=1)
        keys = jnp.where(lane < HEAD_DIM, span32, turned).astype(BF16)
        values = jnp.transpose(span32)[HEAD_DIM:].astype(BF16)
        parts = []
        sinks = []
        for j in range(4):
            own = bq_own[pl.ds(start, 128), 128 * (j // 2) : 128 * (j // 2 + 1)]
            mine = (lane >= HEAD_DIM) if j % 2 else (lane < HEAD_DIM)
            parts.append(jnp.where(mine, own.astype(F32), 0.0).astype(BF16))
            sinks.append(jnp.full((1, 128), sink_in[j] * LOG2E, F32))
        queries = jnp.concatenate(parts, axis=0)
        sink = jnp.concatenate(sinks, axis=1)
        scores = lax.dot_general(keys, queries, NT, preferred_element_type=F32)
        scores = scores * (LOG2E * HEAD_DIM ** (-0.5))
        key_at = lax.broadcasted_iota(jnp.int32, (256, 512), 0)
        query_at = lax.broadcasted_iota(jnp.int32, (256, 512), 1) % 128
        first = jnp.where((s == 0) & (block == 0), 128, 0)
        allowed = (key_at > query_at) & (key_at <= query_at + WINDOW) & (key_at >= first)
        scores = jnp.where(allowed, scores, mask_fill)
        top = jnp.maximum(jnp.max(scores, axis=0, keepdims=True), sink)
        weights = jnp.exp2(scores - top)
        total = jnp.sum(weights, axis=0, keepdims=True) + jnp.exp2(sink - top)
        found = jnp.dot(values, weights.astype(BF16), preferred_element_type=F32) / total
        tall = jnp.concatenate([found[:, 128 * j : 128 * (j + 1)] for j in range(4)], axis=0)
        b_heads[pl.ds(start, 128)] = jnp.transpose(tall).astype(BF16)
        return carry

    windowed(1, 0)
    spread(3)

    @pl.when(mixed)
    def _():
        q_all(7).wait_recv()

    @pl.when(~mixed)
    def _():
        q_all(8).wait_recv()

    for pair in range(2):
        for row in range(4):
            raw = q_raw[4 * pair + row].astype(F32)
            raw = jnp.concatenate(
                [raw[g, 16 * d : 16 * (d + 1)] for d in range(2) for g in range(4)], axis=0
            )
            wide = raw * (LOG2E * HEAD_DIM ** (-0.5))
            high = wide.astype(BF16).astype(F32)
            both = jnp.transpose(jnp.concatenate([high, wide - high], axis=1))
            tall = lax.broadcasted_iota(jnp.int32, (256, 1), 0) % 128
            for m in range(2):
                mine = (tall >= HEAD_DIM) if m else (tall < HEAD_DIM)
                i = pair * 4 + (row // 2) * 2 + m
                span = slice(128 * (row % 2), 128 * (row % 2) + 128)
                q_mul[i, :, span] = jnp.where(mine, both, 0.0).astype(BF16)

    def unit(level, pair):
        keys = kv[0, level, pl.ds(2 * pair, 2)].reshape(1024, 128)
        held = kv[1, level, pl.ds(2 * pair, 2)].reshape(1024, 128)
        lookup = jnp.concatenate([held[128 * k : 128 * (k + 1)] for k in range(8)], axis=1)
        lookup = jnp.concatenate([lookup, jnp.ones((16, 1024), BF16)], axis=0)
        return jnp.concatenate([keys, keys], axis=1), lookup

    def small_unit(level, pair, two):
        rows_of = (pl.ds(2 * pair, 2), pl.ds(2 * two, 2))
        keys = kv[0, level, rows_of[0], rows_of[1]].reshape(512, 128)
        held = kv[1, level, rows_of[0], rows_of[1]].reshape(512, 128)
        lookup = jnp.concatenate([held[128 * k : 128 * (k + 1)] for k in range(4)], axis=1)
        lookup = jnp.concatenate([lookup, jnp.ones((16, 512), BF16)], axis=0)
        return jnp.concatenate([keys, keys], axis=1), lookup

    key_at = lax.broadcasted_iota(jnp.int32, (256, 256), 0)
    query_at = lax.broadcasted_iota(jnp.int32, (256, 256), 1)
    apart = 512 * (key_at // 128) + 64 * ((key_at % 128) // 16) + key_at % 16
    apart = apart - (query_at % 128) - 512 * (query_at // 128)

    def attend(level, pair, sel):
        mark = jnp.where(sel == 0, jnp.minimum(z, mate), jnp.maximum(z, mate))

        def score(keys, i):
            return [
                jnp.dot(keys[256 * k : 256 * (k + 1)], q_mul[i], preferred_element_type=F32)
                for k in range(2)
            ]

        @pl.when(level < mark)
        def _():
            keys, lookup = unit(level, pair)
            items = []
            for h in range(2):
                span = slice(512 * h, 512 * (h + 1))
                for k in range(4):
                    i = sel * 4 + k
                    items.append(
                        (i, functools.partial(score, keys[span], i), lookup[:, span])
                    )
            soft_chunk(items, mx, ls, acc)

        @pl.when(level == mark)
        def _():
            base = 128 * quarter - 32 * pair

            def hidden(keys, i):
                return [
                    jnp.where(apart <= base - 16 * k, piece, mask_fill)
                    for k, piece in enumerate(score(keys, i))
                ]

            items = []
            low = small_unit(level, pair, 0)
            high = small_unit(level, pair, 1)
            for g, (keys, lookup), rule in ((0, low, hidden), (1, low, score), (1, high, hidden)):
                for m in range(2):
                    i = sel * 4 + g * 2 + m
                    items.append((i, functools.partial(rule, keys, i), lookup))
            soft_chunk(items, mx, ls, acc)

    def step(it, carry):
        @pl.when(it == 1)
        def _():
            zrelay(1)
            zfar(0)

        @pl.when(it == 2)
        def _():
            windowed(2, 0)
            zrelay(2)
            windowed(3, 0)
            zrelay(3)

        @pl.when(it == 3)
        def _():
            zfar(1)

        @pl.when(it == 4)
        def _():
            @pl.when(s > 0)
            def _():
                rim_send.wait_recv()

            windowed(0, 0)

        @pl.when(it == 5)
        def _():
            zfar(2)
            zfar(3)

        level = jnp.where(
            it < 2, z,
            jnp.where(
                (it == 2) | (it == 5), down, jnp.where((it == 3) | (it == 6), up, far)
            ),
        )
        pair = jnp.where((it == 1) | (it >= 5), 1, 0)
        @pl.when(level <= most)
        def _():
            cross_wait(level, pair).wait_recv()

            def one(sel, inner):
                attend(level, pair, sel)
                return inner

            lax.fori_loop(0, 2, one, 0)

        return carry

    lax.fori_loop(0, 8, step, 0)

    lam_send.wait_recv()
    mixing = lam[y // 2, y % 2, 0:1, :]
    gain = gain_in[...] * head_scale

    def ret_send(pair, row):
        goal = jnp.minimum(z, mate) if pair == 0 else jnp.maximum(z, mate)
        return remote(
            stage.at[4 * pair + row], back.at[4 * (y % 2) + quarter], ret_s, ret_r,
            4 * goal + row, 2 * x + y // 2,
        )

    def ret_local(pair, row):
        return (pair == z // 2) & (row == y) & (y // 2 == c)

    for pair in range(2):
        for g in range(2):
            i = pair * 4 + g * 2
            first_mean = acc[i] / ls[i]
            second_mean = acc[i + 1] / ls[i + 1]
            gap = first_mean - mixing * second_mean
            square = jnp.mean(gap * gap, axis=0, keepdims=True)
            done = gap * lax.rsqrt(square + norm_eps)
            tall = (jnp.transpose(done) * gain).astype(BF16)
            for k in range(2):
                row = 2 * g + k
                stage[4 * pair + row] = tall[128 * k : 128 * (k + 1)]

                @pl.when(~ret_local(pair, row))
                def _(pair=pair, row=row):
                    ret_send(pair, row).start()

                @pl.when(ret_local(pair, row))
                def _(pair=pair, row=row):
                    back[4 * (y % 2) + quarter] = stage[4 * pair + row]

    def ret_all(count):
        spot = back.at[pl.ds(0, count)]
        return remote(spot, spot, ret_s, ret_r, s, other)

    @pl.when(mixed)
    def _():
        ret_all(7).wait_recv()

    @pl.when(~mixed)
    def _():
        ret_all(8).wait_recv()

    heads = jnp.concatenate(
        [back[0:4].reshape(512, 128), back[4:8].reshape(512, 128), b_heads[...]], axis=1
    )
    first, second = pl.ds(0, 32), pl.ds(32, 32)

    def cross(n):
        return remote(part.at[n, 1 - c], crossed.at[n], cr_s, cr_r.at[n], s, other)

    def far_send(n, way):
        rows = first if way == 0 else second
        return remote(
            chip.at[n, xf, rows], (far_l if way == 0 else far_r).at[n],
            fs, fr.at[n], s, right if way == 0 else left,
        )

    def near_send(n, way):
        rows = second if way == 0 else first
        return remote(
            chip.at[n, xr if way == 0 else xl, rows], (got_l if way == 0 else got_r).at[n, rows],
            gs, gr.at[n], s, right if way == 0 else left,
        )

    def sum_send(n, way):
        rows = first if way == 0 else second
        return remote(
            relayed.at[n, way], (got_l if way == 0 else got_r).at[n, rows],
            ss, gr.at[n], s, right if way == 0 else left,
        )

    def multiply(n):
        partial = jnp.dot(heads, weights[n], preferred_element_type=F32).astype(BF16)
        for col in range(8):
            part[n, col % 2, col // 2] = partial[64 * col : 64 * (col + 1)]
        cross(n).start()

    def join(n):
        cross(n).wait_recv()
        chip[n] = (part[n, c].astype(F32) + crossed[n].astype(F32)).astype(BF16)
        far_send(n, 0).start()
        far_send(n, 1).start()
        near_send(n, 0).start()
        near_send(n, 1).start()

    def pass_on(n, carry):
        remote(relayed.at[n], relayed.at[n], fs, fr.at[n], s, right).wait_recv()
        relayed[n, 0] = (chip[n, xr, first].astype(F32) + far_l[n].astype(F32)).astype(BF16)
        sum_send(n, 0).start()
        relayed[n, 1] = (chip[n, xl, second].astype(F32) + far_r[n].astype(F32)).astype(BF16)
        sum_send(n, 1).start()
        return carry

    remote(weights, weights, gs, w_s, s, other).wait_recv()
    multiply(0)

    def run(n, carry):
        multiply(n)
        join(n - 1)
        return carry

    lax.fori_loop(1, NC, run, 0)
    join(NC - 1)
    def drained(spot, sem):
        remote(spot, spot, sem, q_r, s, other).wait_send()

    drained(rows.at[0], os)
    drained(x_in, xs)
    drained(rows.at[pl.ds(0, 2)], xds)
    @pl.when(z == 3)
    def _():
        drained(kv.at[0, 0], zs)
        drained(kv.at[0, 0], rs)
        drained(kv.at[0, 0, pl.ds(0, 2)], rs)

    @pl.when(z < 3)
    def _():
        drained(kv.at[0, pl.ds(0, 2)], zs)
        drained(kv.at[0, 0, pl.ds(0, 2)], rs)

    @pl.when((z == 0) | (z == 3))
    def _():
        drained(kv.at[0], ds)

    @pl.when((z == 1) | (z == 2))
    def _():
        drained(kv.at[0, pl.ds(0, 3)], ds)

    lam_send.wait_send()

    @pl.when(s < 15)
    def _():
        rim_send.wait_send()

    @pl.when(mixed)
    def _():
        drained(kv.at[0, 0, pl.ds(0, 3)], a2a_s)
        q_all(7).wait_send()
        ret_all(7).wait_send()

    @pl.when(~mixed)
    def _():
        drained(kv.at[0, 0], a2a_s)
        q_all(8).wait_send()
        ret_all(8).wait_send()

    lax.fori_loop(0, NC, pass_on, 0)

    drained(crossed, cr_s)
    drained(relayed, fs)
    drained(relayed, gs)
    for n in range(NC):
        spot = chip.at[n, pl.ds(0, 2)]
        remote(spot, spot, ss, gr.at[n], s, other).wait_recv()
        total = chip[n, x].astype(F32) + got_l[n].astype(F32) + got_r[n].astype(F32)
        out_v[n] = total.astype(BF16)
        pltpu.make_async_copy(out_v.at[n], out.at[:, pl.ds(n * CW, CW)], out_s).start()
    drained(relayed, ss)
    pltpu.make_async_copy(x_in, out, out_s).wait()


def layer(*operands):
    vmem = pl.BlockSpec(memory_space=VMEM)
    hbm = pl.BlockSpec(memory_space=pltpu.HBM)
    smem = pl.BlockSpec(memory_space=pltpu.SMEM)
    dma = pltpu.SemaphoreType.DMA
    return pl.pallas_call(
        layer_kernel,
        out_shape=jax.ShapeDtypeStruct((64, 4096), BF16),
        in_specs=[hbm] * 7 + [smem, vmem, smem] + [hbm] * 2,
        out_specs=hbm,
        scratch_shapes=[
            VMEM((NC, 64, CW), BF16),
            VMEM((64, 4096), BF16),
            VMEM((4, 8, 16, 4096), BF16),
            VMEM((4096, 768), BF16), VMEM((4096, 256), BF16), VMEM((128, 4096), BF16),
            VMEM((2, 4, 128, 128), BF16), VMEM((2, 2, 4, 128, 128), BF16), VMEM((512, 256), BF16),
            VMEM((2, 4, 4, 4, 128, 128), BF16),
            VMEM((8, 4, 32, 128), BF16),
            VMEM((8, 256, 256), BF16),
            VMEM((640, 128), BF16),
            VMEM((2, 2, 8, 256), F32),
            VMEM((8, 128, 256), F32),
            VMEM((8, 1, 256), F32),
            VMEM((8, 1, 256), F32),
            VMEM((8, 128, 128), BF16),
            VMEM((8, 128, 128), BF16),
            VMEM((512, 256), BF16),
            VMEM((NC, 512, CW), BF16),
            VMEM((NC, 2, 4, 64, CW), BF16),
            VMEM((NC, 4, 64, CW), BF16),
            VMEM((NC, 4, 64, CW), BF16),
            VMEM((NC, 32, CW), BF16),
            VMEM((NC, 32, CW), BF16),
            VMEM((NC, 64, CW), BF16),
            VMEM((NC, 64, CW), BF16),
            VMEM((NC, 2, 32, CW), BF16),
            dma, dma, dma((6,)), dma, dma((4, 2, 2)), dma, dma((4,)), dma, dma((4,)),
            dma, dma((4,)), dma, dma((4, 2)), dma, dma((4,)), dma, dma((4, 2)),
            dma, dma, dma((2,)), dma((2,)), dma, dma,
            dma, dma, dma((NC,)), dma, dma((NC,)), dma, dma, dma((NC,)),
        ],
        compiler_params=pltpu.CompilerParams(
            collective_id=0, has_side_effects=True, vmem_limit_bytes=56 * 2**20
        ),
        name="layer",
    )(*operands)


def shards(
    inputs,
    a_query_w,
    a_key_w,
    a_value_w,
    b_query_w,
    b_key_w,
    b_value_w,
    head_lambda,
    head_gain,
    sink_logit,
    a_out_w,
    b_out_w,
):
    return layer(
        inputs, a_query_w, a_key_w, a_value_w, b_query_w, b_key_w.T, b_value_w.T,
        head_lambda, head_gain[None], sink_logit, a_out_w, b_out_w,
    )


def solution(mesh):
    return jax.shard_map(
        shards,
        mesh=mesh,
        in_specs=(
            P(("sp", "tp"), None),
            P(None, "tp"),
            P(None, "tp"),
            P(None, "tp"),
            P(None, "tp"),
            P(None, "tp"),
            P(None, "tp"),
            P("tp"),
            P(),
            P("tp"),
            P("tp", None),
            P("tp", None),
        ),
        out_specs=P(("sp", "tp"), None),
        check_vma=False,
    )
```

```python
import functools

import jax
import jax.numpy as jnp
from jax import lax
from jax.experimental import pallas as pl
from jax.experimental.pallas import tpu as pltpu
from jax.sharding import PartitionSpec as P

HEAD_DIM = 64
VALUE_DIM = 128
WINDOW = 128

norm_eps = 0.0001
head_scale = 0.8
mask_fill = -1e30

MESH = pl.DeviceIdType.MESH
NT = (((1,), (1,)), ((), ()))
LOG2E = 1.4426950408889634
VMEM = pltpu.VMEM
F32 = jnp.float32
BF16 = jnp.bfloat16


def remote(src, dst, send_sem, recv_sem, row, col):
    return pltpu.make_async_remote_copy(
        src_ref=src,
        dst_ref=dst,
        send_sem=send_sem,
        recv_sem=recv_sem,
        device_id=(row, col),
        device_id_type=MESH,
    )


def soft_chunk(items, mx, ls, acc):
    def weights(i, pieces):
        before = mx[i]
        top = before
        for piece in pieces:
            top = jnp.maximum(top, jnp.max(piece, axis=0, keepdims=True))
        shrink = jnp.exp2(before - top)
        mx[i] = top
        return shrink, [jnp.exp2(piece - top).astype(BF16) for piece in pieces]

    def collect(i, lookup, shrink, pieces):
        got = jnp.dot(lookup, jnp.concatenate(pieces, axis=0), preferred_element_type=F32)
        acc[i] = acc[i] * shrink + got[:VALUE_DIM]
        ls[i] = ls[i] * shrink + got[VALUE_DIM : VALUE_DIM + 1]

    now = items[0][1]()
    held = None
    for at, (i, _, lookup) in enumerate(items):
        later = items[at + 1][1]() if at + 1 < len(items) else None
        current = (i, lookup, *weights(i, now))
        if held is not None:
            collect(*held)
        held, now = current, later
    collect(*held)


NC = 8
CW = 512
GROUPS = 4


def layer_kernel(
    x_hbm, wq_in, wk_in, wv_in, wbq_in, wbk_in, wbv_in, few_in, aw_in, bw_in,
    out,
    x_in, rows, wa, wbq, wbkv, q_own, kv_own, bq_own,
    kv, q_raw, q_mul, near, lam, acc, mx, ls, stage, back, b_heads,
    weights, part, crossed, chip, far_l, far_r, got_l, got_r, relayed,
    x_s, pw_s, os, orr, xs, xr_s, xds, xdr,
    a2a_s, a2a_r, zs, zr, rs, rr, ds, dr, q_s, q_r, small_s, small_r, ret_s, ret_r,
    w_s, cr_s, cr_r, fs, fr, gs, ss, gr,
):
    s, t = lax.axis_index("sp"), lax.axis_index("tp")
    z, y = s // 4, s % 4
    x, c = t // 2, t % 2
    xr, xl, xf = (x + 1) % 4, (x + 3) % 4, (x + 2) % 4
    other, right, left = 2 * x + 1 - c, 2 * xr + c, 2 * xl + c
    beyond = 2 * xf + c
    up, down = (z + 1) % 4, (z + 3) % 4
    far = (z + 2) % 4
    mate = 3 - z
    side = z + 1 - 2 * (z % 2)
    quarter = 2 * c + z // 2
    most = jnp.maximum(z, mate)
    lane = lax.broadcasted_iota(jnp.int32, (1, 128), 1)

    x_load = pltpu.make_async_copy(x_hbm, x_in, x_s)
    x_load.start()
    mixed = y // 2 == c
    loads = [
        pltpu.make_async_copy(wq_in, wa.at[:, pl.ds(0, 256)], pw_s.at[2]),
        pltpu.make_async_copy(wk_in, wa.at[:, pl.ds(256, 256)], pw_s.at[0]),
        pltpu.make_async_copy(wv_in, wa.at[:, pl.ds(512, 256)], pw_s.at[1]),
        pltpu.make_async_copy(wbq_in, wbq, pw_s.at[3]),
        pltpu.make_async_copy(wbk_in, wbkv.at[pl.ds(0, 64)], pw_s.at[4]),
        pltpu.make_async_copy(wbv_in, wbkv.at[pl.ds(64, 64)], pw_s.at[5]),
    ]

    def fetch(n, which):
        columns = pl.ds(pl.multiple_of(n * CW, CW), CW)
        source = aw_in if which == 0 else bw_in
        return pltpu.make_async_copy(
            source.at[:, columns], weights.at[n, pl.ds(256 * which, 256)], w_s
        )

    barrier = pltpu.get_barrier_semaphore()

    def greet(row, col):
        pl.semaphore_signal(barrier, inc=1, device_id=(row, col), device_id_type=MESH)

    for j in range(4):
        for core in range(2):
            if j == 0:
                @pl.when(core != c)
                def _(core=core):
                    greet(4 * z + y, 2 * x + core)
            else:
                greet(4 * z + (y + j) % 4, 2 * x + core)
            greet(4 * mate + (y + j) % 4, 2 * x + core)
    greet(4 * side + y, t)
    greet(s, right)
    greet(s, left)
    rim_up = (y == 3) & (z % 2 == 0)
    rim_down = (y == 0) & (z % 2 == 1)

    @pl.when(rim_up)
    def _():
        greet(s + 1, t)

    @pl.when(rim_down)
    def _():
        greet(s - 1, t)

    x_load.wait()
    for load in loads:
        load.start()
    pl.semaphore_wait(barrier, 18 + jnp.where(rim_up | rim_down, 1, 0))

    halves = (pl.ds(0, 2048), pl.ds(2048, 2048))
    every = pl.ds(0, 16)

    def mine16(g):
        return pl.ds(pl.multiple_of(16 * g, 16), 16)

    def own_send(g, way, which):
        return remote(
            x_in.at[mine16(g), halves[which]], rows.at[g, t, every, halves[which]],
            os, orr.at[g, way, which], s, right if way == 0 else left,
        )

    def own_wait(g, way, which):
        spot = rows.at[g, left if way == 0 else right, every, halves[which]]
        return remote(
            spot, spot, os, orr.at[g, way, which],
            s, right if way == 0 else left,
        )

    def xrelay_send(g, way):
        spot = rows.at[g, left if way == 0 else right, every, halves[way]]
        return remote(spot, spot, xs, xr_s.at[g], s, right if way == 0 else left)

    def xrelay_wait(g):
        spot = rows.at[g, beyond]
        return remote(spot, spot, xs, xr_s.at[g], s, right)

    def own_cross(g):
        return remote(x_in.at[mine16(g)], rows.at[g, t], xds, xdr.at[g], s, other)

    def xcross(g, where):
        spot = rows.at[g, 2 * where + c]
        return remote(spot, spot, xds, xdr.at[g], s, other)

    def xcross_wait(g):
        spot = rows.at[g, pl.ds(0, 4)]
        return remote(spot, spot, xds, xdr.at[g], s, other)

    def own_start(g):
        own_send(g, 0, 0).start()
        own_send(g, 1, 1).start()
        own_send(g, 0, 1).start()
        own_send(g, 1, 0).start()
        own_cross(g).start()

    def kv_send(g, head, part_of):
        return remote(
            kv_own.at[head, part_of, g], kv.at[part_of, z, g, y],
            a2a_s, a2a_r.at[g],
            4 * z + 2 * c + head, 2 * x + part_of,
        )

    def kv_local(head, part_of):
        return (2 * c + head == y) & (part_of == c)

    def a2a_wait(g, count):
        spot = kv.at[c, z, g, pl.ds(0, count)]
        return remote(spot, spot, a2a_s, a2a_r.at[g], s, other)

    def z_send(g, way):
        spot = kv.at[c, z, g]
        return remote(spot, spot, zs, zr.at[g, way], 4 * (up, down)[way] + y, t)

    def z_wait(g, way):
        spot = kv.at[c, (down, up)[way], g]
        return remote(spot, spot, zs, zr.at[g, way], 4 * (up, down)[way] + y, t)

    def relay_send(g, way):
        spot = kv.at[c, (down, up)[way], g, pl.ds(2 * way, 2)]
        return remote(spot, spot, rs, rr.at[g], 4 * (up, down)[way] + y, t)

    def relay_whole(g):
        spot = kv.at[c, up, g]
        return remote(spot, spot, rs, rr.at[g], 4 * down + y, t)

    def relay_wait(g):
        spot = kv.at[c, far, g]
        return remote(spot, spot, rs, rr.at[g], 4 * up + y, t)

    def cross_send(level, g):
        spot = kv.at[c, level, g]
        return remote(spot, spot, ds, dr.at[level, g // 2], s, other)

    def cross_wait(level, pair):
        spot = kv.at[1 - c, level, pl.ds(2 * pair, 2)]
        return remote(spot, spot, ds, dr.at[level, pair], s, other)

    def spread(g):
        @pl.when(mixed)
        def _():
            a2a_wait(g, 3).wait_recv()

        @pl.when(~mixed)
        def _():
            a2a_wait(g, 4).wait_recv()

        z_send(g, 0).start()

        @pl.when(z < 3)
        def _():
            z_send(g, 1).start()

        cross_send(z, g).start()

    def zrelay(g):
        z_wait(g, 0).wait_recv()

        @pl.when(z >= 2)
        def _():
            relay_send(g, 0).start()

        cross_send(down, g).start()

        @pl.when(z != 2)
        def _():
            z_wait(g, 1).wait_recv()

            @pl.when(z == 3)
            def _():
                relay_whole(g).start()

            @pl.when(z < 2)
            def _():
                relay_send(g, 1).start()

            cross_send(up, g).start()

    def zfar(g):
        @pl.when(z != 1)
        def _():
            relay_wait(g).wait_recv()
            cross_send(far, g).start()

    own_start(0)
    own_start(1)
    lam_send = remote(lam.at[c], lam.at[c], small_s.at[0], small_r.at[0], s, other)
    for g in range(GROUPS):
        rows[g, t] = x_in[16 * g : 16 * (g + 1)]
    for head in range(2):
        lam[c, head] = jnp.broadcast_to(few_in[0:1, head : head + 1], (8, 256))
    acc[...] = jnp.zeros_like(acc)
    ls[...] = jnp.zeros_like(ls)
    mx[...] = jnp.full_like(mx, mask_fill)

    @pl.when(s == 0)
    def _():
        near[pl.ds(0, 128)] = jnp.zeros((128, 128), BF16)

    def near_rows(g):
        own_wait(g, 0, 0).wait_recv()
        xrelay_send(g, 0).start()
        own_wait(g, 1, 1).wait_recv()
        xrelay_send(g, 1).start()

        @pl.when(g < GROUPS - 2)
        def _():
            own_start(g + 2)

        own_wait(g, 0, 1).wait_recv()
        xcross(g, xl).start()
        own_wait(g, 1, 0).wait_recv()
        xcross(g, xr).start()

    near_rows(0)
    near_rows(1)

    def far_rows(g):
        xrelay_wait(g).wait_recv()
        xcross(g, xf).start()

    def project_b(at, count):
        block = rows[at : at + count].reshape(128 * count, 4096)
        b_queries = jnp.dot(block, wbq[...], preferred_element_type=F32).astype(BF16)
        b_pair = lax.dot_general(block, wbkv[...], NT, preferred_element_type=F32).astype(BF16)
        for k in range(count):
            for d in range(8):
                first_row = 64 * d + 16 * (at + k)
                take = slice(128 * k + 16 * d, 128 * k + 16 * (d + 1))
                bq_own[first_row : first_row + 16] = b_queries[take]
                near[first_row + 128 : first_row + 144] = b_pair[take]

    def gather(g, carry):
        @pl.when(g == 0)
        def _():
            far_rows(0)
            near_rows(2)

        @pl.when(g == 1)
        def _():
            far_rows(1)

        @pl.when(g == 2)
        def _():
            near_rows(3)
            spread(0)
            far_rows(2)

        @pl.when(g == 3)
        def _():
            spread(1)
            far_rows(3)

        @pl.when(g == 0)
        def _():
            for load in loads[:3]:
                load.wait()

        xcross_wait(g).wait_recv()
        block = rows[g].reshape(128, 4096)
        found = jnp.dot(block, wa[...], preferred_element_type=F32)
        q_own[0, g] = found[:, :128].astype(BF16)
        q_own[1, g] = found[:, 128:256].astype(BF16)
        keys, values = found[:, 256:512], found[:, 512:]
        for head in range(2):
            lanes = slice(128 * head, 128 * (head + 1))
            kv_own[head, 0, g] = keys[:, lanes].astype(BF16)
            kv_own[head, 1, g] = jnp.transpose(values[:, lanes]).astype(BF16)

            @pl.when(2 * c + head == y)
            def _(head=head):
                kv[c, z, g, y] = kv_own[head, c, g]

            for part_of in range(2):
                @pl.when(~kv_local(head, part_of))
                def _(head=head, part_of=part_of):
                    kv_send(g, head, part_of).start()

        send_queries(g)

        @pl.when(g == 0)
        def _():
            for n in range(NC):
                fetch(n, 0).start()
                fetch(n, 1).start()
            for load in loads[3:]:
                load.wait()
            project_b(0, 1)

        return carry

    def q_send(g, head, k, core):
        goal = z if k == 0 else mate
        return remote(
            q_own.at[head, g, pl.ds(32 * (2 * core + goal // 2), 32)],
            q_raw.at[4 * (z // 2) + y, g], q_s, q_r,
            4 * goal + 2 * c + head, 2 * x + core,
        )

    def q_local(head, k, core):
        return (2 * c + head == y) & (core == c) & (k == 0)

    def send_queries(g):
        for head in range(2):
            for k in range(2):
                for core in range(2):
                    @pl.when(~q_local(head, k, core))
                    def _(head=head, k=k, core=core):
                        q_send(g, head, k, core).start()

            @pl.when(2 * c + head == y)
            def _(head=head):
                q_raw[4 * (z // 2) + y, g] = q_own[head, g, pl.ds(32 * quarter, 32)]

    def q_all(count):
        spot = q_raw.at[pl.ds(0, count)]
        return remote(spot, spot, q_s, q_r, s, other)

    lam_send.start()
    lax.fori_loop(0, GROUPS, gather, 0)
    project_b(1, 1)
    spread(2)
    project_b(2, 2)
    zrelay(0)

    rim_send = remote(
        near.at[pl.ds(512, 128)], near.at[pl.ds(0, 128)], small_s.at[1], small_r.at[1],
        jnp.minimum(s + 1, 15), t,
    )

    @pl.when(s < 15)
    def _():
        rim_send.start()

    def windowed(block, carry):
        start = pl.multiple_of(block * 128, 128)
        span = near[pl.ds(start, 256)]
        span32 = span.astype(F32)
        turned = jnp.concatenate([span32[:, HEAD_DIM:], span32[:, :HEAD_DIM]], axis=1)
        keys = jnp.where(lane < HEAD_DIM, span32, turned).astype(BF16)
        values = jnp.transpose(span32)[HEAD_DIM:].astype(BF16)
        parts = []
        sinks = []
        for j in range(4):
            own = bq_own[pl.ds(start, 128), 128 * (j // 2) : 128 * (j // 2 + 1)]
            mine = (lane >= HEAD_DIM) if j % 2 else (lane < HEAD_DIM)
            parts.append(jnp.where(mine, own.astype(F32), 0.0).astype(BF16))
            sinks.append(jnp.broadcast_to(few_in[0:1, 2 + j : 3 + j] * LOG2E, (1, 128)))
        queries = jnp.concatenate(parts, axis=0)
        sink = jnp.concatenate(sinks, axis=1)
        scores = lax.dot_general(keys, queries, NT, preferred_element_type=F32)
        scores = scores * (LOG2E * HEAD_DIM ** (-0.5))
        key_at = lax.broadcasted_iota(jnp.int32, (256, 512), 0)
        query_at = lax.broadcasted_iota(jnp.int32, (256, 512), 1) % 128
        first = jnp.where((s == 0) & (block == 0), 128, 0)
        allowed = (key_at > query_at) & (key_at <= query_at + WINDOW) & (key_at >= first)
        scores = jnp.where(allowed, scores, mask_fill)
        top = jnp.maximum(jnp.max(scores, axis=0, keepdims=True), sink)
        weights = jnp.exp2(scores - top)
        total = jnp.sum(weights, axis=0, keepdims=True) + jnp.exp2(sink - top)
        found = jnp.dot(values, weights.astype(BF16), preferred_element_type=F32) / total
        tall = jnp.concatenate([found[:, 128 * j : 128 * (j + 1)] for j in range(4)], axis=0)
        b_heads[pl.ds(start, 128)] = jnp.transpose(tall).astype(BF16)
        return carry

    windowed(1, 0)
    spread(3)

    @pl.when(mixed)
    def _():
        q_all(7).wait_recv()

    @pl.when(~mixed)
    def _():
        q_all(8).wait_recv()

    for pair in range(2):
        for row in range(4):
            raw = q_raw[4 * pair + row].astype(F32)
            raw = jnp.concatenate(
                [raw[g, 16 * d : 16 * (d + 1)] for d in range(2) for g in range(4)], axis=0
            )
            wide = raw * (LOG2E * HEAD_DIM ** (-0.5))
            high = wide.astype(BF16).astype(F32)
            both = jnp.transpose(jnp.concatenate([high, wide - high], axis=1))
            tall = lax.broadcasted_iota(jnp.int32, (256, 1), 0) % 128
            for m in range(2):
                mine = (tall >= HEAD_DIM) if m else (tall < HEAD_DIM)
                i = pair * 4 + (row // 2) * 2 + m
                span = slice(128 * (row % 2), 128 * (row % 2) + 128)
                q_mul[i, :, span] = jnp.where(mine, both, 0.0).astype(BF16)

    def unit(level, pair):
        keys = kv[0, level, pl.ds(2 * pair, 2)].reshape(1024, 128)
        held = kv[1, level, pl.ds(2 * pair, 2)].reshape(1024, 128)
        lookup = jnp.concatenate([held[128 * k : 128 * (k + 1)] for k in range(8)], axis=1)
        lookup = jnp.concatenate([lookup, jnp.ones((16, 1024), BF16)], axis=0)
        return jnp.concatenate([keys, keys], axis=1), lookup

    def small_unit(level, pair, two):
        rows_of = (pl.ds(2 * pair, 2), pl.ds(2 * two, 2))
        keys = kv[0, level, rows_of[0], rows_of[1]].reshape(512, 128)
        held = kv[1, level, rows_of[0], rows_of[1]].reshape(512, 128)
        lookup = jnp.concatenate([held[128 * k : 128 * (k + 1)] for k in range(4)], axis=1)
        lookup = jnp.concatenate([lookup, jnp.ones((16, 512), BF16)], axis=0)
        return jnp.concatenate([keys, keys], axis=1), lookup

    key_at = lax.broadcasted_iota(jnp.int32, (256, 256), 0)
    query_at = lax.broadcasted_iota(jnp.int32, (256, 256), 1)
    apart = 512 * (key_at // 128) + 64 * ((key_at % 128) // 16) + key_at % 16
    apart = apart - (query_at % 128) - 512 * (query_at // 128)

    def attend(level, pair, sel):
        mark = jnp.where(sel == 0, jnp.minimum(z, mate), jnp.maximum(z, mate))

        def score(keys, i):
            return [
                jnp.dot(keys[256 * k : 256 * (k + 1)], q_mul[i], preferred_element_type=F32)
                for k in range(2)
            ]

        @pl.when(level < mark)
        def _():
            keys, lookup = unit(level, pair)
            items = []
            for h in range(2):
                span = slice(512 * h, 512 * (h + 1))
                for k in range(4):
                    i = sel * 4 + k
                    items.append(
                        (i, functools.partial(score, keys[span], i), lookup[:, span])
                    )
            soft_chunk(items, mx, ls, acc)

        @pl.when(level == mark)
        def _():
            base = 128 * quarter - 32 * pair

            def hidden(keys, i):
                return [
                    jnp.where(apart <= base - 16 * k, piece, mask_fill)
                    for k, piece in enumerate(score(keys, i))
                ]

            items = []
            low = small_unit(level, pair, 0)
            high = small_unit(level, pair, 1)
            for g, (keys, lookup), rule in ((0, low, hidden), (1, low, score), (1, high, hidden)):
                for m in range(2):
                    i = sel * 4 + g * 2 + m
                    items.append((i, functools.partial(rule, keys, i), lookup))
            soft_chunk(items, mx, ls, acc)

    def step(it, carry):
        @pl.when(it == 1)
        def _():
            zrelay(1)
            zfar(0)

        @pl.when(it == 2)
        def _():
            windowed(2, 0)
            zrelay(2)
            windowed(3, 0)
            zrelay(3)

        @pl.when(it == 3)
        def _():
            zfar(1)

        @pl.when(it == 4)
        def _():
            @pl.when(s > 0)
            def _():
                rim_send.wait_recv()

            windowed(0, 0)

        @pl.when(it == 5)
        def _():
            zfar(2)
            zfar(3)

        level = jnp.where(
            it < 2, z,
            jnp.where(
                (it == 2) | (it == 5), down, jnp.where((it == 3) | (it == 6), up, far)
            ),
        )
        pair = jnp.where((it == 1) | (it >= 5), 1, 0)
        @pl.when(level <= most)
        def _():
            cross_wait(level, pair).wait_recv()

            def one(sel, inner):
                attend(level, pair, sel)
                return inner

            lax.fori_loop(0, 2, one, 0)

        return carry

    lax.fori_loop(0, 8, step, 0)

    lam_send.wait_recv()
    mixing = lam[y // 2, y % 2, 0:1, :]
    gain = few_in[:, 128:256] * head_scale

    def ret_send(pair, row):
        goal = jnp.minimum(z, mate) if pair == 0 else jnp.maximum(z, mate)
        return remote(
            stage.at[4 * pair + row], back.at[4 * (y % 2) + quarter], ret_s, ret_r,
            4 * goal + row, 2 * x + y // 2,
        )

    def ret_local(pair, row):
        return (pair == z // 2) & (row == y) & (y // 2 == c)

    for pair in range(2):
        for g in range(2):
            i = pair * 4 + g * 2
            first_mean = acc[i] / ls[i]
            second_mean = acc[i + 1] / ls[i + 1]
            gap = first_mean - mixing * second_mean
            square = jnp.mean(gap * gap, axis=0, keepdims=True)
            done = gap * lax.rsqrt(square + norm_eps)
            tall = (jnp.transpose(done) * gain).astype(BF16)
            for k in range(2):
                row = 2 * g + k
                stage[4 * pair + row] = tall[128 * k : 128 * (k + 1)]

                @pl.when(~ret_local(pair, row))
                def _(pair=pair, row=row):
                    ret_send(pair, row).start()

                @pl.when(ret_local(pair, row))
                def _(pair=pair, row=row):
                    back[4 * (y % 2) + quarter] = stage[4 * pair + row]

    def ret_all(count):
        spot = back.at[pl.ds(0, count)]
        return remote(spot, spot, ret_s, ret_r, s, other)

    @pl.when(mixed)
    def _():
        ret_all(7).wait_recv()

    @pl.when(~mixed)
    def _():
        ret_all(8).wait_recv()

    heads = jnp.concatenate(
        [back[0:4].reshape(512, 128), back[4:8].reshape(512, 128), b_heads[...]], axis=1
    )
    first, second = pl.ds(0, 32), pl.ds(32, 32)

    def cross(n):
        return remote(part.at[n, 1 - c], crossed.at[n], cr_s, cr_r.at[n], s, other)

    def far_send(n, way):
        rows = first if way == 0 else second
        return remote(
            chip.at[n, xf, rows], (far_l if way == 0 else far_r).at[n],
            fs, fr.at[n], s, right if way == 0 else left,
        )

    def near_send(n, way):
        rows = second if way == 0 else first
        return remote(
            chip.at[n, xr if way == 0 else xl, rows], (got_l if way == 0 else got_r).at[n, rows],
            gs, gr.at[n], s, right if way == 0 else left,
        )

    def sum_send(n, way):
        rows = first if way == 0 else second
        return remote(
            relayed.at[n, way], (got_l if way == 0 else got_r).at[n, rows],
            ss, gr.at[n], s, right if way == 0 else left,
        )

    def multiply(n):
        partial = jnp.dot(heads, weights[n], preferred_element_type=F32).astype(BF16)
        for col in range(8):
            part[n, col % 2, col // 2] = partial[64 * col : 64 * (col + 1)]
        cross(n).start()

    def join(n):
        cross(n).wait_recv()
        chip[n] = (part[n, c].astype(F32) + crossed[n].astype(F32)).astype(BF16)
        far_send(n, 0).start()
        far_send(n, 1).start()
        near_send(n, 0).start()
        near_send(n, 1).start()

    def pass_on(n, carry):
        remote(relayed.at[n], relayed.at[n], fs, fr.at[n], s, right).wait_recv()
        relayed[n, 0] = (chip[n, xr, first].astype(F32) + far_l[n].astype(F32)).astype(BF16)
        sum_send(n, 0).start()
        relayed[n, 1] = (chip[n, xl, second].astype(F32) + far_r[n].astype(F32)).astype(BF16)
        sum_send(n, 1).start()
        return carry

    remote(weights, weights, gs, w_s, s, other).wait_recv()
    multiply(0)

    def run(n, carry):
        multiply(n)
        join(n - 1)
        return carry

    lax.fori_loop(1, NC, run, 0)
    join(NC - 1)
    def drained(spot, sem):
        remote(spot, spot, sem, q_r, s, other).wait_send()

    drained(rows.at[0], os)
    drained(x_in, xs)
    drained(rows.at[pl.ds(0, 2)], xds)
    @pl.when(z == 3)
    def _():
        drained(kv.at[0, 0], zs)
        drained(kv.at[0, 0], rs)
        drained(kv.at[0, 0, pl.ds(0, 2)], rs)

    @pl.when(z < 3)
    def _():
        drained(kv.at[0, pl.ds(0, 2)], zs)
        drained(kv.at[0, 0, pl.ds(0, 2)], rs)

    @pl.when((z == 0) | (z == 3))
    def _():
        drained(kv.at[0], ds)

    @pl.when((z == 1) | (z == 2))
    def _():
        drained(kv.at[0, pl.ds(0, 3)], ds)

    lam_send.wait_send()

    @pl.when(s < 15)
    def _():
        rim_send.wait_send()

    @pl.when(mixed)
    def _():
        drained(kv.at[0, 0, pl.ds(0, 3)], a2a_s)
        q_all(7).wait_send()
        ret_all(7).wait_send()

    @pl.when(~mixed)
    def _():
        drained(kv.at[0, 0], a2a_s)
        q_all(8).wait_send()
        ret_all(8).wait_send()

    lax.fori_loop(0, NC, pass_on, 0)

    drained(crossed, cr_s)
    drained(relayed, fs)
    drained(relayed, gs)
    for n in range(NC):
        spot = chip.at[n, pl.ds(0, 2)]
        remote(spot, spot, ss, gr.at[n], s, other).wait_recv()
        total = chip[n, x].astype(F32) + got_l[n].astype(F32) + got_r[n].astype(F32)
        out[:, n * CW : (n + 1) * CW] = total.astype(BF16)
    drained(relayed, ss)


def layer(*operands):
    vmem = pl.BlockSpec(memory_space=VMEM)
    hbm = pl.BlockSpec(memory_space=pltpu.HBM)
    dma = pltpu.SemaphoreType.DMA
    return pl.pallas_call(
        layer_kernel,
        out_shape=jax.ShapeDtypeStruct((64, 4096), BF16),
        in_specs=[hbm] * 7 + [vmem] + [hbm] * 2,
        out_specs=vmem,
        scratch_shapes=[
            VMEM((64, 4096), BF16),
            VMEM((4, 8, 16, 4096), BF16),
            VMEM((4096, 768), BF16), VMEM((4096, 256), BF16), VMEM((128, 4096), BF16),
            VMEM((2, 4, 128, 128), BF16), VMEM((2, 2, 4, 128, 128), BF16), VMEM((512, 256), BF16),
            VMEM((2, 4, 4, 4, 128, 128), BF16),
            VMEM((8, 4, 32, 128), BF16),
            VMEM((8, 256, 256), BF16),
            VMEM((640, 128), BF16),
            VMEM((2, 2, 8, 256), F32),
            VMEM((8, 128, 256), F32),
            VMEM((8, 1, 256), F32),
            VMEM((8, 1, 256), F32),
            VMEM((8, 128, 128), BF16),
            VMEM((8, 128, 128), BF16),
            VMEM((512, 256), BF16),
            VMEM((NC, 512, CW), BF16),
            VMEM((NC, 2, 4, 64, CW), BF16),
            VMEM((NC, 4, 64, CW), BF16),
            VMEM((NC, 4, 64, CW), BF16),
            VMEM((NC, 32, CW), BF16),
            VMEM((NC, 32, CW), BF16),
            VMEM((NC, 64, CW), BF16),
            VMEM((NC, 64, CW), BF16),
            VMEM((NC, 2, 32, CW), BF16),
            dma, dma((6,)), dma, dma((4, 2, 2)), dma, dma((4,)), dma, dma((4,)),
            dma, dma((4,)), dma, dma((4, 2)), dma, dma((4,)), dma, dma((4, 2)),
            dma, dma, dma((2,)), dma((2,)), dma, dma,
            dma, dma, dma((NC,)), dma, dma((NC,)), dma, dma, dma((NC,)),
        ],
        compiler_params=pltpu.CompilerParams(
            collective_id=0, has_side_effects=True, vmem_limit_bytes=int(53.2 * 2**20)
        ),
        name="layer",
    )(*operands)


def shards(
    inputs,
    a_query_w,
    a_key_w,
    a_value_w,
    b_query_w,
    b_key_w,
    b_value_w,
    head_lambda,
    head_gain,
    sink_logit,
    a_out_w,
    b_out_w,
):
    few = jnp.concatenate([head_lambda, sink_logit, jnp.zeros((122,), F32), head_gain])[None]
    return layer(
        inputs, a_query_w, a_key_w, a_value_w, b_query_w, b_key_w.T, b_value_w.T,
        few, a_out_w, b_out_w,
    )


def solution(mesh):
    return jax.shard_map(
        shards,
        mesh=mesh,
        in_specs=(
            P(("sp", "tp"), None),
            P(None, "tp"),
            P(None, "tp"),
            P(None, "tp"),
            P(None, "tp"),
            P(None, "tp"),
            P(None, "tp"),
            P("tp"),
            P(),
            P("tp"),
            P("tp", None),
            P("tp", None),
        ),
        out_specs=P(("sp", "tp"), None),
        check_vma=False,
    )
```

```python
import functools

import jax
import jax.numpy as jnp
from jax import lax
from jax.experimental import pallas as pl
from jax.experimental.pallas import tpu as pltpu
from jax.sharding import PartitionSpec as P

HEAD_DIM = 64
VALUE_DIM = 128
WINDOW = 128

norm_eps = 0.0001
head_scale = 0.8
mask_fill = -1e30

MESH = pl.DeviceIdType.MESH
NT = (((1,), (1,)), ((), ()))
LOG2E = 1.4426950408889634
VMEM = pltpu.VMEM
F32 = jnp.float32
BF16 = jnp.bfloat16


def remote(src, dst, send_sem, recv_sem, row, col):
    return pltpu.make_async_remote_copy(
        src_ref=src,
        dst_ref=dst,
        send_sem=send_sem,
        recv_sem=recv_sem,
        device_id=(row, col),
        device_id_type=MESH,
    )


def soft_chunk(items, mx, ls, acc):
    def weights(i, pieces):
        before = mx[i]
        top = before
        for piece in pieces:
            top = jnp.maximum(top, jnp.max(piece, axis=0, keepdims=True))
        shrink = jnp.exp2(before - top)
        mx[i] = top
        return shrink, [jnp.exp2(piece - top).astype(BF16) for piece in pieces]

    def collect(i, lookup, shrink, pieces):
        got = jnp.dot(lookup, jnp.concatenate(pieces, axis=0), preferred_element_type=F32)
        acc[i] = acc[i] * shrink + got[:VALUE_DIM]
        ls[i] = ls[i] * shrink + got[VALUE_DIM : VALUE_DIM + 1]

    now = items[0][1]()
    held = None
    for at, (i, _, lookup) in enumerate(items):
        later = items[at + 1][1]() if at + 1 < len(items) else None
        current = (i, lookup, *weights(i, now))
        if held is not None:
            collect(*held)
        held, now = current, later
    collect(*held)


NC = 8
CW = 512
GROUPS = 4


def layer_kernel(
    x_hbm, wq_in, wk_in, wv_in, wbq_in, wbk_in, wbv_in, few_in, aw_in, bw_in,
    out,
    x_in, rows, wa, wbq, wbkv, q_own, kv_own, bq_own,
    kv, q_raw, q_mul, near, lam, acc, mx, ls, stage, back, b_heads,
    weights, part, crossed, chip, far_l, far_r, got_l, got_r, relayed,
    x_s, pw_s, os, orr, xs, xr_s, xds, xdr,
    a2a_s, a2a_r, zs, zr, rs, rr, ds, dr, q_s, q_r, small_s, small_r, ret_s, ret_r,
    w_s, cr_s, cr_r, fs, fr, gs, ss, gr,
):
    s, t = lax.axis_index("sp"), lax.axis_index("tp")
    z, y = s // 4, s % 4
    x, c = t // 2, t % 2
    xr, xl, xf = (x + 1) % 4, (x + 3) % 4, (x + 2) % 4
    other, right, left = 2 * x + 1 - c, 2 * xr + c, 2 * xl + c
    beyond = 2 * xf + c
    up, down = (z + 1) % 4, (z + 3) % 4
    far = (z + 2) % 4
    mate = 3 - z
    side = z + 1 - 2 * (z % 2)
    quarter = 2 * c + z // 2
    most = jnp.maximum(z, mate)
    lane = lax.broadcasted_iota(jnp.int32, (1, 128), 1)

    x_load = pltpu.make_async_copy(x_hbm, x_in, x_s)
    x_load.start()
    mixed = y // 2 == c
    loads = [
        pltpu.make_async_copy(wq_in, wa.at[:, pl.ds(0, 256)], pw_s.at[2]),
        pltpu.make_async_copy(wk_in, wa.at[:, pl.ds(256, 256)], pw_s.at[0]),
        pltpu.make_async_copy(wv_in, wa.at[:, pl.ds(512, 256)], pw_s.at[1]),
        pltpu.make_async_copy(wbq_in, wbq, pw_s.at[3]),
        pltpu.make_async_copy(wbk_in, wbkv.at[pl.ds(0, 64)], pw_s.at[4]),
        pltpu.make_async_copy(wbv_in, wbkv.at[pl.ds(64, 64)], pw_s.at[5]),
    ]

    def fetch(n, which):
        columns = pl.ds(pl.multiple_of(n * CW, CW), CW)
        source = aw_in if which == 0 else bw_in
        return pltpu.make_async_copy(
            source.at[:, columns], weights.at[n, pl.ds(256 * which, 256)], w_s
        )

    barrier = pltpu.get_barrier_semaphore()

    def greet(row, col):
        pl.semaphore_signal(barrier, inc=1, device_id=(row, col), device_id_type=MESH)

    for j in range(4):
        for core in range(2):
            if j == 0:
                @pl.when(core != c)
                def _(core=core):
                    greet(4 * z + y, 2 * x + core)
            else:
                greet(4 * z + (y + j) % 4, 2 * x + core)
            greet(4 * mate + (y + j) % 4, 2 * x + core)
    greet(4 * side + y, t)
    greet(s, right)
    greet(s, left)
    rim_up = (y == 3) & (z % 2 == 0)
    rim_down = (y == 0) & (z % 2 == 1)

    @pl.when(rim_up)
    def _():
        greet(s + 1, t)

    @pl.when(rim_down)
    def _():
        greet(s - 1, t)

    x_load.wait()
    for load in loads:
        load.start()
    pl.semaphore_wait(barrier, 18 + jnp.where(rim_up | rim_down, 1, 0))

    halves = (pl.ds(0, 2048), pl.ds(2048, 2048))
    every = pl.ds(0, 16)

    def mine16(g):
        return pl.ds(pl.multiple_of(16 * g, 16), 16)

    def own_send(g, way, which):
        return remote(
            x_in.at[mine16(g), halves[which]], rows.at[g, t, every, halves[which]],
            os, orr.at[g, way, which], s, right if way == 0 else left,
        )

    def own_wait(g, way, which):
        spot = rows.at[g, left if way == 0 else right, every, halves[which]]
        return remote(
            spot, spot, os, orr.at[g, way, which],
            s, right if way == 0 else left,
        )

    def xrelay_send(g, way):
        spot = rows.at[g, left if way == 0 else right, every, halves[way]]
        return remote(spot, spot, xs, xr_s.at[g], s, right if way == 0 else left)

    def xrelay_wait(g):
        spot = rows.at[g, beyond]
        return remote(spot, spot, xs, xr_s.at[g], s, right)

    def own_cross(g):
        return remote(x_in.at[mine16(g)], rows.at[g, t], xds, xdr.at[g], s, other)

    def xcross(g, where):
        spot = rows.at[g, 2 * where + c]
        return remote(spot, spot, xds, xdr.at[g], s, other)

    def xcross_wait(g):
        spot = rows.at[g, pl.ds(0, 4)]
        return remote(spot, spot, xds, xdr.at[g], s, other)

    def own_start(g):
        own_send(g, 0, 0).start()
        own_send(g, 1, 1).start()
        own_send(g, 0, 1).start()
        own_send(g, 1, 0).start()
        own_cross(g).start()

    def kv_send(g, head, part_of):
        return remote(
            kv_own.at[head, part_of, g], kv.at[part_of, z, g, y],
            a2a_s, a2a_r.at[g],
            4 * z + 2 * c + head, 2 * x + part_of,
        )

    def kv_local(head, part_of):
        return (2 * c + head == y) & (part_of == c)

    def a2a_wait(g, count):
        spot = kv.at[c, z, g, pl.ds(0, count)]
        return remote(spot, spot, a2a_s, a2a_r.at[g], s, other)

    def z_send(g, way):
        spot = kv.at[c, z, g]
        return remote(spot, spot, zs, zr.at[g, way], 4 * (up, down)[way] + y, t)

    def z_wait(g, way):
        spot = kv.at[c, (down, up)[way], g]
        return remote(spot, spot, zs, zr.at[g, way], 4 * (up, down)[way] + y, t)

    def relay_send(g, way):
        spot = kv.at[c, (down, up)[way], g, pl.ds(2 * way, 2)]
        return remote(spot, spot, rs, rr.at[g], 4 * (up, down)[way] + y, t)

    def relay_whole(g):
        spot = kv.at[c, up, g]
        return remote(spot, spot, rs, rr.at[g], 4 * down + y, t)

    def relay_wait(g):
        spot = kv.at[c, far, g]
        return remote(spot, spot, rs, rr.at[g], 4 * up + y, t)

    def cross_send(level, g):
        spot = kv.at[c, level, g]
        return remote(spot, spot, ds, dr.at[level, g // 2], s, other)

    def cross_wait(level, pair):
        spot = kv.at[1 - c, level, pl.ds(2 * pair, 2)]
        return remote(spot, spot, ds, dr.at[level, pair], s, other)

    def spread(g):
        @pl.when(mixed)
        def _():
            a2a_wait(g, 3).wait_recv()

        @pl.when(~mixed)
        def _():
            a2a_wait(g, 4).wait_recv()

        z_send(g, 0).start()

        @pl.when(z < 3)
        def _():
            z_send(g, 1).start()

        cross_send(z, g).start()

    def zrelay(g):
        z_wait(g, 0).wait_recv()

        @pl.when(z >= 2)
        def _():
            relay_send(g, 0).start()

        cross_send(down, g).start()

        @pl.when(z != 2)
        def _():
            z_wait(g, 1).wait_recv()

            @pl.when(z == 3)
            def _():
                relay_whole(g).start()

            @pl.when(z < 2)
            def _():
                relay_send(g, 1).start()

            cross_send(up, g).start()

    def zfar(g):
        @pl.when(z != 1)
        def _():
            relay_wait(g).wait_recv()
            cross_send(far, g).start()

    own_start(0)
    own_start(1)
    lam_send = remote(lam.at[c], lam.at[c], small_s.at[0], small_r.at[0], s, other)
    for g in range(GROUPS):
        rows[g, t] = x_in[16 * g : 16 * (g + 1)]
    for head in range(2):
        lam[c, head] = jnp.broadcast_to(few_in[0:1, head : head + 1], (8, 256))
    acc[...] = jnp.zeros_like(acc)
    ls[...] = jnp.zeros_like(ls)
    mx[...] = jnp.full_like(mx, mask_fill)

    @pl.when(s == 0)
    def _():
        near[pl.ds(0, 128)] = jnp.zeros((128, 128), BF16)

    def near_rows(g):
        own_wait(g, 0, 0).wait_recv()
        xrelay_send(g, 0).start()
        own_wait(g, 1, 1).wait_recv()
        xrelay_send(g, 1).start()

        @pl.when(g < GROUPS - 2)
        def _():
            own_start(g + 2)

        own_wait(g, 0, 1).wait_recv()
        xcross(g, xl).start()
        own_wait(g, 1, 0).wait_recv()
        xcross(g, xr).start()

    near_rows(0)
    near_rows(1)

    def far_rows(g):
        xrelay_wait(g).wait_recv()
        xcross(g, xf).start()

    def project_b(at, count):
        block = rows[at : at + count].reshape(128 * count, 4096)
        b_queries = jnp.dot(block, wbq[...], preferred_element_type=F32).astype(BF16)
        b_pair = lax.dot_general(block, wbkv[...], NT, preferred_element_type=F32).astype(BF16)
        for k in range(count):
            for d in range(8):
                first_row = 64 * d + 16 * (at + k)
                take = slice(128 * k + 16 * d, 128 * k + 16 * (d + 1))
                bq_own[first_row : first_row + 16] = b_queries[take]
                near[first_row + 128 : first_row + 144] = b_pair[take]

    def gather(g, carry):
        @pl.when(g == 0)
        def _():
            far_rows(0)
            near_rows(2)

        @pl.when(g == 1)
        def _():
            far_rows(1)

        @pl.when(g == 2)
        def _():
            near_rows(3)
            spread(0)
            far_rows(2)

        @pl.when(g == 3)
        def _():
            spread(1)
            far_rows(3)

        @pl.when(g == 0)
        def _():
            for load in loads[:3]:
                load.wait()

        xcross_wait(g).wait_recv()
        block = rows[g].reshape(128, 4096)
        found = jnp.dot(block, wa[...], preferred_element_type=F32)
        q_own[0, g] = found[:, :128].astype(BF16)
        q_own[1, g] = found[:, 128:256].astype(BF16)
        keys, values = found[:, 256:512], found[:, 512:]
        for head in range(2):
            lanes = slice(128 * head, 128 * (head + 1))
            kv_own[head, 0, g] = keys[:, lanes].astype(BF16)
            kv_own[head, 1, g] = jnp.transpose(values[:, lanes]).astype(BF16)

            @pl.when(2 * c + head == y)
            def _(head=head):
                kv[c, z, g, y] = kv_own[head, c, g]

            for part_of in range(2):
                @pl.when(~kv_local(head, part_of))
                def _(head=head, part_of=part_of):
                    kv_send(g, head, part_of).start()

        send_queries(g)

        @pl.when(g == 0)
        def _():
            for n in range(NC):
                fetch(n, 0).start()
                fetch(n, 1).start()
            for load in loads[3:]:
                load.wait()
            project_b(0, 1)

        return carry

    def q_send(g, head, k, core):
        goal = z if k == 0 else mate
        return remote(
            q_own.at[head, g, pl.ds(32 * (2 * core + goal // 2), 32)],
            q_raw.at[4 * (z // 2) + y, g], q_s, q_r,
            4 * goal + 2 * c + head, 2 * x + core,
        )

    def q_local(head, k, core):
        return (2 * c + head == y) & (core == c) & (k == 0)

    def send_queries(g):
        for head in range(2):
            for k in range(2):
                for core in range(2):
                    @pl.when(~q_local(head, k, core))
                    def _(head=head, k=k, core=core):
                        q_send(g, head, k, core).start()

            @pl.when(2 * c + head == y)
            def _(head=head):
                q_raw[4 * (z // 2) + y, g] = q_own[head, g, pl.ds(32 * quarter, 32)]

    def q_all(count):
        spot = q_raw.at[pl.ds(0, count)]
        return remote(spot, spot, q_s, q_r, s, other)

    lam_send.start()
    lax.fori_loop(0, GROUPS, gather, 0)
    project_b(1, 1)
    spread(2)
    project_b(2, 2)
    zrelay(0)

    rim_send = remote(
        near.at[pl.ds(512, 128)], near.at[pl.ds(0, 128)], small_s.at[1], small_r.at[1],
        jnp.minimum(s + 1, 15), t,
    )

    @pl.when(s < 15)
    def _():
        rim_send.start()

    def windowed(block, carry):
        start = pl.multiple_of(block * 128, 128)
        span = near[pl.ds(start, 256)]
        span32 = span.astype(F32)
        turned = jnp.concatenate([span32[:, HEAD_DIM:], span32[:, :HEAD_DIM]], axis=1)
        keys = jnp.where(lane < HEAD_DIM, span32, turned).astype(BF16)
        values = jnp.transpose(span32)[HEAD_DIM:].astype(BF16)
        parts = []
        sinks = []
        for j in range(4):
            own = bq_own[pl.ds(start, 128), 128 * (j // 2) : 128 * (j // 2 + 1)]
            mine = (lane >= HEAD_DIM) if j % 2 else (lane < HEAD_DIM)
            parts.append(jnp.where(mine, own.astype(F32), 0.0).astype(BF16))
            sinks.append(jnp.broadcast_to(few_in[0:1, 2 + j : 3 + j] * LOG2E, (1, 128)))
        queries = jnp.concatenate(parts, axis=0)
        sink = jnp.concatenate(sinks, axis=1)
        scores = lax.dot_general(keys, queries, NT, preferred_element_type=F32)
        scores = scores * (LOG2E * HEAD_DIM ** (-0.5))
        key_at = lax.broadcasted_iota(jnp.int32, (256, 512), 0)
        query_at = lax.broadcasted_iota(jnp.int32, (256, 512), 1) % 128
        first = jnp.where((s == 0) & (block == 0), 128, 0)
        allowed = (key_at > query_at) & (key_at <= query_at + WINDOW) & (key_at >= first)
        scores = jnp.where(allowed, scores, mask_fill)
        top = jnp.maximum(jnp.max(scores, axis=0, keepdims=True), sink)
        weights = jnp.exp2(scores - top)
        total = jnp.sum(weights, axis=0, keepdims=True) + jnp.exp2(sink - top)
        found = jnp.dot(values, weights.astype(BF16), preferred_element_type=F32) / total
        tall = jnp.concatenate([found[:, 128 * j : 128 * (j + 1)] for j in range(4)], axis=0)
        b_heads[pl.ds(start, 128)] = jnp.transpose(tall).astype(BF16)
        return carry

    windowed(1, 0)
    spread(3)

    @pl.when(mixed)
    def _():
        q_all(7).wait_recv()

    @pl.when(~mixed)
    def _():
        q_all(8).wait_recv()

    for pair in range(2):
        for row in range(4):
            raw = q_raw[4 * pair + row].astype(F32)
            raw = jnp.concatenate(
                [raw[g, 16 * d : 16 * (d + 1)] for d in range(2) for g in range(4)], axis=0
            )
            wide = raw * (LOG2E * HEAD_DIM ** (-0.5))
            high = wide.astype(BF16).astype(F32)
            both = jnp.transpose(jnp.concatenate([high, wide - high], axis=1))
            tall = lax.broadcasted_iota(jnp.int32, (256, 1), 0) % 128
            for m in range(2):
                mine = (tall >= HEAD_DIM) if m else (tall < HEAD_DIM)
                i = pair * 4 + (row // 2) * 2 + m
                span = slice(128 * (row % 2), 128 * (row % 2) + 128)
                q_mul[i, :, span] = jnp.where(mine, both, 0.0).astype(BF16)

    def unit(level, pair):
        keys = kv[0, level, pl.ds(2 * pair, 2)].reshape(1024, 128)
        held = kv[1, level, pl.ds(2 * pair, 2)].reshape(1024, 128)
        lookup = jnp.concatenate([held[128 * k : 128 * (k + 1)] for k in range(8)], axis=1)
        lookup = jnp.concatenate([lookup, jnp.ones((16, 1024), BF16)], axis=0)
        return jnp.concatenate([keys, keys], axis=1), lookup

    def small_unit(level, pair, two):
        rows_of = (pl.ds(2 * pair, 2), pl.ds(2 * two, 2))
        keys = kv[0, level, rows_of[0], rows_of[1]].reshape(512, 128)
        held = kv[1, level, rows_of[0], rows_of[1]].reshape(512, 128)
        lookup = jnp.concatenate([held[128 * k : 128 * (k + 1)] for k in range(4)], axis=1)
        lookup = jnp.concatenate([lookup, jnp.ones((16, 512), BF16)], axis=0)
        return jnp.concatenate([keys, keys], axis=1), lookup

    key_at = lax.broadcasted_iota(jnp.int32, (256, 256), 0)
    query_at = lax.broadcasted_iota(jnp.int32, (256, 256), 1)
    apart = 512 * (key_at // 128) + 64 * ((key_at % 128) // 16) + key_at % 16
    apart = apart - (query_at % 128) - 512 * (query_at // 128)

    def attend(level, pair, sel):
        mark = jnp.where(sel == 0, jnp.minimum(z, mate), jnp.maximum(z, mate))

        def score(keys, i):
            return [
                jnp.dot(keys[256 * k : 256 * (k + 1)], q_mul[i], preferred_element_type=F32)
                for k in range(2)
            ]

        @pl.when(level < mark)
        def _():
            keys, lookup = unit(level, pair)
            items = []
            for h in range(2):
                span = slice(512 * h, 512 * (h + 1))
                for k in range(4):
                    i = sel * 4 + k
                    items.append(
                        (i, functools.partial(score, keys[span], i), lookup[:, span])
                    )
            soft_chunk(items, mx, ls, acc)

        @pl.when(level == mark)
        def _():
            base = 128 * quarter - 32 * pair

            def hidden(keys, i):
                return [
                    jnp.where(apart <= base - 16 * k, piece, mask_fill)
                    for k, piece in enumerate(score(keys, i))
                ]

            items = []
            low = small_unit(level, pair, 0)
            high = small_unit(level, pair, 1)
            for g, (keys, lookup), rule in ((0, low, hidden), (1, low, score), (1, high, hidden)):
                for m in range(2):
                    i = sel * 4 + g * 2 + m
                    items.append((i, functools.partial(rule, keys, i), lookup))
            soft_chunk(items, mx, ls, acc)

    lam_send.wait_recv()
    mixing = lam[y // 2, y % 2, 0:1, :]
    gain = few_in[:, 128:256] * head_scale

    def ret_send(pair, row):
        goal = jnp.minimum(z, mate) if pair == 0 else jnp.maximum(z, mate)
        return remote(
            stage.at[4 * pair + row], back.at[4 * (y % 2) + quarter], ret_s, ret_r,
            4 * goal + row, 2 * x + y // 2,
        )

    def ret_local(pair, row):
        return (pair == z // 2) & (row == y) & (y // 2 == c)

    def finish(pair):
        for g in range(2):
            i = pair * 4 + g * 2
            first_mean = acc[i] / ls[i]
            second_mean = acc[i + 1] / ls[i + 1]
            gap = first_mean - mixing * second_mean
            square = jnp.mean(gap * gap, axis=0, keepdims=True)
            done = gap * lax.rsqrt(square + norm_eps)
            tall = (jnp.transpose(done) * gain).astype(BF16)
            for k in range(2):
                row = 2 * g + k
                stage[4 * pair + row] = tall[128 * k : 128 * (k + 1)]

                @pl.when(~ret_local(pair, row))
                def _(pair=pair, row=row):
                    ret_send(pair, row).start()

                @pl.when(ret_local(pair, row))
                def _(pair=pair, row=row):
                    back[4 * (y % 2) + quarter] = stage[4 * pair + row]

    def step(it, carry):
        @pl.when(it == 1)
        def _():
            zrelay(1)
            zfar(0)

        @pl.when(it == 2)
        def _():
            windowed(2, 0)
            zrelay(2)
            windowed(3, 0)
            zrelay(3)

        @pl.when(it == 3)
        def _():
            zfar(1)

        @pl.when(it == 4)
        def _():
            @pl.when(s > 0)
            def _():
                rim_send.wait_recv()

            windowed(0, 0)

        @pl.when(it == 5)
        def _():
            zfar(2)
            zfar(3)

        @pl.when((it == 7) & (z != 2))
        def _():
            finish(0)

        level = jnp.where(
            it < 2, z,
            jnp.where(
                (it == 2) | (it == 5), down, jnp.where((it == 3) | (it == 6), up, far)
            ),
        )
        pair = jnp.where((it == 1) | (it >= 5), 1, 0)
        @pl.when(level <= most)
        def _():
            cross_wait(level, pair).wait_recv()

            def one(sel, inner):
                attend(level, pair, sel)
                return inner

            lax.fori_loop(0, 2, one, 0)

        return carry

    lax.fori_loop(0, 8, step, 0)

    @pl.when(z == 2)
    def _():
        finish(0)

    finish(1)

    def ret_all(count):
        spot = back.at[pl.ds(0, count)]
        return remote(spot, spot, ret_s, ret_r, s, other)

    @pl.when(mixed)
    def _():
        ret_all(7).wait_recv()

    @pl.when(~mixed)
    def _():
        ret_all(8).wait_recv()

    heads = jnp.concatenate(
        [back[0:4].reshape(512, 128), back[4:8].reshape(512, 128), b_heads[...]], axis=1
    )
    first, second = pl.ds(0, 32), pl.ds(32, 32)

    def cross(n):
        return remote(part.at[n, 1 - c], crossed.at[n], cr_s, cr_r.at[n], s, other)

    def far_send(n, way):
        rows = first if way == 0 else second
        return remote(
            chip.at[n, xf, rows], (far_l if way == 0 else far_r).at[n],
            fs, fr.at[n], s, right if way == 0 else left,
        )

    def near_send(n, way):
        rows = second if way == 0 else first
        return remote(
            chip.at[n, xr if way == 0 else xl, rows], (got_l if way == 0 else got_r).at[n, rows],
            gs, gr.at[n], s, right if way == 0 else left,
        )

    def sum_send(n, way):
        rows = first if way == 0 else second
        return remote(
            relayed.at[n, way], (got_l if way == 0 else got_r).at[n, rows],
            ss, gr.at[n], s, right if way == 0 else left,
        )

    def multiply(n):
        partial = jnp.dot(heads, weights[n], preferred_element_type=F32).astype(BF16)
        for col in range(8):
            part[n, col % 2, col // 2] = partial[64 * col : 64 * (col + 1)]
        cross(n).start()

    def join(n):
        cross(n).wait_recv()
        chip[n] = (part[n, c].astype(F32) + crossed[n].astype(F32)).astype(BF16)
        far_send(n, 0).start()
        far_send(n, 1).start()
        near_send(n, 0).start()
        near_send(n, 1).start()

    def pass_on(n, carry):
        remote(relayed.at[n], relayed.at[n], fs, fr.at[n], s, right).wait_recv()
        relayed[n, 0] = (chip[n, xr, first].astype(F32) + far_l[n].astype(F32)).astype(BF16)
        sum_send(n, 0).start()
        relayed[n, 1] = (chip[n, xl, second].astype(F32) + far_r[n].astype(F32)).astype(BF16)
        sum_send(n, 1).start()
        return carry

    remote(weights, weights, gs, w_s, s, other).wait_recv()
    multiply(0)

    def run(n, carry):
        multiply(n)
        join(n - 1)
        return carry

    lax.fori_loop(1, NC, run, 0)
    join(NC - 1)
    def drained(spot, sem):
        remote(spot, spot, sem, q_r, s, other).wait_send()

    drained(rows.at[0], os)
    drained(x_in, xs)
    drained(rows.at[pl.ds(0, 2)], xds)
    @pl.when(z == 3)
    def _():
        drained(kv.at[0, 0], zs)
        drained(kv.at[0, 0], rs)
        drained(kv.at[0, 0, pl.ds(0, 2)], rs)

    @pl.when(z < 3)
    def _():
        drained(kv.at[0, pl.ds(0, 2)], zs)
        drained(kv.at[0, 0, pl.ds(0, 2)], rs)

    @pl.when((z == 0) | (z == 3))
    def _():
        drained(kv.at[0], ds)

    @pl.when((z == 1) | (z == 2))
    def _():
        drained(kv.at[0, pl.ds(0, 3)], ds)

    lam_send.wait_send()

    @pl.when(s < 15)
    def _():
        rim_send.wait_send()

    @pl.when(mixed)
    def _():
        drained(kv.at[0, 0, pl.ds(0, 3)], a2a_s)
        q_all(7).wait_send()
        ret_all(7).wait_send()

    @pl.when(~mixed)
    def _():
        drained(kv.at[0, 0], a2a_s)
        q_all(8).wait_send()
        ret_all(8).wait_send()

    lax.fori_loop(0, NC, pass_on, 0)

    drained(crossed, cr_s)
    drained(relayed, fs)
    drained(relayed, gs)
    for n in range(NC):
        spot = chip.at[n, pl.ds(0, 2)]
        remote(spot, spot, ss, gr.at[n], s, other).wait_recv()
        total = chip[n, x].astype(F32) + got_l[n].astype(F32) + got_r[n].astype(F32)
        out[:, n * CW : (n + 1) * CW] = total.astype(BF16)
    drained(relayed, ss)


def layer(*operands):
    vmem = pl.BlockSpec(memory_space=VMEM)
    hbm = pl.BlockSpec(memory_space=pltpu.HBM)
    dma = pltpu.SemaphoreType.DMA
    return pl.pallas_call(
        layer_kernel,
        out_shape=jax.ShapeDtypeStruct((64, 4096), BF16),
        in_specs=[hbm] * 7 + [vmem] + [hbm] * 2,
        out_specs=vmem,
        scratch_shapes=[
            VMEM((64, 4096), BF16),
            VMEM((4, 8, 16, 4096), BF16),
            VMEM((4096, 768), BF16), VMEM((4096, 256), BF16), VMEM((128, 4096), BF16),
            VMEM((2, 4, 128, 128), BF16), VMEM((2, 2, 4, 128, 128), BF16), VMEM((512, 256), BF16),
            VMEM((2, 4, 4, 4, 128, 128), BF16),
            VMEM((8, 4, 32, 128), BF16),
            VMEM((8, 256, 256), BF16),
            VMEM((640, 128), BF16),
            VMEM((2, 2, 8, 256), F32),
            VMEM((8, 128, 256), F32),
            VMEM((8, 1, 256), F32),
            VMEM((8, 1, 256), F32),
            VMEM((8, 128, 128), BF16),
            VMEM((8, 128, 128), BF16),
            VMEM((512, 256), BF16),
            VMEM((NC, 512, CW), BF16),
            VMEM((NC, 2, 4, 64, CW), BF16),
            VMEM((NC, 4, 64, CW), BF16),
            VMEM((NC, 4, 64, CW), BF16),
            VMEM((NC, 32, CW), BF16),
            VMEM((NC, 32, CW), BF16),
            VMEM((NC, 64, CW), BF16),
            VMEM((NC, 64, CW), BF16),
            VMEM((NC, 2, 32, CW), BF16),
            dma, dma((6,)), dma, dma((4, 2, 2)), dma, dma((4,)), dma, dma((4,)),
            dma, dma((4,)), dma, dma((4, 2)), dma, dma((4,)), dma, dma((4, 2)),
            dma, dma, dma((2,)), dma((2,)), dma, dma,
            dma, dma, dma((NC,)), dma, dma((NC,)), dma, dma, dma((NC,)),
        ],
        compiler_params=pltpu.CompilerParams(
            collective_id=0, has_side_effects=True, vmem_limit_bytes=int(53.2 * 2**20)
        ),
        name="layer",
    )(*operands)


def shards(
    inputs,
    a_query_w,
    a_key_w,
    a_value_w,
    b_query_w,
    b_key_w,
    b_value_w,
    head_lambda,
    head_gain,
    sink_logit,
    a_out_w,
    b_out_w,
):
    few = jnp.concatenate([head_lambda, sink_logit, jnp.zeros((122,), F32), head_gain])[None]
    return layer(
        inputs, a_query_w, a_key_w, a_value_w, b_query_w, b_key_w.T, b_value_w.T,
        few, a_out_w, b_out_w,
    )


def solution(mesh):
    return jax.shard_map(
        shards,
        mesh=mesh,
        in_specs=(
            P(("sp", "tp"), None),
            P(None, "tp"),
            P(None, "tp"),
            P(None, "tp"),
            P(None, "tp"),
            P(None, "tp"),
            P(None, "tp"),
            P("tp"),
            P(),
            P("tp"),
            P("tp", None),
            P("tp", None),
        ),
        out_specs=P(("sp", "tp"), None),
        check_vma=False,
    )
```
